128 devices in a mesh: kv: 32 (over z, y, core), tp: 4 (over x).
Axes of the slice: x: 4, y: 4, z: 4, core: 2. Of those that a mesh axis runs over, the one named last changes fastest.
Arguments:
- queries: bfloat16 [2, 12288, 1024], P(None, 'kv', 'tp'), may hold values from -112 to 112
- key_states: bfloat16 [2, 12288, 256], P(None, 'kv', 'tp'), may hold values from -4 to 4
- value_states: bfloat16 [2, 12288, 256], P(None, 'kv', 'tp'), may hold values from -6 to 6
- cotangent: bfloat16 [2, 12288, 1024], P(None, 'kv', 'tp'), may hold values from -6 to 6
- gate_logits: float32 [2, 12288, 16], P(None, 'kv', 'tp'), may hold values from -6 to 6
- layer_input: bfloat16 [2, 12288, 4096], P(None, ('kv', 'tp')), may hold values from -6 to 6
- chosen: int32 [2, 192, 4, 16], P(None, 'kv', 'tp'), may hold values from 0 to 191, as said below
Outputs:
- query_grad: bfloat16 [2, 12288, 1024], P(None, 'kv', 'tp')
- key_grad: bfloat16 [2, 12288, 256], P(None, 'kv', 'tp')
- value_grad: bfloat16 [2, 12288, 256], P(None, 'kv', 'tp')
- value_weight_grad: float32 [4096, 256], P(('kv', 'tp'))
The draws below stay inside these ranges and needn't reach their ends.
Inputs may be any that keep to these rules, and one draw needn't show every extreme that they name: `chosen`: for each sequence, query block b and key head, the 16 entries are distinct blocks; they include b itself and block 0; blocks after b hold only keys after all of the block's queries. Taking the 6 query blocks of one index of kv together (aligned), one sequence and one key head, at most 2 distinct blocks held by any one earlier index of kv are named, and some index reaches 2.
All inputs are finite; a program needn't handle non-finite values.
Results may differ from the reference program's by a relative error of at most 0.0058.
Values may be sent and summed in bfloat16 or wider, within the bound.
A program may use at most 128 MiB of HBM per device.

```python
import jax
import jax.numpy as jnp
from jax import lax

D = 4096
H = 16
KVH = 4
HD = 64
BLK = 64
TOPK = 16
MOST = 2
SEQS = 2
BPD = 6
SEQ = 12288
NBLK = 192
N_KV = 32


def key_field(key):
    drawn = jax.random.normal(jax.random.fold_in(key, 11), (SEQS, SEQ, KVH * HD), jnp.float32)
    return jnp.clip(drawn, -4.0, 4.0)


def draw_key_states(key, part):
    return key_field(key).astype(jnp.bfloat16)


def draw_queries(key, part):
    drawn = jnp.clip(jax.random.normal(jax.random.fold_in(key, 23), (SEQS, SEQ, H * HD), jnp.float32), -4.0, 4.0)
    return drawn.astype(jnp.bfloat16)


def draw_chosen(key, part):
    blocks = jnp.arange(NBLK, dtype=jnp.int32)
    holder = blocks // BPD
    within = blocks % BPD
    query_dev = blocks // BPD
    query_in = blocks % BPD
    jitter = jax.random.randint(jax.random.fold_in(key, 3), (SEQS, N_KV, KVH, NBLK), 0, 1024)
    ranking = jitter * BPD + within
    ranking = jnp.where(blocks == 0, 1024 * BPD + 1, ranking)
    grouped = ranking.reshape(SEQS, N_KV, KVH, N_KV, BPD)
    order_rank = jnp.sum((grouped[..., None, :] > grouped[..., :, None]).astype(jnp.int32), axis=-1)
    usable = (order_rank < MOST).reshape(SEQS, N_KV, KVH, NBLK)
    usable_q = usable[:, query_dev]
    earlier = (holder[None, :] < query_dev[:, None])[None, :, None, :]
    own_ok = (holder[None, :] == query_dev[:, None]) & (within[None, :] <= query_in[:, None])
    forced = (own_ok | (blocks == 0)[None, :])[None, :, None, :]
    future = (blocks[None, :] > blocks[:, None])[None, :, None, :]
    levels = jnp.where(forced, 3, jnp.where(earlier & usable_q, 2, jnp.where(future, 1, 0)))
    pick_noise = jax.random.randint(jax.random.fold_in(key, 5), (SEQS, NBLK, KVH, NBLK), 0, 512)
    distance = query_dev[:, None] - holder[None, :]
    closeness = jnp.clip(512 - 64 * distance, 0, 1023)
    skewed = pick_noise + closeness[None, :, None, :]
    nearness = 1023 - jnp.minimum(jnp.abs(blocks[None, :] - blocks[:, None]), 1023)
    secondary = jnp.where(levels == 1, nearness[None, :, None, :], skewed)
    priority = levels * 2 ** 22 + secondary * NBLK + blocks[None, None, None, :]
    values_top, picked = lax.top_k(priority.astype(jnp.int32), TOPK)
    return picked.astype(jnp.int32)


def level_of(own_key, shape, shards, smallest, top_value):
    loudness = 1.0
    for axis_at, shards_of in shards:
        heights = jax.random.uniform(jax.random.fold_in(jax.random.fold_in(own_key, 6), axis_at), (shards_of,), jnp.float32, smallest / len(shards), top_value / len(shards))
        loudness = loudness * jnp.repeat(jnp.exp(heights), shape[axis_at] // shards_of).reshape((-1,) + (1,) * (len(shape) - 1 - axis_at))
    return loudness


def centred(key, shape, deviation, bound, shards=(), held_as=jnp.bfloat16):
    result = jax.random.normal(key, shape, jnp.float32) * deviation
    if len(shards) > 0:
        result = level_of(key, shape, shards, -0.22, 0.18) * result
    return jnp.clip(result, min=-bound, max=bound).astype(held_as)


def setup_inputs(seed: int = 0) -> dict:
    key_list = jax.random.split(jax.random.key(seed), 8)
    return {
        "queries": draw_queries(jax.random.fold_in(key_list[7], 71), 0),
        "key_states": draw_key_states(jax.random.fold_in(key_list[7], 71), 0),
        "value_states": centred(key_list[2], (SEQS, SEQ, KVH * HD), 1.0, 6.0, ((1, 32), (2, 4))),
        "cotangent": centred(key_list[3], (SEQS, SEQ, H * HD), 1.0, 6.0, ((1, 32), (2, 4))),
        "gate_logits": centred(key_list[4], (SEQS, SEQ, H), 1.5, 6.0, ((1, 32), (2, 4)), jnp.float32),
        "layer_input": centred(key_list[5], (SEQS, SEQ, D), 1.0, 6.0, ((1, 128),)),
        "chosen": draw_chosen(jax.random.fold_in(key_list[7], 71), 0),
    }


def reference(queries, key_states, value_states, cotangent, gate_logits, layer_input, chosen):
    seq_count, seq_len, row_width = queries.shape
    per_group = H // KVH
    total_blocks = seq_len // BLK
    score_scale = HD ** -0.5
    key_blocks = key_states.reshape(seq_count, total_blocks, BLK, KVH, HD)
    value_blocks = value_states.reshape(seq_count, total_blocks, BLK, KVH, HD)
    query_blocks = queries.reshape(seq_count, total_blocks, BLK, KVH, per_group, HD)
    grad_blocks = cotangent.reshape(seq_count, total_blocks, BLK, KVH, per_group, HD)
    gate_values = jax.nn.sigmoid(gate_logits.astype(jnp.float32)).reshape(seq_count, total_blocks, BLK, KVH, per_group)
    group_index = jnp.arange(KVH, dtype=jnp.int32)[:, None]
    offsets = jnp.arange(BLK, dtype=jnp.int32)

    def advance(totals, position):
        key_acc, value_acc = totals
        seq_index = position // total_blocks
        block_index = position % total_blocks
        picked = chosen[seq_index, block_index]
        picked_keys = key_blocks[seq_index][picked, :, group_index].astype(jnp.float32)
        picked_values = value_blocks[seq_index][picked, :, group_index].astype(jnp.float32)
        query_rows = query_blocks[seq_index, block_index].astype(jnp.float32)
        scores = jnp.einsum("qgpd,gknd->gpqkn", query_rows, picked_keys) * score_scale
        query_pos = block_index * BLK + offsets
        key_pos = picked[:, :, None] * BLK + offsets
        allowed = key_pos[:, None, None, :, :] <= query_pos[None, None, :, None, None]
        scores = jnp.where(allowed, scores, -jnp.inf)
        row_max = jnp.max(scores, axis=(3, 4), keepdims=True)
        exp_terms = jnp.exp(scores - row_max)
        weights = exp_terms / jnp.sum(exp_terms, axis=(3, 4), keepdims=True)
        weights_bf = weights.astype(jnp.bfloat16).astype(jnp.float32)
        branch_out = jnp.einsum("gpqkn,gknd->qgpd", weights_bf, picked_values)
        branch_grad = (gate_values[seq_index, block_index][..., None] * grad_blocks[seq_index, block_index].astype(jnp.float32)).astype(jnp.bfloat16).astype(jnp.float32)
        row_dot = jnp.sum(branch_grad * branch_out, axis=3)
        weight_grad = jnp.einsum("qgpd,gknd->gpqkn", branch_grad, picked_values)
        score_grad = (weights * (weight_grad - jnp.transpose(row_dot, (1, 2, 0))[..., None, None]) * score_scale).astype(jnp.bfloat16).astype(jnp.float32)
        query_grad = jnp.einsum("gpqkn,gknd->qgpd", score_grad, picked_keys).astype(jnp.bfloat16)
        pick_key = jnp.einsum("gpqkn,qgpd->gknd", score_grad, query_rows)
        pick_value = jnp.einsum("gpqkn,qgpd->gknd", weights_bf, branch_grad)
        key_acc = key_acc.at[seq_index, picked, :, group_index].add(pick_key)
        value_acc = value_acc.at[seq_index, picked, :, group_index].add(pick_value)
        return (key_acc, value_acc), query_grad

    empty = jnp.zeros((seq_count, total_blocks, BLK, KVH, HD), jnp.float32)
    (key_acc, value_acc), query_parts = lax.scan(advance, (empty, empty), jnp.arange(seq_count * total_blocks, dtype=jnp.int32))
    query_grad = query_parts.reshape(seq_count, seq_len, H * HD)
    key_grad = key_acc.reshape(seq_count, seq_len, KVH * HD).astype(jnp.bfloat16)
    value_grad = value_acc.reshape(seq_count, seq_len, KVH * HD).astype(jnp.bfloat16)
    value_weight_grad = jnp.einsum("std,ste->de", layer_input.astype(jnp.float32), value_grad.astype(jnp.float32))
    return query_grad, key_grad, value_grad, value_weight_grad
```

```python
import functools

import jax
import jax.numpy as jnp
from jax import lax
from jax.experimental import pallas as pl
from jax.experimental.pallas import tpu as pltpu
from jax.sharding import PartitionSpec as P

BLK = 64
MESH = pl.DeviceIdType.MESH
F32 = jnp.float32
BF16 = jnp.bfloat16
SEQS = 2
BPD = 6
ROWS = BPD * BLK
ZN = 4
YN = 4
DEVS = ZN * YN * 2
HD = 64
HEADS = 4
TOPK = 16
NEG = -1e30


def place():
    kv = lax.axis_index("kv")
    tp = lax.axis_index("tp")
    z, y, c = kv // 8, (kv // 2) % 4, kv % 2
    return kv, tp, z, y, c


def rcopy(src, dst, ssem, rsem, device):
    return pltpu.make_async_remote_copy(
        src_ref=src, dst_ref=dst, send_sem=ssem, recv_sem=rsem, device_id=device, device_id_type=MESH
    )


def entry_barrier(peers):
    sem = pltpu.get_barrier_semaphore()
    for peer in peers:
        pl.semaphore_signal(sem, inc=1, device_id=peer, device_id_type=MESH)
    pl.semaphore_wait(sem, len(peers))


def gather_kernel(k_ref, v_ref, out_ref, ssem, rsem, psend, precv):
    kv, tp, z, y, c = place()

    def zy(z_, y_):
        return (z_ % 4) * 8 + (y_ % 4) * 2 + c

    for s in range(SEQS):
        out_ref[s, kv] = jnp.concatenate([k_ref[s], v_ref[s]], axis=-1)
    partner = (kv + 1 - 2 * c, tp)
    entry_barrier([(zy(z, y + 1), tp), (zy(z, y + 3), tp), (zy(z + 1, y), tp), (zy(z + 3, y), tp), partner])

    half = ROWS // 2

    class Seq:
        def __init__(self, s):
            self.s = s
            self.base = s * 20
            self.sends = []
            self.pcount = 0

        def at(self, a, b):
            return zy(z + b, y + a) if self.s == 0 else zy(z + a, y + b)

        def dev(self, a, b):
            return (self.at(a, b), tp)

        def ref(self, a, b, part):
            chunk = out_ref.at[self.s, self.at(a, b)]
            if part is None:
                return chunk
            return chunk.at[pl.ds(part * half, half)]

        def send(self, i, a, b, part, to):
            r = self.ref(a, b, part)
            d = rcopy(r, r, ssem.at[self.base + i], rsem.at[self.base + i], self.dev(*to))
            d.start()
            self.sends.append(d)

        def recv(self, i, a, b, part):
            r = self.ref(a, b, part)
            rcopy(r, r, ssem.at[self.base + i], rsem.at[self.base + i], self.dev(0, 0)).wait_recv()

        def share(self, a, b):
            i = self.s * 16 + self.pcount
            self.pcount += 1
            r = self.ref(a, b, None)
            d = rcopy(r, r, psend.at[i], precv.at[i], partner)
            d.start()
            self.sends.append(d)

        def first(self):
            self.send(0, 0, 0, None, (1, 0))
            self.send(1, 0, 0, None, (-1, 0))
            self.second_start(0, 0)
            self.share(0, 0)

        def second_start(self, q, a):
            self.send(4 + 4 * q, a, 0, None, (0, 1))
            self.send(5 + 4 * q, a, 0, None, (0, -1))

        def second_forward(self, q, a):
            self.recv(4 + 4 * q, a, -1, None)
            self.send(6 + 4 * q, a, -1, 0, (0, 1))
            self.recv(5 + 4 * q, a, 1, None)
            self.send(7 + 4 * q, a, 1, 1, (0, -1))
            self.share(a, -1)
            self.share(a, 1)

        def second_end(self, q, a):
            self.recv(6 + 4 * q, a, 2, 0)
            self.recv(7 + 4 * q, a, 2, 1)
            self.share(a, 2)

        def first_forward(self):
            self.recv(0, -1, 0, None)
            self.send(2, -1, 0, 0, (1, 0))
            self.recv(1, 1, 0, None)
            self.send(3, 1, 0, 1, (-1, 0))
            self.second_start(1, -1)
            self.second_start(2, 1)
            self.share(-1, 0)
            self.share(1, 0)

        def first_end(self):
            self.recv(2, 2, 0, 0)
            self.recv(3, 2, 0, 1)
            self.second_start(3, 2)
            self.share(2, 0)

    seqs = [Seq(0), Seq(1)]
    for q in seqs:
        q.first()
    for q in seqs:
        q.first_forward()
    for q in seqs:
        q.second_forward(0, 0)
    for q in seqs:
        q.first_end()
    for q in seqs:
        q.second_forward(1, -1)
    for q in seqs:
        q.second_end(0, 0)
    for q in seqs:
        q.second_forward(2, 1)
    for q in seqs:
        q.second_end(1, -1)
    for q in seqs:
        q.second_forward(3, 2)
    for q in seqs:
        q.second_end(2, 1)
    for q in seqs:
        q.second_end(3, 2)
    order = [(0, 0), (-1, 0), (1, 0), (0, -1), (0, 1), (2, 0), (-1, -1), (-1, 1), (0, 2), (1, -1), (1, 1),
             (-1, 2), (2, -1), (2, 1), (1, 2), (2, 2)]
    for s in range(SEQS):
        q = seqs[s]
        for n, (a, b) in enumerate(order):
            r = out_ref.at[s, q.at(a, b) + 1 - 2 * c]
            rcopy(r, r, psend.at[s * 16 + n], precv.at[s * 16 + n], partner).wait_recv()
    for q in seqs:
        for d in q.sends:
            d.wait_send()


def gather_kv(keys, values):
    return pl.pallas_call(
        gather_kernel,
        out_shape=jax.ShapeDtypeStruct((SEQS, DEVS, ROWS, 2 * HD), BF16),
        in_specs=[pl.BlockSpec(memory_space=pltpu.VMEM)] * 2,
        out_specs=pl.BlockSpec(memory_space=pltpu.VMEM),
        scratch_shapes=[
            pltpu.SemaphoreType.DMA((40,)),
            pltpu.SemaphoreType.DMA((40,)),
            pltpu.SemaphoreType.DMA((32,)),
            pltpu.SemaphoreType.DMA((32,)),
        ],
        compiler_params=pltpu.CompilerParams(
            collective_id=0, has_side_effects=True, vmem_limit_bytes=16 * 2**20
        ),
        name="gather_kv",
    )(keys, values)


def attend_kernel(
    ids_ref, kv_ref, q_ref, g_ref, gate_ref, dq_ref, table_ref, acc, kvbuf, rows_buf, scores, packed
):
    s = pl.program_id(0)
    qb = pl.program_id(1)
    keys = TOPK * BLK
    nrow = HEADS * BLK

    @pl.when(qb == 0)
    def _():
        def clear(i, carry):
            acc[pl.ds(i * 6, 6)] = jnp.zeros((6, BLK, 2 * HD), F32)
            return carry

        lax.fori_loop(0, DEVS, clear, 0)

    block = lax.axis_index("kv") * BPD + qb
    base = (s * BPD + qb) * TOPK
    picked = [ids_ref[base + k] for k in range(TOPK)]
    for k in range(TOPK):
        kvbuf[k * BLK : (k + 1) * BLK] = kv_ref[0, picked[k]]

    lane = lax.broadcasted_iota(jnp.int32, (BLK, 2 * HD), 1)
    low = lane < HD
    for h in range(HEADS):
        pair = slice((h // 2) * 128, (h // 2) * 128 + 128)
        qv = q_ref[0, :, pair].astype(F32) * 0.125
        gate = jax.nn.sigmoid(gate_ref[0, :, h : h + 1])
        gv = gate * g_ref[0, :, pair].astype(F32)
        if h % 2 == 0:
            gv = pltpu.roll(gv, HD, 1)
        else:
            qv = pltpu.roll(qv, HD, 1)
        rows_buf[h * BLK : (h + 1) * BLK] = jnp.where(low, qv, 0.0).astype(BF16)
        rows_buf[nrow + h * BLK : nrow + (h + 1) * BLK] = jnp.where(low, 0.0, gv).astype(BF16)

    scores[...] = lax.dot_general(
        kvbuf[...], rows_buf[...], (((1,), (1,)), ((), ())), preferred_element_type=F32
    )
    qpos = block * BLK + lax.broadcasted_iota(jnp.int32, (BLK, nrow), 1) % BLK
    koff = lax.broadcasted_iota(jnp.int32, (BLK, nrow), 0)
    ahead = koff - qpos

    def masked(k):
        sc = scores[k * BLK : (k + 1) * BLK, :nrow]
        return jnp.where(ahead <= -(picked[k] * BLK), sc, NEG)

    top = None
    for k in range(TOPK):
        m = masked(k).reshape(8, 8, nrow)
        m = jnp.max(m, axis=0)
        top = m if top is None else jnp.maximum(top, m)
    top = jnp.max(top, axis=0, keepdims=True)
    total = jnp.zeros((8, nrow), F32)
    for k in range(TOPK):
        e = jnp.exp(masked(k) - top)
        scores[k * BLK : (k + 1) * BLK, :nrow] = e
        total = total + jnp.sum(e.reshape(8, 8, nrow), axis=0)
    inv = 1.0 / jnp.sum(total, axis=0, keepdims=True)
    dot = jnp.zeros((8, nrow), F32)
    for k in range(TOPK):
        rows = slice(k * BLK, (k + 1) * BLK)
        w = (scores[rows, :nrow] * inv).astype(BF16)
        packed[rows, nrow:] = w
        t = w.astype(F32) * scores[rows, nrow:]
        dot = dot + jnp.sum(t.reshape(8, 8, nrow), axis=0)
    row_dot = jnp.sum(dot, axis=0, keepdims=True)
    for k in range(TOPK):
        rows = slice(k * BLK, (k + 1) * BLK)
        ds = (scores[rows, :nrow] * inv) * (scores[rows, nrow:] - row_dot)
        packed[rows, :nrow] = ds.astype(BF16)

    pick = jnp.dot(packed[...], rows_buf[...], preferred_element_type=F32)
    for k in range(TOPK):
        acc[picked[k]] += pick[k * BLK : (k + 1) * BLK]
    dq_t = jnp.dot(kvbuf[...].T, packed[:, :nrow], preferred_element_type=F32)
    dq = (dq_t[:HD] * 0.125).T
    dq_ref[0] = jnp.concatenate([dq[h * BLK : (h + 1) * BLK] for h in range(HEADS)], axis=1).astype(BF16)

    @pl.when(qb == BPD - 1)
    def _():
        def put(i, carry):
            table_ref[0, pl.ds(i * 6, 6)] = acc[pl.ds(i * 6, 6)].astype(BF16)
            return carry

        lax.fori_loop(0, DEVS, put, 0)


def attend(ids, kv_all, queries, cotangent, gates):
    nblk = DEVS * BPD
    keys = TOPK * BLK
    nrow = HEADS * BLK
    return pl.pallas_call(
        attend_kernel,
        grid_spec=pltpu.PrefetchScalarGridSpec(
            num_scalar_prefetch=1,
            grid=(SEQS, BPD),
            in_specs=[
                pl.BlockSpec((1, nblk, BLK, 2 * HD), lambda s, q, ids: (s, 0, 0, 0)),
                pl.BlockSpec((1, BLK, HEADS * HD), lambda s, q, ids: (s, q, 0)),
                pl.BlockSpec((1, BLK, HEADS * HD), lambda s, q, ids: (s, q, 0)),
                pl.BlockSpec((1, BLK, HEADS), lambda s, q, ids: (s, q, 0)),
            ],
            out_specs=[
                pl.BlockSpec((1, BLK, HEADS * HD), lambda s, q, ids: (s, q, 0)),
                pl.BlockSpec((1, nblk, BLK, 2 * HD), lambda s, q, ids: (s, 0, 0, 0)),
            ],
            scratch_shapes=[
                pltpu.VMEM((nblk, BLK, 2 * HD), F32),
                pltpu.VMEM((keys, 2 * HD), BF16),
                pltpu.VMEM((2 * nrow, 2 * HD), BF16),
                pltpu.VMEM((keys, 2 * nrow), F32),
                pltpu.VMEM((keys, 2 * nrow), BF16),
            ],
        ),
        out_shape=[
            jax.ShapeDtypeStruct((SEQS, ROWS, HEADS * HD), BF16),
            jax.ShapeDtypeStruct((SEQS, nblk, BLK, 2 * HD), BF16),
        ],
        compiler_params=pltpu.CompilerParams(
            vmem_limit_bytes=44 * 2**20, dimension_semantics=("arbitrary", "arbitrary")
        ),
        name="attend",
    )(ids, kv_all.reshape(SEQS, nblk, BLK, 2 * HD), queries, cotangent, gates)


class Ring:
    def __init__(self, pos, plus, minus, bufs, ssem, rsem):
        self.pos, self.plus, self.minus = pos, plus, minus
        self.sb, self.rb = bufs
        self.ssem, self.rsem = ssem, rsem
        self.sends = []

    def copy(self, i, dev):
        return rcopy(self.sb.at[i], self.rb.at[i], self.ssem.at[i], self.rsem.at[i], dev)

    def send(self, i, dev, value):
        self.sb[i] = value.astype(BF16)
        d = self.copy(i, dev)
        d.start()
        self.sends.append(d)

    def got(self, i):
        self.copy(i, self.plus).wait_recv()
        return self.rb[i].astype(F32)

    def start(self, part):
        p = self.pos
        self.send(0, self.plus, part((p + 2) % 4, 0))
        self.send(1, self.minus, part((p + 2) % 4, 1))

    def near(self, part):
        p = self.pos
        self.send(3, self.plus, part((p + 1) % 4, 1))
        self.send(4, self.minus, part((p + 3) % 4, 0))

    def middle(self, part):
        p = self.pos
        self.send(2, self.plus, part((p + 1) % 4, 0) + self.got(0))
        self.send(5, self.minus, part((p + 3) % 4, 1) + self.got(1))

    def end(self, part):
        p = self.pos
        first = part(p, 0) + self.got(2) + self.got(4)
        second = part(p, 1) + self.got(3) + self.got(5)
        return first, second

    def drain(self):
        for d in self.sends:
            d.wait_send()


def reduce_kernel(
    table, x_in, kg_ref, vg_ref, wg_ref,
    mate, acc, sa0, ra0, sa1, ra1, sb0, rb0, sb1, rb1,
    vsend, vland, li_t, rhs, part_w, mate_w, acc_x, acc_y, sx, rx, sy, ry, sz, rz,
    s_mate, r_mate, s_ring, r_ring, s_x, r_x, s_w, r_w,
):
    kv, tp, z, y, c = place()

    def zy(z_, y_):
        return ((z_ % 4) * 8 + (y_ % 4) * 2 + c, tp)

    partner = (kv + 1 - 2 * c, tp)
    xs = [(kv, (tp + d) % 4) for d in (1, 2, 3)]
    yp, ym, zp, zm = zy(z, y + 1), zy(z, y + 3), zy(z + 1, y), zy(z + 3, y)
    entry_barrier([partner, yp, ym, zp, zm] + xs)
    other = 1 - c
    sends = []

    for g in (2, 1, 3, 0):
        for s in range(SEQS):
            if s == 0:
                src = table.at[s, :, (y + g) % 4, other]
                dst = mate.at[s, :, (y + g) % 4]
            else:
                src = table.at[s, (z + g) % 4, :, other]
                dst = mate.at[s, (z + g) % 4]
            d = rcopy(src, dst, s_mate.at[s * 4 + g], r_mate.at[s * 4 + g], partner)
            d.start()
            sends.append(d)

    def mate_ready(s, g):
        dst = mate.at[s, :, (y + g) % 4] if s == 0 else mate.at[s, (z + g) % 4]
        rcopy(dst, dst, s_mate.at[s * 4 + g], r_mate.at[s * 4 + g], partner).wait_recv()

    def first_part(s):
        def part(d, h):
            if s == 0:
                a, b = table[s, 2 * h : 2 * h + 2, d, c], mate[s, 2 * h : 2 * h + 2, d]
            else:
                a, b = table[s, d, 2 * h : 2 * h + 2, c], mate[s, d, 2 * h : 2 * h + 2]
            return a.astype(F32) + b.astype(F32)

        return part

    rings_a = [
        Ring(y, yp, ym, (sa0, ra0), s_ring.at[0], r_ring.at[0]),
        Ring(z, zp, zm, (sa1, ra1), s_ring.at[1], r_ring.at[1]),
    ]
    rings_b = [
        Ring(z, zp, zm, (sb0, rb0), s_ring.at[2], r_ring.at[2]),
        Ring(y, yp, ym, (sb1, rb1), s_ring.at[3], r_ring.at[3]),
    ]
    for s in range(SEQS):
        mate_ready(s, 2)
        rings_a[s].start(first_part(s))
    for s in range(SEQS):
        mate_ready(s, 1)
        mate_ready(s, 3)
        rings_a[s].near(first_part(s))
    for s in range(SEQS):
        rings_a[s].middle(first_part(s))

    def turn(i, carry):
        lo = pl.multiple_of(i * 512, 512)
        for s in range(SEQS):
            li_t[pl.ds(lo, 512), s * 96 : (s + 1) * 96] = x_in[s, :, pl.ds(lo, 512)].T
        return carry

    lax.fori_loop(0, 8, turn, 0)

    half = ROWS // 2

    def second_part(s):
        def part(d, h):
            return acc[s, d, h * half : (h + 1) * half]

        return part

    for s in range(SEQS):
        mate_ready(s, 0)
        first, second = rings_a[s].end(first_part(s))
        acc[s, 0:2] = first
        acc[s, 2:4] = second
        rings_b[s].start(second_part(s))
        rings_b[s].near(second_part(s))
    for s in range(SEQS):
        rings_b[s].middle(second_part(s))
    for s in range(SEQS):
        first, second = rings_b[s].end(second_part(s))
        for h, value in enumerate((first, second)):
            rows = slice(h * half, (h + 1) * half)
            value = value.astype(BF16)
            vsend[s, rows] = value
            kg_ref[s, rows] = value[:, :HD]
            vg_ref[s, rows] = value[:, HD:]

    quarter = ROWS // 4
    for n in range(3):
        to = (tp + n + 1) % 4
        lo = pl.multiple_of(to * quarter, quarter)
        d = rcopy(vsend.at[:, pl.ds(lo, quarter)], vland.at[tp], s_x.at[n], r_x.at[n], (kv, to))
        d.start()
        sends.append(d)
    vland[tp] = vsend[:, pl.ds(pl.multiple_of(tp * quarter, quarter), quarter)]
    for n in range(3):
        frm = (tp + 3 - n) % 4
        d = rcopy(vland.at[frm], vland.at[frm], s_x.at[n], r_x.at[n], (kv, frm))
        d.wait_recv()
    lane = lax.broadcasted_iota(jnp.int32, (quarter, 2 * HD), 1)
    for s in range(SEQS):
        for p in range(2):
            even = pltpu.roll(vland[2 * p, s].astype(F32), HD, 1)
            odd = vland[2 * p + 1, s].astype(F32)
            rhs[s * quarter : (s + 1) * quarter, p * 128 : (p + 1) * 128] = jnp.where(
                lane < HD, even, odd
            ).astype(BF16)

    def product(i, carry):
        lo = pl.multiple_of(i * 256, 256)
        w = jnp.dot(li_t[pl.ds(lo, 256)], rhs[...], preferred_element_type=F32)
        part_w[i] = w.reshape(2, 4, 32, 256).astype(BF16)
        return carry

    lax.fori_loop(0, 16, product, 0)
    d = rcopy(part_w.at[:, other], mate_w, s_w.at[0, 0], r_w.at[0, 0], partner)
    d.start()
    sends.append(d)
    d.wait_recv()

    def w_part(d, h):
        a = part_w[8 * h : 8 * h + 8, c, d]
        return a.astype(F32) + mate_w[8 * h : 8 * h + 8, d].astype(F32)

    ring_x = Ring(tp, xs[0], xs[2], (sx, rx), s_w.at[1], r_w.at[1])
    ring_x.start(w_part)
    ring_x.near(w_part)
    ring_x.middle(w_part)
    first, second = ring_x.end(w_part)
    acc_x[0:2] = first.reshape(2, 4, 32, 256)
    acc_x[2:4] = second.reshape(2, 4, 32, 256)

    def y_part(d, h):
        return acc_x[2 * h : 2 * h + 2, d]

    ring_y = Ring(y, yp, ym, (sy, ry), s_w.at[2], r_w.at[2])
    ring_y.start(y_part)
    ring_y.near(y_part)
    ring_y.middle(y_part)
    first, second = ring_y.end(y_part)
    acc_y[0:2] = first
    acc_y[2:4] = second

    def z_part(d, h):
        return acc_y[d, 16 * h : 16 * h + 16]

    ring_z = Ring(z, zp, zm, (sz, rz), s_w.at[3], r_w.at[3])
    ring_z.start(z_part)
    ring_z.near(z_part)
    ring_z.middle(z_part)
    first, second = ring_z.end(z_part)
    wg_ref[0:16] = first
    wg_ref[16:32] = second

    for d in sends:
        d.wait_send()
    for r in rings_a + rings_b + [ring_x, ring_y, ring_z]:
        r.drain()


def reduce_grads(table, layer_input):
    v = pltpu.VMEM
    return pl.pallas_call(
        reduce_kernel,
        out_shape=[
            jax.ShapeDtypeStruct((SEQS, ROWS, HD), BF16),
            jax.ShapeDtypeStruct((SEQS, ROWS, HD), BF16),
            jax.ShapeDtypeStruct((32, 256), F32),
        ],
        in_specs=[pl.BlockSpec(memory_space=v)] * 2,
        out_specs=[pl.BlockSpec(memory_space=v)] * 3,
        scratch_shapes=[
            v((SEQS, ZN, YN, ROWS, 2 * HD), BF16),
            v((SEQS, 4, ROWS, 2 * HD), F32),
            *[v((6, 2, ROWS, 2 * HD), BF16) for _ in range(4)],
            *[v((6, ROWS // 2, 2 * HD), BF16) for _ in range(4)],
            v((SEQS, ROWS, 2 * HD), BF16),
            v((4, SEQS, ROWS // 4, 2 * HD), BF16),
            v((4096, 192), BF16),
            v((192, 256), BF16),
            v((16, 2, 4, 32, 256), BF16),
            v((16, 4, 32, 256), BF16),
            v((4, 4, 32, 256), F32),
            v((4, 32, 256), F32),
            *[v((6, 8, 32, 256), BF16) for _ in range(2)],
            *[v((6, 2, 32, 256), BF16) for _ in range(2)],
            *[v((6, 16, 256), BF16) for _ in range(2)],
            pltpu.SemaphoreType.DMA((8,)),
            pltpu.SemaphoreType.DMA((8,)),
            pltpu.SemaphoreType.DMA((4, 6)),
            pltpu.SemaphoreType.DMA((4, 6)),
            pltpu.SemaphoreType.DMA((3,)),
            pltpu.SemaphoreType.DMA((3,)),
            pltpu.SemaphoreType.DMA((4, 6)),
            pltpu.SemaphoreType.DMA((4, 6)),
        ],
        compiler_params=pltpu.CompilerParams(
            collective_id=1, has_side_effects=True, vmem_limit_bytes=44 * 2**20
        ),
        name="reduce_grads",
    )(table.reshape(SEQS, ZN, YN, 2, ROWS, 2 * HD), layer_input)


def on_device(queries, key_states, value_states, cotangent, gate_logits, layer_input, chosen):
    kv_all = gather_kv(key_states, value_states)
    query_grad, table = attend(chosen.reshape(-1), kv_all, queries, cotangent, gate_logits)
    key_grad, value_grad, weight_grad = reduce_grads(table, layer_input)
    return query_grad, key_grad, value_grad, weight_grad


def solution(mesh):
    placed = (
        P(None, "kv", "tp"),
        P(None, "kv", "tp"),
        P(None, "kv", "tp"),
        P(None, "kv", "tp"),
        P(None, "kv", "tp"),
        P(None, ("kv", "tp"), None),
        P(None, "kv", "tp", None),
    )
    return jax.shard_map(
        on_device,
        mesh=mesh,
        in_specs=placed,
        out_specs=(P(None, "kv", "tp"), P(None, "kv", "tp"), P(None, "kv", "tp"), P(("kv", "tp"), None)),
        check_vma=False,
    )
```

```python
import functools

import jax
import jax.numpy as jnp
from jax import lax
from jax.experimental import pallas as pl
from jax.experimental.pallas import tpu as pltpu
from jax.sharding import PartitionSpec as P

BLK = 64
MESH = pl.DeviceIdType.MESH
F32 = jnp.float32
BF16 = jnp.bfloat16
SEQS = 2
BPD = 6
ROWS = BPD * BLK
ZN = 4
YN = 4
DEVS = ZN * YN * 2
HD = 64
HEADS = 4
TOPK = 16
NEG = -1e30


def place():
    kv = lax.axis_index("kv")
    tp = lax.axis_index("tp")
    z, y, c = kv // 8, (kv // 2) % 4, kv % 2
    return kv, tp, z, y, c


def rcopy(src, dst, ssem, rsem, device):
    return pltpu.make_async_remote_copy(
        src_ref=src, dst_ref=dst, send_sem=ssem, recv_sem=rsem, device_id=device, device_id_type=MESH
    )


def entry_barrier(peers):
    sem = pltpu.get_barrier_semaphore()
    for peer in peers:
        pl.semaphore_signal(sem, inc=1, device_id=peer, device_id_type=MESH)
    pl.semaphore_wait(sem, len(peers))


def gather_kernel(k_ref, v_ref, out_ref, ssem, rsem, psend, precv):
    kv, tp, z, y, c = place()

    def zy(z_, y_):
        return (z_ % 4) * 8 + (y_ % 4) * 2 + c

    for s in range(SEQS):
        out_ref[s, kv] = jnp.concatenate([k_ref[s], v_ref[s]], axis=0).T
    partner = (kv + 1 - 2 * c, tp)
    entry_barrier([(zy(z, y + 1), tp), (zy(z, y + 3), tp), (zy(z + 1, y), tp), (zy(z + 3, y), tp), partner])

    half = ROWS // 2

    class Seq:
        def __init__(self, s):
            self.s = s
            self.base = s * 20
            self.sends = []
            self.pcount = 0

        def at(self, a, b):
            return zy(z + b, y + a) if self.s == 0 else zy(z + a, y + b)

        def dev(self, a, b):
            return (self.at(a, b), tp)

        def ref(self, a, b, part):
            chunk = out_ref.at[self.s, self.at(a, b)]
            if part is None:
                return chunk
            return chunk.at[pl.ds(part * half, half)]

        def send(self, i, a, b, part, to):
            r = self.ref(a, b, part)
            d = rcopy(r, r, ssem.at[self.base + i], rsem.at[self.base + i], self.dev(*to))
            d.start()
            self.sends.append(d)

        def recv(self, i, a, b, part):
            r = self.ref(a, b, part)
            rcopy(r, r, ssem.at[self.base + i], rsem.at[self.base + i], self.dev(0, 0)).wait_recv()

        def share(self, a, b):
            i = self.s * 16 + self.pcount
            self.pcount += 1
            r = self.ref(a, b, None)
            d = rcopy(r, r, psend.at[i], precv.at[i], partner)
            d.start()
            self.sends.append(d)

        def first(self):
            self.send(0, 0, 0, None, (1, 0))
            self.send(1, 0, 0, None, (-1, 0))

        def own(self):
            self.second_start(0, 0)
            self.share(0, 0)

        def second_start(self, q, a):
            self.send(4 + 4 * q, a, 0, None, (0, 1))
            self.send(5 + 4 * q, a, 0, None, (0, -1))

        def second_forward(self, q, a):
            self.recv(4 + 4 * q, a, -1, None)
            self.send(6 + 4 * q, a, -1, 0, (0, 1))
            self.recv(5 + 4 * q, a, 1, None)
            self.send(7 + 4 * q, a, 1, 1, (0, -1))
            self.share(a, -1)
            self.share(a, 1)

        def second_end(self, q, a):
            self.recv(6 + 4 * q, a, 2, 0)
            self.recv(7 + 4 * q, a, 2, 1)
            self.share(a, 2)

        def first_forward(self):
            self.recv(0, -1, 0, None)
            self.send(2, -1, 0, 0, (1, 0))
            self.recv(1, 1, 0, None)
            self.send(3, 1, 0, 1, (-1, 0))
            self.second_start(1, -1)
            self.second_start(2, 1)
            self.share(-1, 0)
            self.share(1, 0)

        def first_end(self):
            self.recv(2, 2, 0, 0)
            self.recv(3, 2, 0, 1)
            self.second_start(3, 2)
            self.share(2, 0)

    seqs = [Seq(0), Seq(1)]
    for q in seqs:
        q.first()
    for q in seqs:
        q.own()
    for q in seqs:
        q.first_forward()
    for q in seqs:
        q.second_forward(0, 0)
    for q in seqs:
        q.first_end()
    for q in seqs:
        q.second_forward(1, -1)
    for q in seqs:
        q.second_end(0, 0)
    for q in seqs:
        q.second_forward(2, 1)
    for q in seqs:
        q.second_end(1, -1)
    for q in seqs:
        q.second_forward(3, 2)
    for q in seqs:
        q.second_end(2, 1)
    for q in seqs:
        q.second_end(3, 2)
    order = [(0, 0), (-1, 0), (1, 0), (0, -1), (0, 1), (2, 0), (-1, -1), (-1, 1), (0, 2), (1, -1), (1, 1),
             (-1, 2), (2, -1), (2, 1), (1, 2), (2, 2)]
    for s in range(SEQS):
        q = seqs[s]
        for n, (a, b) in enumerate(order):
            r = out_ref.at[s, q.at(a, b) + 1 - 2 * c]
            rcopy(r, r, psend.at[s * 16 + n], precv.at[s * 16 + n], partner).wait_recv()
    for q in seqs:
        for d in q.sends:
            d.wait_send()


def gather_kv(keys, values):
    return pl.pallas_call(
        gather_kernel,
        out_shape=jax.ShapeDtypeStruct((SEQS, DEVS, ROWS, 2 * HD), BF16),
        in_specs=[pl.BlockSpec(memory_space=pltpu.VMEM)] * 2,
        out_specs=pl.BlockSpec(memory_space=pltpu.VMEM),
        scratch_shapes=[
            pltpu.SemaphoreType.DMA((40,)),
            pltpu.SemaphoreType.DMA((40,)),
            pltpu.SemaphoreType.DMA((32,)),
            pltpu.SemaphoreType.DMA((32,)),
        ],
        compiler_params=pltpu.CompilerParams(
            collective_id=0, has_side_effects=True, vmem_limit_bytes=16 * 2**20
        ),
        name="gather_kv",
    )(keys, values)


def attend_kernel(
    ids_ref, kv_ref, q_ref, g_ref, gate_ref, dq_ref, table_ref, acc, kvbuf, rows_buf, scores, packed, gates_t
):
    s = pl.program_id(0)
    qb = pl.program_id(1)
    keys = TOPK * BLK
    nrow = HEADS * BLK

    @pl.when(qb == 0)
    def _():
        def clear(i, carry):
            acc[pl.ds(i * 6, 6)] = jnp.zeros((6, BLK, 2 * HD), F32)
            return carry

        lax.fori_loop(0, DEVS, clear, 0)
        gates_t[...] = jax.nn.sigmoid(gate_ref[s]).T

    block = lax.axis_index("kv") * BPD + qb
    picked = [ids_ref[s, qb, 0, k] for k in range(TOPK)]
    for k in range(TOPK):
        kvbuf[k * BLK : (k + 1) * BLK] = kv_ref[s, picked[k]]

    lane = lax.broadcasted_iota(jnp.int32, (BLK, 2 * HD), 1)
    low = lane < HD
    gates = gates_t[pl.ds(pl.multiple_of(qb * BLK, BLK), BLK)]
    for h in range(HEADS):
        pair = slice((h // 2) * 128, (h // 2) * 128 + 128)
        qv = q_ref[0, :, pair].astype(F32) * 0.125
        gate = gates[:, h : h + 1]
        gv = gate * g_ref[0, :, pair].astype(F32)
        if h % 2 == 0:
            gv = pltpu.roll(gv, HD, 1)
        else:
            qv = pltpu.roll(qv, HD, 1)
        rows_buf[h * BLK : (h + 1) * BLK] = jnp.where(low, qv, 0.0).astype(BF16)
        rows_buf[nrow + h * BLK : nrow + (h + 1) * BLK] = jnp.where(low, 0.0, gv).astype(BF16)

    scores[...] = lax.dot_general(
        kvbuf[...], rows_buf[...], (((1,), (1,)), ((), ())), preferred_element_type=F32
    )
    qpos = block * BLK + lax.broadcasted_iota(jnp.int32, (BLK, nrow), 1) % BLK
    koff = lax.broadcasted_iota(jnp.int32, (BLK, nrow), 0)
    ahead = koff - qpos

    def masked(k):
        sc = scores[k * BLK : (k + 1) * BLK, :nrow]
        return jnp.where(ahead <= -(picked[k] * BLK), sc, NEG)

    top = None
    for k in range(TOPK):
        m = masked(k).reshape(8, 8, nrow)
        m = jnp.max(m, axis=0)
        top = m if top is None else jnp.maximum(top, m)
    top = jnp.max(top, axis=0, keepdims=True)
    total = jnp.zeros((8, nrow), F32)
    for k in range(TOPK):
        e = jnp.exp(masked(k) - top)
        scores[k * BLK : (k + 1) * BLK, :nrow] = e
        total = total + jnp.sum(e.reshape(8, 8, nrow), axis=0)
    inv = 1.0 / jnp.sum(total, axis=0, keepdims=True)
    dot = jnp.zeros((8, nrow), F32)
    for k in range(TOPK):
        rows = slice(k * BLK, (k + 1) * BLK)
        w = (scores[rows, :nrow] * inv).astype(BF16)
        packed[rows, nrow:] = w
        t = w.astype(F32) * scores[rows, nrow:]
        dot = dot + jnp.sum(t.reshape(8, 8, nrow), axis=0)
    row_dot = jnp.sum(dot, axis=0, keepdims=True)
    for k in range(TOPK):
        rows = slice(k * BLK, (k + 1) * BLK)
        ds = (scores[rows, :nrow] * inv) * (scores[rows, nrow:] - row_dot)
        packed[rows, :nrow] = ds.astype(BF16)

    pick = jnp.dot(packed[...], rows_buf[...], preferred_element_type=F32)
    for k in range(TOPK):
        acc[picked[k]] += pick[k * BLK : (k + 1) * BLK]
    dq_t = jnp.dot(kvbuf[...].T, packed[:, :nrow], preferred_element_type=F32)
    dq = (dq_t[:HD] * 0.125).T
    dq_ref[0] = jnp.concatenate([dq[h * BLK : (h + 1) * BLK] for h in range(HEADS)], axis=1).astype(BF16)

    @pl.when(qb == BPD - 1)
    def _():
        def put(i, carry):
            table_ref[s, pl.ds(i * 6, 6)] = acc[pl.ds(i * 6, 6)].astype(BF16)
            return carry

        lax.fori_loop(0, DEVS, put, 0)


def attend(ids, kv_all, queries, cotangent, gates):
    nblk = DEVS * BPD
    keys = TOPK * BLK
    nrow = HEADS * BLK
    return pl.pallas_call(
        attend_kernel,
        grid_spec=pltpu.PrefetchScalarGridSpec(
            num_scalar_prefetch=1,
            grid=(SEQS, BPD),
            in_specs=[
                pl.BlockSpec(memory_space=pltpu.VMEM),
                pl.BlockSpec((1, BLK, HEADS * HD), lambda s, q, ids: (s, q, 0)),
                pl.BlockSpec((1, BLK, HEADS * HD), lambda s, q, ids: (s, q, 0)),
                pl.BlockSpec(memory_space=pltpu.VMEM),
            ],
            out_specs=[
                pl.BlockSpec((1, BLK, HEADS * HD), lambda s, q, ids: (s, q, 0)),
                pl.BlockSpec(memory_space=pltpu.VMEM),
            ],
            scratch_shapes=[
                pltpu.VMEM((nblk, BLK, 2 * HD), F32),
                pltpu.VMEM((keys, 2 * HD), BF16),
                pltpu.VMEM((2 * nrow, 2 * HD), BF16),
                pltpu.VMEM((keys, 2 * nrow), F32),
                pltpu.VMEM((keys, 2 * nrow), BF16),
                pltpu.VMEM((ROWS, HEADS), F32),
            ],
        ),
        out_shape=[
            jax.ShapeDtypeStruct((SEQS, ROWS, HEADS * HD), BF16),
            jax.ShapeDtypeStruct((SEQS, nblk, BLK, 2 * HD), BF16),
        ],
        compiler_params=pltpu.CompilerParams(
            vmem_limit_bytes=24 * 2**20, dimension_semantics=("arbitrary", "arbitrary")
        ),
        name="attend",
    )(ids, kv_all.reshape(SEQS, nblk, BLK, 2 * HD), queries, cotangent, gates)


class Ring:
    def __init__(self, pos, plus, minus, bufs, ssem, rsem):
        self.pos, self.plus, self.minus = pos, plus, minus
        self.sb, self.rb = bufs
        self.ssem, self.rsem = ssem, rsem
        self.sends = []

    def copy(self, i, dev):
        return rcopy(self.sb.at[i], self.rb.at[i], self.ssem.at[i], self.rsem.at[i], dev)

    def send(self, i, dev, value):
        self.sb[i] = value.astype(BF16)
        d = self.copy(i, dev)
        d.start()
        self.sends.append(d)

    def got(self, i):
        self.copy(i, self.plus).wait_recv()
        return self.rb[i].astype(F32)

    def start(self, part):
        p = self.pos
        self.send(0, self.plus, part((p + 2) % 4, 0))
        self.send(1, self.minus, part((p + 2) % 4, 1))

    def near(self, part):
        p = self.pos
        self.send(3, self.plus, part((p + 1) % 4, 1))
        self.send(4, self.minus, part((p + 3) % 4, 0))

    def middle(self, part):
        p = self.pos
        self.send(2, self.plus, part((p + 1) % 4, 0) + self.got(0))
        self.send(5, self.minus, part((p + 3) % 4, 1) + self.got(1))

    def end(self, part):
        p = self.pos
        first = part(p, 0) + self.got(2) + self.got(4)
        second = part(p, 1) + self.got(3) + self.got(5)
        return first, second

    def drain(self):
        for d in self.sends:
            d.wait_send()


def reduce_kernel(
    table, x_in, kg_ref, vg_ref, wg_ref,
    mate, acc, sa0, ra0, sa1, ra1, sb0, rb0, sb1, rb1,
    vsend, vland, li_t, rhs, part_w, mate_w, acc_x, wsend, wland, sx, rx,
    s_mate, r_mate, s_ring, r_ring, s_x, r_x, s_w, r_w, s_d, r_d,
):
    kv, tp, z, y, c = place()

    def zy(z_, y_):
        return ((z_ % 4) * 8 + (y_ % 4) * 2 + c, tp)

    partner = (kv + 1 - 2 * c, tp)
    xs = [(kv, (tp + d) % 4) for d in (1, 2, 3)]
    yp, ym, zp, zm = zy(z, y + 1), zy(z, y + 3), zy(z + 1, y), zy(z + 3, y)
    offsets = [(dz, dy) for dz in (2, 1, 3, 0) for dy in (2, 1, 3, 0)][:-1]
    entry_barrier([partner] + xs + [zy(z + dz, y + dy) for dz, dy in offsets])
    other = 1 - c
    sends = []

    for g in (2, 1, 3, 0):
        for s in range(SEQS):
            if s == 0:
                src = table.at[s, :, (y + g) % 4, other]
                dst = mate.at[s, :, (y + g) % 4]
            else:
                src = table.at[s, (z + g) % 4, :, other]
                dst = mate.at[s, (z + g) % 4]
            d = rcopy(src, dst, s_mate.at[s * 4 + g], r_mate.at[s * 4 + g], partner)
            d.start()
            sends.append(d)

    def mate_ready(s, g):
        dst = mate.at[s, :, (y + g) % 4] if s == 0 else mate.at[s, (z + g) % 4]
        rcopy(dst, dst, s_mate.at[s * 4 + g], r_mate.at[s * 4 + g], partner).wait_recv()

    def first_part(s):
        def part(d, h):
            if s == 0:
                a, b = table[s, 2 * h : 2 * h + 2, d, c], mate[s, 2 * h : 2 * h + 2, d]
            else:
                a, b = table[s, d, 2 * h : 2 * h + 2, c], mate[s, d, 2 * h : 2 * h + 2]
            return a.astype(F32) + b.astype(F32)

        return part

    rings_a = [
        Ring(y, yp, ym, (sa0, ra0), s_ring.at[0], r_ring.at[0]),
        Ring(z, zp, zm, (sa1, ra1), s_ring.at[1], r_ring.at[1]),
    ]
    rings_b = [
        Ring(z, zp, zm, (sb0, rb0), s_ring.at[2], r_ring.at[2]),
        Ring(y, yp, ym, (sb1, rb1), s_ring.at[3], r_ring.at[3]),
    ]
    for s in range(SEQS):
        mate_ready(s, 2)
        rings_a[s].start(first_part(s))
    for s in range(SEQS):
        mate_ready(s, 1)
        mate_ready(s, 3)
        rings_a[s].near(first_part(s))
    for s in range(SEQS):
        rings_a[s].middle(first_part(s))

    def turn(i, carry):
        lo = pl.multiple_of(i * 512, 512)
        for s in range(SEQS):
            li_t[pl.ds(lo, 512), s * 96 : (s + 1) * 96] = x_in[s, :, pl.ds(lo, 512)].T
        return carry

    lax.fori_loop(0, 8, turn, 0)

    half = ROWS // 2

    def second_part(s):
        def part(d, h):
            return acc[s, d, h * half : (h + 1) * half]

        return part

    for s in range(SEQS):
        mate_ready(s, 0)
        first, second = rings_a[s].end(first_part(s))
        acc[s, 0:2] = first
        acc[s, 2:4] = second
        rings_b[s].start(second_part(s))
        rings_b[s].near(second_part(s))
    for s in range(SEQS):
        rings_b[s].middle(second_part(s))
    for s in range(SEQS):
        first, second = rings_b[s].end(second_part(s))
        for h, value in enumerate((first, second)):
            rows = slice(h * half, (h + 1) * half)
            value = value.astype(BF16)
            vsend[s, rows] = value

    quarter = ROWS // 4
    for n in range(3):
        to = (tp + n + 1) % 4
        lo = pl.multiple_of(to * quarter, quarter)
        d = rcopy(vsend.at[:, pl.ds(lo, quarter)], vland.at[tp], s_x.at[n], r_x.at[n], (kv, to))
        d.start()
        sends.append(d)
    for s in range(SEQS):
        turned = vsend[s].T
        kg_ref[s] = turned[:HD]
        vg_ref[s] = turned[HD:]
    vland[tp] = vsend[:, pl.ds(pl.multiple_of(tp * quarter, quarter), quarter)]
    for n in range(3):
        frm = (tp + 3 - n) % 4
        d = rcopy(vland.at[frm], vland.at[frm], s_x.at[n], r_x.at[n], (kv, frm))
        d.wait_recv()
    lane = lax.broadcasted_iota(jnp.int32, (quarter, 2 * HD), 1)
    for s in range(SEQS):
        for p in range(2):
            even = pltpu.roll(vland[2 * p, s].astype(F32), HD, 1)
            odd = vland[2 * p + 1, s].astype(F32)
            rhs[s * quarter : (s + 1) * quarter, p * 128 : (p + 1) * 128] = jnp.where(
                lane < HD, even, odd
            ).astype(BF16)

    def product(i, carry):
        lo = pl.multiple_of(i * 256, 256)
        w = jnp.dot(li_t[pl.ds(lo, 256)], rhs[...], preferred_element_type=F32)
        part_w[i] = w.reshape(2, 4, 32, 256).astype(BF16)
        return carry

    pieces = []
    for n in range(4):
        lax.fori_loop(4 * n, 4 * n + 4, product, 0)
        d = rcopy(
            part_w.at[4 * n : 4 * n + 4, other], mate_w.at[4 * n : 4 * n + 4], s_w.at[0, n], r_w.at[0, n], partner
        )
        d.start()
        pieces.append(d)
        sends.append(d)
    for d in pieces:
        d.wait_recv()

    def w_part(d, h):
        a = part_w[8 * h : 8 * h + 8, c, d]
        return a.astype(F32) + mate_w[8 * h : 8 * h + 8, d].astype(F32)

    ring_x = Ring(tp, xs[0], xs[2], (sx, rx), s_w.at[1], r_w.at[1])
    ring_x.start(w_part)
    ring_x.near(w_part)
    ring_x.middle(w_part)
    first, second = ring_x.end(w_part)
    wsend[0:8] = first.astype(BF16)
    wsend[8:16] = second.astype(BF16)
    mine = zy(z, y)[0] // 2
    for n, (dz, dy) in enumerate(offsets):
        to = zy(z + dz, y + dy)
        d = rcopy(wsend.at[to[0] // 2], wland.at[mine], s_d.at[n], r_d.at[n], to)
        d.start()
        sends.append(d)
    acc_x[0:8] = first
    acc_x[8:16] = second
    total = acc_x[mine]
    for n, (dz, dy) in enumerate(offsets):
        frm = zy(z - dz, y - dy)
        slot = wland.at[frm[0] // 2]
        rcopy(slot, slot, s_d.at[n], r_d.at[n], frm).wait_recv()
        total = total + wland[frm[0] // 2].astype(F32)
    wg_ref[...] = total

    for d in sends:
        d.wait_send()
    for r in rings_a + rings_b + [ring_x]:
        r.drain()


def reduce_grads(table, layer_input):
    v = pltpu.VMEM
    return pl.pallas_call(
        reduce_kernel,
        out_shape=[
            jax.ShapeDtypeStruct((SEQS, HD, ROWS), BF16),
            jax.ShapeDtypeStruct((SEQS, HD, ROWS), BF16),
            jax.ShapeDtypeStruct((32, 256), F32),
        ],
        in_specs=[pl.BlockSpec(memory_space=v)] * 2,
        out_specs=[pl.BlockSpec(memory_space=v)] * 3,
        scratch_shapes=[
            v((SEQS, ZN, YN, ROWS, 2 * HD), BF16),
            v((SEQS, 4, ROWS, 2 * HD), F32),
            *[v((6, 2, ROWS, 2 * HD), BF16) for _ in range(4)],
            *[v((6, ROWS // 2, 2 * HD), BF16) for _ in range(4)],
            v((SEQS, ROWS, 2 * HD), BF16),
            v((4, SEQS, ROWS // 4, 2 * HD), BF16),
            v((4096, 192), BF16),
            v((192, 256), BF16),
            v((16, 2, 4, 32, 256), BF16),
            v((16, 4, 32, 256), BF16),
            v((16, 32, 256), F32),
            v((16, 32, 256), BF16),
            v((16, 32, 256), BF16),
            *[v((6, 8, 32, 256), BF16) for _ in range(2)],
            pltpu.SemaphoreType.DMA((8,)),
            pltpu.SemaphoreType.DMA((8,)),
            pltpu.SemaphoreType.DMA((4, 6)),
            pltpu.SemaphoreType.DMA((4, 6)),
            pltpu.SemaphoreType.DMA((3,)),
            pltpu.SemaphoreType.DMA((3,)),
            pltpu.SemaphoreType.DMA((2, 6)),
            pltpu.SemaphoreType.DMA((2, 6)),
            pltpu.SemaphoreType.DMA((15,)),
            pltpu.SemaphoreType.DMA((15,)),
        ],
        compiler_params=pltpu.CompilerParams(
            collective_id=1, has_side_effects=True, vmem_limit_bytes=44 * 2**20
        ),
        name="reduce_grads",
    )(table.reshape(SEQS, ZN, YN, 2, ROWS, 2 * HD), layer_input)


def on_device(queries, key_states, value_states, cotangent, gate_logits, layer_input, chosen):
    def turned(a):
        return jnp.swapaxes(a, 1, 2)

    kv_all = gather_kv(turned(key_states), turned(value_states))
    query_grad, table = attend(chosen, kv_all, queries, cotangent, turned(gate_logits))
    key_grad, value_grad, weight_grad = reduce_grads(table, layer_input)
    return query_grad, turned(key_grad), turned(value_grad), weight_grad


def solution(mesh):
    placed = (
        P(None, "kv", "tp"),
        P(None, "kv", "tp"),
        P(None, "kv", "tp"),
        P(None, "kv", "tp"),
        P(None, "kv", "tp"),
        P(None, ("kv", "tp"), None),
        P(None, "kv", "tp", None),
    )
    return jax.shard_map(
        on_device,
        mesh=mesh,
        in_specs=placed,
        out_specs=(P(None, "kv", "tp"), P(None, "kv", "tp"), P(None, "kv", "tp"), P(("kv", "tp"), None)),
        check_vma=False,
    )
```

```python
import jax
import jax.numpy as jnp
from jax import lax
from jax.experimental import pallas as pl
from jax.experimental.pallas import tpu as pltpu
from jax.sharding import PartitionSpec as P

BLK = 64
MESH = pl.DeviceIdType.MESH
F32 = jnp.float32
BF16 = jnp.bfloat16
SEQS = 2
BPD = 6
ROWS = BPD * BLK
ZN = 4
YN = 4
DEVS = ZN * YN * 2
HD = 64
HEADS = 4
TOPK = 16
NEG = -1e30
HALF = ROWS // 2
QUART = ROWS // 4


def place():
    kv = lax.axis_index("kv")
    tp = lax.axis_index("tp")
    z, y, c = kv // 8, (kv // 2) % 4, kv % 2
    return kv, tp, z, y, c


def rcopy(src, dst, ssem, rsem, device):
    return pltpu.make_async_remote_copy(
        src_ref=src, dst_ref=dst, send_sem=ssem, recv_sem=rsem, device_id=device, device_id_type=MESH
    )


def entry_barrier(peers):
    sem = pltpu.get_barrier_semaphore()
    for peer in peers:
        pl.semaphore_signal(sem, inc=1, device_id=peer, device_id_type=MESH)
    pl.semaphore_wait(sem, len(peers))


class Ring:
    def __init__(self, pos, plus, minus, bufs, ssem, rsem):
        self.pos, self.plus, self.minus = pos, plus, minus
        self.sb, self.rb = bufs
        self.ssem, self.rsem = ssem, rsem
        self.used = []

    def copy(self, i, dev):
        return rcopy(self.sb.at[i], self.rb.at[i], self.ssem.at[i], self.rsem.at[i], dev)

    def send(self, i, dev, value):
        self.sb[i] = value.astype(BF16)
        self.copy(i, dev).start()
        self.used.append((i, dev))

    def got(self, i):
        self.copy(i, self.plus).wait_recv()
        return self.rb[i].astype(F32)

    def start(self, part):
        p = self.pos
        self.send(0, self.plus, part((p + 2) % 4, 0))
        self.send(1, self.minus, part((p + 2) % 4, 1))

    def near(self, part):
        p = self.pos
        self.send(3, self.plus, part((p + 1) % 4, 1))
        self.send(4, self.minus, part((p + 3) % 4, 0))

    def middle(self, part):
        p = self.pos
        self.send(2, self.plus, part((p + 1) % 4, 0) + self.got(0))
        self.send(5, self.minus, part((p + 3) % 4, 1) + self.got(1))

    def end(self, part):
        p = self.pos
        first = part(p, 0) + self.got(2) + self.got(4)
        second = part(p, 1) + self.got(3) + self.got(5)
        return first, second

    def drain(self):
        for i, dev in self.used:
            self.copy(i, dev).wait_send()


class Gather:
    def __init__(self, h, kv_ref, where, ssem, rsem, psend, precv):
        self.h, self.kv_ref, self.where = h, kv_ref, where
        self.ssem, self.rsem, self.psend, self.precv = ssem, rsem, psend, precv
        self.kv, self.tp, self.z, self.y, self.c = where
        self.partner = (self.kv + 1 - 2 * self.c, self.tp)
        self.sends = []
        self.shares = []

    def at(self, a, b):
        dz, dy = (b, a) if self.h == 0 else (a, b)
        return ((self.z + dz) % 4) * 8 + ((self.y + dy) % 4) * 2 + self.c

    def ref(self, a, b, part, shift=0):
        lo, n = self.h * HALF, HALF
        if part is not None:
            lo, n = lo + part * QUART, QUART
        return self.kv_ref.at[self.at(a, b) + shift, pl.ds(lo, n)]

    def copy(self, i, a, b, part, to):
        r = self.ref(a, b, part)
        return rcopy(r, r, self.ssem.at[i], self.rsem.at[i], (self.at(*to), self.tp))

    def send(self, *args):
        self.copy(*args).start()
        self.sends.append(args)

    def recv(self, i, a, b, part):
        self.copy(i, a, b, part, (1, 0)).wait_recv()

    def share_copy(self, n, a, b, shift=0):
        r = self.ref(a, b, None, shift)
        return rcopy(r, r, self.psend.at[n], self.precv.at[n], self.partner)

    def share(self, a, b):
        n = len(self.shares)
        self.shares.append((a, b))
        self.share_copy(n, a, b).start()

    def shared(self):
        for n, (a, b) in enumerate(self.shares):
            self.share_copy(n, a, b, 1 - 2 * self.c).wait_recv()

    def drain(self):
        for args in self.sends:
            self.copy(*args).wait_send()
        for n, (a, b) in enumerate(self.shares):
            self.share_copy(n, a, b).wait_send()

    def first(self):
        self.send(0, 0, 0, None, (1, 0))
        self.send(1, 0, 0, None, (-1, 0))

    def own(self):
        self.second_start(0, 0)
        self.share(0, 0)

    def second_start(self, q, a):
        self.send(4 + 4 * q, a, 0, None, (0, 1))
        self.send(5 + 4 * q, a, 0, None, (0, -1))

    def second_forward(self, q, a):
        self.recv(4 + 4 * q, a, -1, None)
        self.send(6 + 4 * q, a, -1, 0, (0, 1))
        self.recv(5 + 4 * q, a, 1, None)
        self.send(7 + 4 * q, a, 1, 1, (0, -1))
        self.share(a, -1)
        self.share(a, 1)

    def second_end(self, q, a):
        self.recv(6 + 4 * q, a, 2, 0)
        self.recv(7 + 4 * q, a, 2, 1)
        self.share(a, 2)

    def first_forward(self):
        self.recv(0, -1, 0, None)
        self.send(2, -1, 0, 0, (1, 0))
        self.second_start(1, -1)
        self.recv(1, 1, 0, None)
        self.send(3, 1, 0, 1, (-1, 0))
        self.second_start(2, 1)
        self.share(-1, 0)
        self.share(1, 0)

    def first_end(self):
        self.recv(2, 2, 0, 0)
        self.recv(3, 2, 0, 1)
        self.second_start(3, 2)
        self.share(2, 0)


def gather_steps(pair):
    def each(*calls):
        def run():
            for name, *args in calls:
                for g in pair:
                    getattr(g, name)(*args)

        return run

    return [
        each(("first",), ("own",)),
        each(("first_forward",)),
        each(("second_forward", 0, 0), ("first_end",)),
        each(("second_forward", 1, -1), ("second_forward", 2, 1), ("second_end", 0, 0)),
        each(("second_forward", 3, 2), ("second_end", 1, -1), ("second_end", 2, 1)),
        each(("second_end", 3, 2), ("shared",)),
    ]


class Reduce:
    def __init__(self, table, mate, acc, abufs, bbufs, where, s_mate, r_mate, s_ring, r_ring):
        self.table, self.mate, self.acc = table, mate, acc
        self.kv, self.tp, self.z, self.y, self.c = where
        self.s_mate, self.r_mate = s_mate, r_mate
        kv, tp, z, y, c = where
        self.partner = (kv + 1 - 2 * c, tp)

        def to(dz, dy):
            return (((z + dz) % 4) * 8 + ((y + dy) % 4) * 2 + c, tp)

        ydir = (y, to(0, 1), to(0, 3))
        zdir = (z, to(1, 0), to(3, 0))
        self.ra = [
            Ring(*(ydir if h == 0 else zdir), [b.at[h] for b in abufs], s_ring.at[h], r_ring.at[h])
            for h in range(2)
        ]
        self.rb = [
            Ring(*(zdir if h == 0 else ydir), [b.at[h] for b in bbufs], s_ring.at[2 + h], r_ring.at[2 + h])
            for h in range(2)
        ]

    def mate_copy(self, h, g):
        rows = pl.ds(h * HALF, HALF)
        if h == 0:
            src = self.table.at[:, (self.y + g) % 4, 1 - self.c, rows]
            dst = self.mate.at[:, (self.y + g) % 4, rows]
        else:
            src = self.table.at[(self.z + g) % 4, :, 1 - self.c, rows]
            dst = self.mate.at[(self.z + g) % 4, :, rows]
        return rcopy(src, dst, self.s_mate.at[h * 4 + g], self.r_mate.at[h * 4 + g], self.partner)

    def share(self):
        for g in (2, 1, 3, 0):
            for h in range(2):
                self.mate_copy(h, g).start()

    def part_a(self, h):
        rows = slice(h * HALF, (h + 1) * HALF)

        def part(d, q):
            if h == 0:
                a = self.table[2 * q : 2 * q + 2, d, self.c, rows]
                b = self.mate[2 * q : 2 * q + 2, d, rows]
            else:
                a = self.table[d, 2 * q : 2 * q + 2, self.c, rows]
                b = self.mate[d, 2 * q : 2 * q + 2, rows]
            return a.astype(F32) + b.astype(F32)

        return part

    def part_b(self, h):
        def part(d, q):
            return self.acc[h, d, q * QUART : (q + 1) * QUART]

        return part

    def begin(self):
        for h in range(2):
            self.mate_copy(h, 2).wait_recv()
            self.ra[h].start(self.part_a(h))
        for h in range(2):
            self.mate_copy(h, 1).wait_recv()
            self.mate_copy(h, 3).wait_recv()
            self.ra[h].near(self.part_a(h))

    def middle(self):
        for h in range(2):
            self.ra[h].middle(self.part_a(h))

    def turn(self):
        for h in range(2):
            self.mate_copy(h, 0).wait_recv()
            first, second = self.ra[h].end(self.part_a(h))
            self.acc[h, 0:2] = first
            self.acc[h, 2:4] = second
            self.rb[h].start(self.part_b(h))
            self.rb[h].near(self.part_b(h))

    def middle_b(self):
        for h in range(2):
            self.rb[h].middle(self.part_b(h))

    def finish(self, out):
        for h in range(2):
            for q, value in enumerate(self.rb[h].end(self.part_b(h))):
                lo = h * HALF + q * QUART
                out[lo : lo + QUART] = value

    def drain(self):
        for h in range(2):
            for g in range(4):
                self.mate_copy(h, g).wait_send()
            self.ra[h].drain()
            self.rb[h].drain()


def whole_kernel(
    ids_ref, inv_ref, k_ref, v_ref, gate_ref, q_hbm, g_hbm, x_hbm,
    dq_ref, kg_ref, vg_ref, wg_ref,
    kv0, kv1, table0, table1, mate0, mate1, acc0, acc1, sa0, ra0, sa1, ra1, sb0, rb0, sb1, rb1,
    q_in, g_in, x_in, gates_t, rows_all, kvbuf, scores, packed, picks, final,
    li_t, li_in, vsend, vland, rhs, w_out, w_own, w_mate, wsend, wland,
    l_sem, ag_s, ag_r, agp_s, agp_r, s_mate, r_mate, s_ring, r_ring, s_li, r_li, s_x, r_x, s_w, r_w, s_d, r_d,
):
    where = place()
    kv, tp, z, y, c = where
    other = 1 - c
    nrow = HEADS * BLK

    def zy(z_, y_):
        return ((z_ % 4) * 8 + (y_ % 4) * 2 + c, tp)

    partner = (kv + 1 - 2 * c, tp)
    xs = [(kv, (tp + d) % 4) for d in (1, 2, 3)]
    offsets = [(dz, dy) for dz in (2, 1, 3, 0) for dy in (2, 1, 3, 0)][:-1]
    kvs, tables = (kv0, kv1), (table0, table1)

    local = [
        pltpu.make_async_copy(x_hbm, x_in, l_sem.at[0]),
        pltpu.make_async_copy(q_hbm, q_in, l_sem.at[1]),
        pltpu.make_async_copy(g_hbm, g_in, l_sem.at[2]),
    ]
    for d in local:
        d.start()
    for s in range(SEQS):
        kvs[s][kv] = jnp.concatenate([k_ref[s], v_ref[s]], axis=0).T
    entry_barrier([partner] + xs + [zy(z + dz, y + dy) for dz, dy in offsets])

    gathers = [
        [Gather(h, kvs[s], where, ag_s.at[s, h], ag_r.at[s, h], agp_s.at[s, h], agp_r.at[s, h]) for h in range(2)]
        for s in range(SEQS)
    ]
    steps = [gather_steps(pair) for pair in gathers]
    reduces = [
        Reduce(
            tables[s], (mate0, mate1)[s], (acc0, acc1)[s],
            ((sa0, ra0), (sa1, ra1))[s], ((sb0, rb0), (sb1, rb1))[s],
            where, s_mate.at[s], r_mate.at[s], s_ring.at[s], r_ring.at[s],
        )
        for s in range(SEQS)
    ]

    def turn_input(i, carry):
        lo = pl.multiple_of(i * 512, 512)
        for s in range(SEQS):
            t = x_in[s, :, pl.ds(lo, 512)].T.reshape(2, 2, 4, 32, 96)
            for n in range(4):
                li_t[n, pl.ds(i * 2, 2), :, :, s * 96 : (s + 1) * 96] = t[:, :, n]
        return carry

    def li_copy(n):
        to = (tp + n + 1) % 4
        return rcopy(li_t.at[to], li_in.at[tp], s_li.at[n], r_li.at[n], (kv, to))

    def prepare(s, qb):
        lane = lax.broadcasted_iota(jnp.int32, (BLK, 2 * HD), 1)
        low = lane < HD
        rows = pl.ds(pl.multiple_of(qb * BLK, BLK), BLK)
        gates = gates_t[s, rows]
        at = s * BPD + qb
        for h in range(HEADS):
            pair = slice((h // 2) * 128, (h // 2) * 128 + 128)
            qv = q_in[s, rows, pair].astype(F32) * 0.125
            gv = gates[:, h : h + 1] * g_in[s, rows, pair].astype(F32)
            if h % 2 == 0:
                gv = pltpu.roll(gv, HD, 1)
            else:
                qv = pltpu.roll(qv, HD, 1)
            rows_all[at, h * BLK : (h + 1) * BLK] = jnp.where(low, qv, 0.0).astype(BF16)
            rows_all[at, nrow + h * BLK : nrow + (h + 1) * BLK] = jnp.where(low, 0.0, gv).astype(BF16)

    def attend(s, qb):
        at = s * BPD + qb
        kv_ref = kvs[s]
        block = kv * BPD + qb
        picked = [ids_ref[s, qb, 0, k] for k in range(TOPK)]
        for k in range(TOPK):
            kvbuf[k * BLK : (k + 1) * BLK] = kv_ref[picked[k] // BPD, pl.ds((picked[k] % BPD) * BLK, BLK)]
        scores[...] = lax.dot_general(
            kvbuf[...], rows_all[at], (((1,), (1,)), ((), ())), preferred_element_type=F32
        )
        qpos = block * BLK + lax.broadcasted_iota(jnp.int32, (BLK, nrow), 1) % BLK
        ahead = lax.broadcasted_iota(jnp.int32, (BLK, nrow), 0) - qpos

        def masked(k):
            sc = scores[k * BLK : (k + 1) * BLK, :nrow]
            return jnp.where(ahead <= -(picked[k] * BLK), sc, NEG)

        top = None
        for k in range(TOPK):
            m = jnp.max(masked(k).reshape(8, 8, nrow), axis=0)
            top = m if top is None else jnp.maximum(top, m)
        top = jnp.max(top, axis=0, keepdims=True)
        total = jnp.zeros((8, nrow), F32)
        for k in range(TOPK):
            e = jnp.exp(masked(k) - top)
            scores[k * BLK : (k + 1) * BLK, :nrow] = e
            total = total + jnp.sum(e.reshape(8, 8, nrow), axis=0)
        scale = 1.0 / jnp.sum(total, axis=0, keepdims=True)
        dot = jnp.zeros((8, nrow), F32)
        for k in range(TOPK):
            rows = slice(k * BLK, (k + 1) * BLK)
            w = (scores[rows, :nrow] * scale).astype(BF16)
            packed[rows, nrow:] = w
            t = w.astype(F32) * scores[rows, nrow:]
            dot = dot + jnp.sum(t.reshape(8, 8, nrow), axis=0)
        row_dot = jnp.sum(dot, axis=0, keepdims=True)
        for k in range(TOPK):
            rows = slice(k * BLK, (k + 1) * BLK)
            ds = (scores[rows, :nrow] * scale) * (scores[rows, nrow:] - row_dot)
            packed[rows, :nrow] = ds.astype(BF16)
        pick = jnp.dot(packed[...], rows_all[at], preferred_element_type=F32)
        picks[pl.ds(qb * TOPK, TOPK)] = pick.reshape(TOPK, BLK, 2 * HD)
        dq_t = jnp.dot(kvbuf[...].T, packed[:, :nrow], preferred_element_type=F32)
        dq = (dq_t[:HD] * 0.125).T
        dq_ref[s, pl.ds(pl.multiple_of(qb * BLK, BLK), BLK)] = jnp.concatenate(
            [dq[h * BLK : (h + 1) * BLK] for h in range(HEADS)], axis=1
        ).astype(BF16)

    def collect(s):
        def one(j, carry):
            for b in range(BPD):
                total = picks[inv_ref[s, 0, j * BPD + b]]
                for q in range(1, BPD):
                    total = total + picks[inv_ref[s, q, j * BPD + b]]
                tables[s][j // 8, (j // 2) % 4, j % 2, b * BLK : (b + 1) * BLK] = total.astype(BF16)
            return carry

        lax.fori_loop(0, DEVS, one, 0)

    quarter = ROWS // 4

    def x_copy(s, n):
        to = (tp + n + 1) % 4
        return rcopy(vsend.at[s], vland.at[s, tp], s_x.at[s, n], r_x.at[s, n], (kv, to))

    def finish(s):
        reduces[s].finish(final)
        lane = lax.broadcasted_iota(jnp.int32, (HALF, 2 * HD), 1)
        low = pltpu.roll(final[0:HALF].astype(BF16).astype(F32), HD, 1)
        value = jnp.where(lane < HD, low, final[HALF:]).astype(BF16)
        vsend[s] = value
        vland[s, tp] = value
        for n in (1, 0, 2):
            x_copy(s, n).start()
        turned = final[...].T
        kg_ref[s] = turned[:HD].astype(BF16)
        vg_ref[s] = turned[HD:].astype(BF16)

    def landed(s):
        for n in range(3):
            frm = (tp + 3 - n) % 4
            slot = vland.at[s, frm]
            rcopy(slot, slot, s_x.at[s, n], r_x.at[s, n], (kv, frm)).wait_recv()
        lane = lax.broadcasted_iota(jnp.int32, (quarter, 2 * HD), 1)
        for t in range(4):
            rows = slice((t % 2) * quarter, (t % 2 + 1) * quarter)
            for p in range(2):
                even = vland[s, 2 * p, rows].astype(F32)
                odd = vland[s, 2 * p + 1, rows].astype(F32)
                if t < 2:
                    odd = pltpu.roll(odd, HD, 1)
                else:
                    even = pltpu.roll(even, HD, 1)
                rhs[t, s * quarter : (s + 1) * quarter, p * 128 : (p + 1) * 128] = jnp.where(
                    lane < HD, even, odd
                ).astype(BF16)

    steps[0][0]()
    local[0].wait()
    lax.fori_loop(0, 8, turn_input, 0)
    for n in (1, 0, 2):
        li_copy(n).start()
    steps[0][1]()
    local[1].wait()
    local[2].wait()
    for s in range(SEQS):
        gates_t[s] = jax.nn.sigmoid(gate_ref[s]).T
    picks[BPD * TOPK] = jnp.zeros((BLK, 2 * HD), F32)
    for n in range(2, 5):
        steps[0][n]()

        def some(i, carry, n=n):
            at = (n - 2) * 4 + i
            prepare(at // BPD, at % BPD)
            return carry

        lax.fori_loop(0, 4, some, 0)
    steps[0][5]()

    def between(n, step):
        def at(qb):
            @pl.when(qb == n)
            def _():
                step()

        return at

    steps[1][0]()
    marks = [between(n, steps[1][n + 1]) for n in range(5)]

    def attend0(qb, carry):
        attend(0, qb)
        for mark in marks:
            mark(qb)
        return carry

    lax.fori_loop(0, BPD, attend0, 0)
    collect(0)
    reduces[0].share()

    late = [reduces[0].begin, reduces[0].middle, reduces[0].turn, reduces[0].middle_b, lambda: finish(0)]
    marks1 = [between(n, late[n]) for n in range(5)]

    def attend1(qb, carry):
        attend(1, qb)
        for mark in marks1:
            mark(qb)
        return carry

    lax.fori_loop(0, BPD, attend1, 0)
    collect(1)
    reduces[1].share()
    landed(0)
    reduces[1].begin()
    reduces[1].middle()
    reduces[1].turn()
    reduces[1].middle_b()
    finish(1)
    for n in range(3):
        frm = (tp + 3 - n) % 4
        rcopy(li_in.at[frm], li_in.at[frm], s_li.at[n], r_li.at[n], (kv, frm)).wait_recv()
    mine_li = pltpu.make_async_copy(li_t.at[tp], li_in.at[tp], l_sem.at[3])
    mine_li.start()
    mine_li.wait()
    landed(1)

    def product(side, i):
        total = None
        for t in range(4):
            a = li_in[t, pl.ds(i * 4, 4), side].reshape(128, 192)
            p = jnp.dot(a, rhs[t], preferred_element_type=F32)
            total = p if total is None else total + p
        return total.reshape(4, 32, 256)

    def for_mate(i, carry):
        w_out[pl.ds(i * 4, 4)] = product(other, i).astype(BF16)
        return carry

    def for_self(i, carry):
        w_own[pl.ds(i * 4, 4)] = product(c, i)
        return carry

    lax.fori_loop(0, 4, for_mate, 0)
    w_copy = rcopy(w_out, w_mate, s_w.at[0], r_w.at[0], partner)
    w_copy.start()
    lax.fori_loop(0, 4, for_self, 0)
    w_copy.wait_recv()
    w_own[...] = w_own[...] + w_mate[...].astype(F32)
    wsend[...] = w_own[...].astype(BF16)
    mine = kv // 2

    def d_copy(n):
        dz, dy = offsets[n]
        to = zy(z + dz, y + dy)
        return rcopy(wsend.at[to[0] // 2], wland.at[mine], s_d.at[n], r_d.at[n], to)

    for n in range(len(offsets)):
        d_copy(n).start()
    total = w_own[mine]
    for n, (dz, dy) in enumerate(offsets):
        frm = zy(z - dz, y - dy)
        slot = wland.at[frm[0] // 2]
        rcopy(slot, slot, s_d.at[n], r_d.at[n], frm).wait_recv()
        total = total + wland[frm[0] // 2].astype(F32)
    wg_ref[...] = total

    for pair in gathers:
        for g in pair:
            g.drain()
    for r in reduces:
        r.drain()
    for n in range(3):
        li_copy(n).wait_send()
        for s in range(SEQS):
            x_copy(s, n).wait_send()
    w_copy.wait_send()
    for n in range(len(offsets)):
        d_copy(n).wait_send()


def whole(chosen, inverse, keys, values, gates, queries, cotangent, layer_input):
    v = pltpu.VMEM
    dma = pltpu.SemaphoreType.DMA
    wide = 2 * HD
    anywhere = pl.BlockSpec(memory_space=pl.ANY)
    onchip = pl.BlockSpec(memory_space=v)
    smem = pl.BlockSpec(memory_space=pltpu.SMEM)
    keys_n = TOPK * BLK
    nrow = HEADS * BLK
    return pl.pallas_call(
        whole_kernel,
        out_shape=[
            jax.ShapeDtypeStruct((SEQS, ROWS, HEADS * HD), BF16),
            jax.ShapeDtypeStruct((SEQS, HD, ROWS), BF16),
            jax.ShapeDtypeStruct((SEQS, HD, ROWS), BF16),
            jax.ShapeDtypeStruct((32, 256), F32),
        ],
        in_specs=[smem, smem, onchip, onchip, onchip, anywhere, anywhere, anywhere],
        out_specs=[onchip] * 4,
        scratch_shapes=[
            *[v((DEVS, ROWS, wide), BF16) for _ in range(2)],
            *[v((ZN, YN, 2, ROWS, wide), BF16) for _ in range(2)],
            *[v((ZN, YN, ROWS, wide), BF16) for _ in range(2)],
            *[v((2, 4, HALF, wide), F32) for _ in range(2)],
            *[v((2, 6, 2, HALF, wide), BF16) for _ in range(4)],
            *[v((2, 6, QUART, wide), BF16) for _ in range(4)],
            v((SEQS, ROWS, HEADS * HD), BF16),
            v((SEQS, ROWS, HEADS * HD), BF16),
            v((SEQS, ROWS // 4, 4096), BF16),
            v((SEQS, ROWS, HEADS), F32),
            v((SEQS * BPD, 2 * nrow, wide), BF16),
            v((keys_n, wide), BF16),
            v((keys_n, 2 * nrow), F32),
            v((keys_n, 2 * nrow), BF16),
            v((BPD * TOPK + 1, BLK, wide), F32),
            v((ROWS, wide), F32),
            v((4, 16, 2, 32, 192), BF16),
            v((4, 16, 2, 32, 192), BF16),
            v((SEQS, HALF, wide), BF16),
            v((SEQS, 4, HALF, wide), BF16),
            v((4, 192, 256), BF16),
            v((16, 32, 256), BF16),
            v((16, 32, 256), F32),
            v((16, 32, 256), BF16),
            v((16, 32, 256), BF16),
            v((16, 32, 256), BF16),
            dma((4,)),
            *[dma((2, 2, 20)) for _ in range(2)],
            *[dma((2, 2, 16)) for _ in range(2)],
            *[dma((2, 8)) for _ in range(2)],
            *[dma((2, 4, 6)) for _ in range(2)],
            *[dma((3,)) for _ in range(2)],
            *[dma((2, 3)) for _ in range(2)],
            *[dma((1,)) for _ in range(2)],
            *[dma((15,)) for _ in range(2)],
        ],
        compiler_params=pltpu.CompilerParams(
            collective_id=0, has_side_effects=True, vmem_limit_bytes=58 * 2**20
        ),
        name="whole",
    )(chosen, inverse, keys, values, gates, queries, cotangent, layer_input)


def on_device(queries, key_states, value_states, cotangent, gate_logits, layer_input, chosen):
    def turned(a):
        return jnp.swapaxes(a, 1, 2)

    blocks = jnp.arange(DEVS * BPD, dtype=jnp.int32)
    order = jnp.arange(TOPK, dtype=jnp.int32)[:, None]
    first = jnp.arange(BPD, dtype=jnp.int32)[:, None, None] * TOPK
    hit = chosen[:, :, 0, :, None] == blocks
    inverse = jnp.min(jnp.where(hit, order + first, BPD * TOPK), axis=2)
    query_grad, key_grad, value_grad, weight_grad = whole(
        chosen, inverse, turned(key_states), turned(value_states), turned(gate_logits),
        queries, cotangent, layer_input,
    )
    return query_grad, turned(key_grad), turned(value_grad), weight_grad


def solution(mesh):
    placed = (
        P(None, "kv", "tp"),
        P(None, "kv", "tp"),
        P(None, "kv", "tp"),
        P(None, "kv", "tp"),
        P(None, "kv", "tp"),
        P(None, ("kv", "tp"), None),
        P(None, "kv", "tp", None),
    )
    return jax.shard_map(
        on_device,
        mesh=mesh,
        in_specs=placed,
        out_specs=(P(None, "kv", "tp"), P(None, "kv", "tp"), P(None, "kv", "tp"), P(("kv", "tp"), None)),
        check_vma=False,
    )
```

```python
import jax
import jax.numpy as jnp
from jax import lax
from jax.experimental import pallas as pl
from jax.experimental.pallas import tpu as pltpu
from jax.sharding import PartitionSpec as P

BLK = 64
MESH = pl.DeviceIdType.MESH
F32 = jnp.float32
BF16 = jnp.bfloat16
SEQS = 2
BPD = 6
ROWS = BPD * BLK
ZN = 4
YN = 4
DEVS = ZN * YN * 2
HD = 64
HEADS = 4
TOPK = 16
NEG = -1e30
HALF = ROWS // 2
QUART = ROWS // 4


def place():
    kv = lax.axis_index("kv")
    tp = lax.axis_index("tp")
    z, y, c = kv // 8, (kv // 2) % 4, kv % 2
    return kv, tp, z, y, c


def rcopy(src, dst, ssem, rsem, device):
    return pltpu.make_async_remote_copy(
        src_ref=src, dst_ref=dst, send_sem=ssem, recv_sem=rsem, device_id=device, device_id_type=MESH
    )


def entry_barrier(peers):
    sem = pltpu.get_barrier_semaphore()
    for peer in peers:
        pl.semaphore_signal(sem, inc=1, device_id=peer, device_id_type=MESH)
    pl.semaphore_wait(sem, len(peers))


class Ring:
    def __init__(self, pos, plus, minus, bufs, ssem, rsem):
        self.pos, self.plus, self.minus = pos, plus, minus
        self.sb, self.rb = bufs
        self.ssem, self.rsem = ssem, rsem
        self.used = []

    def copy(self, i, dev):
        return rcopy(self.sb.at[i], self.rb.at[i], self.ssem.at[i], self.rsem.at[i], dev)

    def send(self, i, dev, value):
        self.sb[i] = value.astype(BF16)
        self.copy(i, dev).start()
        self.used.append((i, dev))

    def got(self, i):
        self.copy(i, self.plus).wait_recv()
        return self.rb[i].astype(F32)

    def start(self, part):
        p = self.pos
        self.send(0, self.plus, part((p + 2) % 4, 0))
        self.send(1, self.minus, part((p + 2) % 4, 1))

    def near(self, part):
        p = self.pos
        self.send(3, self.plus, part((p + 1) % 4, 1))
        self.send(4, self.minus, part((p + 3) % 4, 0))

    def middle(self, part):
        p = self.pos
        self.send(2, self.plus, part((p + 1) % 4, 0) + self.got(0))
        self.send(5, self.minus, part((p + 3) % 4, 1) + self.got(1))

    def end(self, part):
        p = self.pos
        first = part(p, 0) + self.got(2) + self.got(4)
        second = part(p, 1) + self.got(3) + self.got(5)
        return first, second

    def drain(self):
        for i, dev in self.used:
            self.copy(i, dev).wait_send()


class Gather:
    def __init__(self, h, kv_ref, where, ssem, rsem, psend, precv):
        self.h, self.kv_ref, self.where = h, kv_ref, where
        self.ssem, self.rsem, self.psend, self.precv = ssem, rsem, psend, precv
        self.kv, self.tp, self.z, self.y, self.c = where
        self.partner = (self.kv + 1 - 2 * self.c, self.tp)
        self.sends = []
        self.shares = []

    def at(self, a, b):
        dz, dy = (b, a) if self.h == 0 else (a, b)
        return ((self.z + dz) % 4) * 8 + ((self.y + dy) % 4) * 2 + self.c

    def ref(self, a, b, part, shift=0):
        lo, n = self.h * HALF, HALF
        if part is not None:
            lo, n = lo + part * QUART, QUART
        return self.kv_ref.at[self.at(a, b) + shift, pl.ds(lo, n)]

    def copy(self, i, a, b, part, to):
        r = self.ref(a, b, part)
        return rcopy(r, r, self.ssem.at[i], self.rsem.at[i], (self.at(*to), self.tp))

    def send(self, *args):
        self.copy(*args).start()
        self.sends.append(args)

    def recv(self, i, a, b, part):
        self.copy(i, a, b, part, (1, 0)).wait_recv()

    def share_copy(self, n, a, b, shift=0):
        r = self.ref(a, b, None, shift)
        return rcopy(r, r, self.psend.at[n], self.precv.at[n], self.partner)

    def share(self, a, b):
        n = len(self.shares)
        self.shares.append((a, b))
        self.share_copy(n, a, b).start()

    def shared(self):
        for n, (a, b) in enumerate(self.shares):
            self.share_copy(n, a, b, 1 - 2 * self.c).wait_recv()

    def drain(self):
        for args in self.sends:
            self.copy(*args).wait_send()
        for n, (a, b) in enumerate(self.shares):
            self.share_copy(n, a, b).wait_send()

    def first(self):
        self.send(0, 0, 0, None, (1, 0))
        self.send(1, 0, 0, None, (-1, 0))

    def own(self):
        self.second_start(0, 0)
        self.share(0, 0)

    def second_start(self, q, a):
        self.send(4 + 4 * q, a, 0, None, (0, 1))
        self.send(5 + 4 * q, a, 0, None, (0, -1))

    def second_forward(self, q, a):
        self.recv(4 + 4 * q, a, -1, None)
        self.send(6 + 4 * q, a, -1, 0, (0, 1))
        self.recv(5 + 4 * q, a, 1, None)
        self.send(7 + 4 * q, a, 1, 1, (0, -1))
        self.share(a, -1)
        self.share(a, 1)

    def second_end(self, q, a):
        self.recv(6 + 4 * q, a, 2, 0)
        self.recv(7 + 4 * q, a, 2, 1)
        self.share(a, 2)

    def first_forward(self):
        self.recv(0, -1, 0, None)
        self.send(2, -1, 0, 0, (1, 0))
        self.second_start(1, -1)
        self.recv(1, 1, 0, None)
        self.send(3, 1, 0, 1, (-1, 0))
        self.second_start(2, 1)
        self.share(-1, 0)
        self.share(1, 0)

    def first_end(self):
        self.recv(2, 2, 0, 0)
        self.recv(3, 2, 0, 1)
        self.second_start(3, 2)
        self.share(2, 0)


def gather_steps(pair):
    def each(*calls):
        def run():
            for name, *args in calls:
                for g in pair:
                    getattr(g, name)(*args)

        return run

    return [
        each(("first",), ("own",)),
        each(("first_forward",)),
        each(("second_forward", 0, 0), ("first_end",)),
        each(("second_forward", 1, -1), ("second_forward", 2, 1), ("second_end", 0, 0)),
        each(("second_forward", 3, 2), ("second_end", 1, -1), ("second_end", 2, 1)),
        each(("second_end", 3, 2), ("shared",)),
    ]


class Reduce:
    def __init__(self, table, mate, acc, abufs, bbufs, where, s_mate, r_mate, s_ring, r_ring):
        self.table, self.mate, self.acc = table, mate, acc
        self.kv, self.tp, self.z, self.y, self.c = where
        self.s_mate, self.r_mate = s_mate, r_mate
        kv, tp, z, y, c = where
        self.partner = (kv + 1 - 2 * c, tp)

        def to(dz, dy):
            return (((z + dz) % 4) * 8 + ((y + dy) % 4) * 2 + c, tp)

        ydir = (y, to(0, 1), to(0, 3))
        zdir = (z, to(1, 0), to(3, 0))
        self.ra = [
            Ring(*(ydir if h == 0 else zdir), [b.at[h] for b in abufs], s_ring.at[h], r_ring.at[h])
            for h in range(2)
        ]
        self.rb = [
            Ring(*(zdir if h == 0 else ydir), [b.at[h] for b in bbufs], s_ring.at[2 + h], r_ring.at[2 + h])
            for h in range(2)
        ]

    def mate_copy(self, h, g):
        rows = pl.ds(h * HALF, HALF)
        if h == 0:
            src = self.table.at[:, (self.y + g) % 4, 1 - self.c, rows]
            dst = self.mate.at[:, (self.y + g) % 4, rows]
        else:
            src = self.table.at[(self.z + g) % 4, :, 1 - self.c, rows]
            dst = self.mate.at[(self.z + g) % 4, :, rows]
        return rcopy(src, dst, self.s_mate.at[h * 4 + g], self.r_mate.at[h * 4 + g], self.partner)

    def share(self):
        for g in (2, 1, 3, 0):
            for h in range(2):
                self.mate_copy(h, g).start()

    def part_a(self, h):
        rows = slice(h * HALF, (h + 1) * HALF)

        def part(d, q):
            if h == 0:
                a = self.table[2 * q : 2 * q + 2, d, self.c, rows]
                b = self.mate[2 * q : 2 * q + 2, d, rows]
            else:
                a = self.table[d, 2 * q : 2 * q + 2, self.c, rows]
                b = self.mate[d, 2 * q : 2 * q + 2, rows]
            return a.astype(F32) + b.astype(F32)

        return part

    def part_b(self, h):
        def part(d, q):
            return self.acc[h, d, q * QUART : (q + 1) * QUART]

        return part

    def begin(self):
        for h in range(2):
            self.mate_copy(h, 2).wait_recv()
            self.ra[h].start(self.part_a(h))
        for h in range(2):
            self.mate_copy(h, 1).wait_recv()
            self.mate_copy(h, 3).wait_recv()
            self.ra[h].near(self.part_a(h))

    def middle(self):
        for h in range(2):
            self.ra[h].middle(self.part_a(h))

    def turn(self):
        for h in range(2):
            self.mate_copy(h, 0).wait_recv()
            first, second = self.ra[h].end(self.part_a(h))
            self.acc[h, 0:2] = first
            self.acc[h, 2:4] = second
            self.rb[h].start(self.part_b(h))
            self.rb[h].near(self.part_b(h))

    def middle_b(self):
        for h in range(2):
            self.rb[h].middle(self.part_b(h))

    def finish(self, out):
        for h in range(2):
            for q, value in enumerate(self.rb[h].end(self.part_b(h))):
                lo = h * HALF + q * QUART
                out[lo : lo + QUART] = value

    def drain(self):
        for h in range(2):
            for g in range(4):
                self.mate_copy(h, g).wait_send()
            self.ra[h].drain()
            self.rb[h].drain()


def whole_kernel(
    ids_ref, inv_ref, k_hbm, v_hbm, gate_hbm, q_hbm, g_hbm, x_hbm,
    dq_ref, kg_ref, vg_ref, wg_ref,
    kv0, kv1, table0, table1, mate0, mate1, acc0, acc1, sa0, ra0, sa1, ra1, sb0, rb0, sb1, rb1,
    k_ref, v_ref, gate_ref, q_in, g_in, x_in, gates_t, rows_all, kvbuf, scores, packed, picks, final,
    li_t, li_in, vsend, vland, rhs, w_out, w_own, w_mate, wsend, wland,
    l_sem, ag_s, ag_r, agp_s, agp_r, s_mate, r_mate, s_ring, r_ring, s_li, r_li, s_x, r_x, s_w, r_w, s_d, r_d,
):
    where = place()
    kv, tp, z, y, c = where
    other = 1 - c
    nrow = HEADS * BLK

    def zy(z_, y_):
        return ((z_ % 4) * 8 + (y_ % 4) * 2 + c, tp)

    partner = (kv + 1 - 2 * c, tp)
    xs = [(kv, (tp + d) % 4) for d in (1, 2, 3)]
    offsets = [(dz, dy) for dz in (2, 1, 3, 0) for dy in (2, 1, 3, 0)][:-1]
    kvs, tables = (kv0, kv1), (table0, table1)

    pairs = ((k_hbm, k_ref), (v_hbm, v_ref), (x_hbm, x_in), (q_hbm, q_in), (g_hbm, g_in), (gate_hbm, gate_ref))
    local = [pltpu.make_async_copy(a, b, l_sem.at[n]) for n, (a, b) in enumerate(pairs)]
    for d in local:
        d.start()
    peers = [partner] + xs + [zy(z + dz, y + dy) for dz, dy in offsets]
    barrier = pltpu.get_barrier_semaphore()
    for peer in peers:
        pl.semaphore_signal(barrier, inc=1, device_id=peer, device_id_type=MESH)
    local[0].wait()
    local[1].wait()
    for s in range(SEQS):
        kvs[s][kv] = jnp.concatenate([k_ref[s], v_ref[s]], axis=0).T
    pl.semaphore_wait(barrier, len(peers))

    gathers = [
        [Gather(h, kvs[s], where, ag_s.at[s, h], ag_r.at[s, h], agp_s.at[s, h], agp_r.at[s, h]) for h in range(2)]
        for s in range(SEQS)
    ]
    steps = [gather_steps(pair) for pair in gathers]
    reduces = [
        Reduce(
            tables[s], (mate0, mate1)[s], (acc0, acc1)[s],
            ((sa0, ra0), (sa1, ra1))[s], ((sb0, rb0), (sb1, rb1))[s],
            where, s_mate.at[s], r_mate.at[s], s_ring.at[s], r_ring.at[s],
        )
        for s in range(SEQS)
    ]

    def turn_input(i, carry):
        lo = pl.multiple_of(i * 512, 512)
        for s in range(SEQS):
            t = x_in[s, :, pl.ds(lo, 512)].T.reshape(2, 2, 4, 32, 96)
            for n in range(4):
                li_t[n, pl.ds(i * 2, 2), :, :, s * 96 : (s + 1) * 96] = t[:, :, n]
        return carry

    def li_copy(n):
        to = (tp + n + 1) % 4
        return rcopy(li_t.at[to], li_in.at[tp], s_li.at[n], r_li.at[n], (kv, to))

    def prepare(s, qb):
        lane = lax.broadcasted_iota(jnp.int32, (BLK, 2 * HD), 1)
        low = lane < HD
        rows = pl.ds(pl.multiple_of(qb * BLK, BLK), BLK)
        gates = gates_t[s, rows]
        at = s * BPD + qb
        for h in range(HEADS):
            pair = slice((h // 2) * 128, (h // 2) * 128 + 128)
            qv = q_in[s, rows, pair].astype(F32) * 0.125
            gv = gates[:, h : h + 1] * g_in[s, rows, pair].astype(F32)
            if h % 2 == 0:
                gv = pltpu.roll(gv, HD, 1)
            else:
                qv = pltpu.roll(qv, HD, 1)
            rows_all[at, h * BLK : (h + 1) * BLK] = jnp.where(low, qv, 0.0).astype(BF16)
            rows_all[at, nrow + h * BLK : nrow + (h + 1) * BLK] = jnp.where(low, 0.0, gv).astype(BF16)

    def attend(s, qb):
        at = s * BPD + qb
        kv_ref = kvs[s]
        block = kv * BPD + qb
        picked = [ids_ref[s, qb, 0, k] for k in range(TOPK)]
        for k in range(TOPK):
            kvbuf[k * BLK : (k + 1) * BLK] = kv_ref[picked[k] // BPD, pl.ds((picked[k] % BPD) * BLK, BLK)]
        scores[...] = lax.dot_general(
            kvbuf[...], rows_all[at], (((1,), (1,)), ((), ())), preferred_element_type=F32
        )
        qpos = block * BLK + lax.broadcasted_iota(jnp.int32, (BLK, nrow), 1) % BLK
        ahead = lax.broadcasted_iota(jnp.int32, (BLK, nrow), 0) - qpos

        def masked(k):
            sc = scores[k * BLK : (k + 1) * BLK, :nrow]
            return jnp.where(ahead <= -(picked[k] * BLK), sc, NEG)

        top = None
        for k in range(TOPK):
            m = jnp.max(masked(k).reshape(8, 8, nrow), axis=0)
            top = m if top is None else jnp.maximum(top, m)
        top = jnp.max(top, axis=0, keepdims=True)
        total = jnp.zeros((8, nrow), F32)
        for k in range(TOPK):
            e = jnp.exp(masked(k) - top)
            scores[k * BLK : (k + 1) * BLK, :nrow] = e
            total = total + jnp.sum(e.reshape(8, 8, nrow), axis=0)
        scale = 1.0 / jnp.sum(total, axis=0, keepdims=True)
        dot = jnp.zeros((8, nrow), F32)
        for k in range(TOPK):
            rows = slice(k * BLK, (k + 1) * BLK)
            w = (scores[rows, :nrow] * scale).astype(BF16)
            packed[rows, nrow:] = w
            t = w.astype(F32) * scores[rows, nrow:]
            dot = dot + jnp.sum(t.reshape(8, 8, nrow), axis=0)
        row_dot = jnp.sum(dot, axis=0, keepdims=True)
        for k in range(TOPK):
            rows = slice(k * BLK, (k + 1) * BLK)
            ds = (scores[rows, :nrow] * scale) * (scores[rows, nrow:] - row_dot)
            packed[rows, :nrow] = ds.astype(BF16)
        pick = jnp.dot(packed[...], rows_all[at], preferred_element_type=F32)
        picks[pl.ds(qb * TOPK, TOPK)] = pick.reshape(TOPK, BLK, 2 * HD)
        dq_t = jnp.dot(kvbuf[...].T, packed[:, :nrow], preferred_element_type=F32)
        dq = (dq_t[:HD] * 0.125).T
        dq_ref[s, pl.ds(pl.multiple_of(qb * BLK, BLK), BLK)] = jnp.concatenate(
            [dq[h * BLK : (h + 1) * BLK] for h in range(HEADS)], axis=1
        ).astype(BF16)

    def collect(s):
        def one(j, carry):
            for b in range(BPD):
                total = picks[inv_ref[s, 0, j * BPD + b]]
                for q in range(1, BPD):
                    total = total + picks[inv_ref[s, q, j * BPD + b]]
                tables[s][j // 8, (j // 2) % 4, j % 2, b * BLK : (b + 1) * BLK] = total.astype(BF16)
            return carry

        lax.fori_loop(0, DEVS, one, 0)

    quarter = ROWS // 4

    def x_copy(s, n):
        to = (tp + n + 1) % 4
        return rcopy(vsend.at[s], vland.at[s, tp], s_x.at[s, n], r_x.at[s, n], (kv, to))

    def finish(s):
        reduces[s].finish(final)
        lane = lax.broadcasted_iota(jnp.int32, (HALF, 2 * HD), 1)
        low = pltpu.roll(final[0:HALF].astype(BF16).astype(F32), HD, 1)
        value = jnp.where(lane < HD, low, final[HALF:]).astype(BF16)
        vsend[s] = value
        vland[s, tp] = value
        for n in (1, 0, 2):
            x_copy(s, n).start()
        turned = final[...].T
        kg_ref[s] = turned[:HD].astype(BF16)
        vg_ref[s] = turned[HD:].astype(BF16)

    def landed(s):
        for n in range(3):
            frm = (tp + 3 - n) % 4
            slot = vland.at[s, frm]
            rcopy(slot, slot, s_x.at[s, n], r_x.at[s, n], (kv, frm)).wait_recv()
        lane = lax.broadcasted_iota(jnp.int32, (quarter, 2 * HD), 1)
        for t in range(4):
            rows = slice((t % 2) * quarter, (t % 2 + 1) * quarter)
            for p in range(2):
                even = vland[s, 2 * p, rows].astype(F32)
                odd = vland[s, 2 * p + 1, rows].astype(F32)
                if t < 2:
                    odd = pltpu.roll(odd, HD, 1)
                else:
                    even = pltpu.roll(even, HD, 1)
                rhs[t, s * quarter : (s + 1) * quarter, p * 128 : (p + 1) * 128] = jnp.where(
                    lane < HD, even, odd
                ).astype(BF16)

    steps[0][0]()
    steps[1][0]()
    local[2].wait()
    lax.fori_loop(0, 4, turn_input, 0)
    steps[0][1]()
    steps[1][1]()
    lax.fori_loop(4, 8, turn_input, 0)
    for n in (1, 0, 2):
        li_copy(n).start()
    for n in (3, 4, 5):
        local[n].wait()
    for s in range(SEQS):
        gates_t[s] = jax.nn.sigmoid(gate_ref[s]).T
    picks[BPD * TOPK] = jnp.zeros((BLK, 2 * HD), F32)
    for n in range(2, 5):
        steps[0][n]()
        if n < 4:
            steps[1][n]()

        def some(i, carry, n=n):
            at = (n - 2) * 4 + i
            prepare(at // BPD, at % BPD)
            return carry

        lax.fori_loop(0, 4, some, 0)
    steps[0][5]()

    def between(n, step):
        def at(qb):
            @pl.when(qb == n)
            def _():
                step()

        return at

    marks = [between(0, steps[1][4]), between(2, steps[1][5])]

    def attend0(qb, carry):
        attend(0, qb)
        for mark in marks:
            mark(qb)
        return carry

    lax.fori_loop(0, BPD, attend0, 0)
    collect(0)
    reduces[0].share()

    marks1 = [between(1, reduces[0].begin), between(3, reduces[0].middle), between(5, reduces[0].turn)]

    def attend1(qb, carry):
        attend(1, qb)
        for mark in marks1:
            mark(qb)
        return carry

    lax.fori_loop(0, BPD, attend1, 0)
    collect(1)
    reduces[1].share()
    reduces[0].middle_b()
    reduces[1].begin()
    reduces[1].middle()
    finish(0)
    reduces[1].turn()
    landed(0)
    reduces[1].middle_b()
    finish(1)
    for n in range(3):
        frm = (tp + 3 - n) % 4
        rcopy(li_in.at[frm], li_in.at[frm], s_li.at[n], r_li.at[n], (kv, frm)).wait_recv()
    mine_li = pltpu.make_async_copy(li_t.at[tp], li_in.at[tp], l_sem.at[6])
    mine_li.start()
    mine_li.wait()
    landed(1)

    def product(side, i):
        total = None
        for t in range(4):
            a = li_in[t, pl.ds(i * 4, 4), side].reshape(128, 192)
            p = jnp.dot(a, rhs[t], preferred_element_type=F32)
            total = p if total is None else total + p
        return total.reshape(4, 32, 256)

    def for_mate(i, carry):
        w_out[pl.ds(i * 4, 4)] = product(other, i).astype(BF16)
        return carry

    def for_self(i, carry):
        w_own[pl.ds(i * 4, 4)] = product(c, i)
        return carry

    lax.fori_loop(0, 4, for_mate, 0)
    w_copy = rcopy(w_out, w_mate, s_w.at[0], r_w.at[0], partner)
    w_copy.start()
    lax.fori_loop(0, 4, for_self, 0)
    w_copy.wait_recv()
    w_own[...] = w_own[...] + w_mate[...].astype(F32)
    wsend[...] = w_own[...].astype(BF16)
    mine = kv // 2

    def d_copy(n):
        dz, dy = offsets[n]
        to = zy(z + dz, y + dy)
        return rcopy(wsend.at[to[0] // 2], wland.at[mine], s_d.at[n], r_d.at[n], to)

    for n in range(len(offsets)):
        d_copy(n).start()
    total = w_own[mine]
    for n, (dz, dy) in enumerate(offsets):
        frm = zy(z - dz, y - dy)
        slot = wland.at[frm[0] // 2]
        rcopy(slot, slot, s_d.at[n], r_d.at[n], frm).wait_recv()
        total = total + wland[frm[0] // 2].astype(F32)
    wg_ref[...] = total

    for pair in gathers:
        for g in pair:
            g.drain()
    for r in reduces:
        r.drain()
    for n in range(3):
        li_copy(n).wait_send()
        for s in range(SEQS):
            x_copy(s, n).wait_send()
    w_copy.wait_send()
    for n in range(len(offsets)):
        d_copy(n).wait_send()


def whole(chosen, inverse, keys, values, gates, queries, cotangent, layer_input):
    v = pltpu.VMEM
    dma = pltpu.SemaphoreType.DMA
    wide = 2 * HD
    anywhere = pl.BlockSpec(memory_space=pltpu.HBM)
    onchip = pl.BlockSpec(memory_space=v)
    smem = pl.BlockSpec(memory_space=pltpu.SMEM)
    keys_n = TOPK * BLK
    nrow = HEADS * BLK
    return pl.pallas_call(
        whole_kernel,
        out_shape=[
            jax.ShapeDtypeStruct((SEQS, ROWS, HEADS * HD), BF16),
            jax.ShapeDtypeStruct((SEQS, HD, ROWS), BF16),
            jax.ShapeDtypeStruct((SEQS, HD, ROWS), BF16),
            jax.ShapeDtypeStruct((32, 256), F32),
        ],
        in_specs=[smem, smem] + [anywhere] * 6,
        out_specs=[onchip] * 4,
        scratch_shapes=[
            *[v((DEVS, ROWS, wide), BF16) for _ in range(2)],
            *[v((ZN, YN, 2, ROWS, wide), BF16) for _ in range(2)],
            *[v((ZN, YN, ROWS, wide), BF16) for _ in range(2)],
            *[v((2, 4, HALF, wide), F32) for _ in range(2)],
            *[v((2, 6, 2, HALF, wide), BF16) for _ in range(4)],
            *[v((2, 6, QUART, wide), BF16) for _ in range(4)],
            v((SEQS, HD, ROWS), BF16),
            v((SEQS, HD, ROWS), BF16),
            v((SEQS, HEADS, ROWS), F32),
            v((SEQS, ROWS, HEADS * HD), BF16),
            v((SEQS, ROWS, HEADS * HD), BF16),
            v((SEQS, ROWS // 4, 4096), BF16),
            v((SEQS, ROWS, HEADS), F32),
            v((SEQS * BPD, 2 * nrow, wide), BF16),
            v((keys_n, wide), BF16),
            v((keys_n, 2 * nrow), F32),
            v((keys_n, 2 * nrow), BF16),
            v((BPD * TOPK + 1, BLK, wide), F32),
            v((ROWS, wide), F32),
            v((4, 16, 2, 32, 192), BF16),
            v((4, 16, 2, 32, 192), BF16),
            v((SEQS, HALF, wide), BF16),
            v((SEQS, 4, HALF, wide), BF16),
            v((4, 192, 256), BF16),
            v((16, 32, 256), BF16),
            v((16, 32, 256), F32),
            v((16, 32, 256), BF16),
            v((16, 32, 256), BF16),
            v((16, 32, 256), BF16),
            dma((7,)),
            *[dma((2, 2, 20)) for _ in range(2)],
            *[dma((2, 2, 16)) for _ in range(2)],
            *[dma((2, 8)) for _ in range(2)],
            *[dma((2, 4, 6)) for _ in range(2)],
            *[dma((3,)) for _ in range(2)],
            *[dma((2, 3)) for _ in range(2)],
            *[dma((1,)) for _ in range(2)],
            *[dma((15,)) for _ in range(2)],
        ],
        compiler_params=pltpu.CompilerParams(
            collective_id=0, has_side_effects=True, vmem_limit_bytes=44 * 2**20
        ),
        name="whole",
    )(
        chosen,
        inverse,
        *[
            pltpu.with_memory_space_constraint(a, pltpu.HBM)
            for a in (keys, values, gates, queries, cotangent, layer_input)
        ],
    )


def on_device(queries, key_states, value_states, cotangent, gate_logits, layer_input, chosen):
    def turned(a):
        return jnp.swapaxes(a, 1, 2)

    blocks = jnp.arange(DEVS * BPD, dtype=jnp.int32)
    order = jnp.arange(TOPK, dtype=jnp.int32)[:, None]
    first = jnp.arange(BPD, dtype=jnp.int32)[:, None, None] * TOPK
    hit = chosen[:, :, 0, :, None] == blocks
    inverse = jnp.min(jnp.where(hit, order + first, BPD * TOPK), axis=2)
    query_grad, key_grad, value_grad, weight_grad = whole(
        chosen, inverse, turned(key_states), turned(value_states), turned(gate_logits),
        queries, cotangent, layer_input,
    )
    return query_grad, turned(key_grad), turned(value_grad), weight_grad


def solution(mesh):
    placed = (
        P(None, "kv", "tp"),
        P(None, "kv", "tp"),
        P(None, "kv", "tp"),
        P(None, "kv", "tp"),
        P(None, "kv", "tp"),
        P(None, ("kv", "tp"), None),
        P(None, "kv", "tp", None),
    )
    return jax.shard_map(
        on_device,
        mesh=mesh,
        in_specs=placed,
        out_specs=(P(None, "kv", "tp"), P(None, "kv", "tp"), P(None, "kv", "tp"), P(("kv", "tp"), None)),
        check_vma=False,
    )
```

```python
import jax
import jax.numpy as jnp
from jax import lax
from jax.experimental import pallas as pl
from jax.experimental.pallas import tpu as pltpu
from jax.sharding import PartitionSpec as P

BLK = 64
MESH = pl.DeviceIdType.MESH
F32 = jnp.float32
BF16 = jnp.bfloat16
SEQS = 2
BPD = 6
ROWS = BPD * BLK
ZN = 4
YN = 4
DEVS = ZN * YN * 2
HD = 64
HEADS = 4
TOPK = 16
NEG = -1e30
HALF = ROWS // 2
QUART = ROWS // 4


def place():
    kv = lax.axis_index("kv")
    tp = lax.axis_index("tp")
    z, y, c = kv // 8, (kv // 2) % 4, kv % 2
    return kv, tp, z, y, c


def rcopy(src, dst, ssem, rsem, device):
    return pltpu.make_async_remote_copy(
        src_ref=src, dst_ref=dst, send_sem=ssem, recv_sem=rsem, device_id=device, device_id_type=MESH
    )


def entry_barrier(peers):
    sem = pltpu.get_barrier_semaphore()
    for peer in peers:
        pl.semaphore_signal(sem, inc=1, device_id=peer, device_id_type=MESH)
    pl.semaphore_wait(sem, len(peers))


class Ring:
    def __init__(self, pos, plus, minus, bufs, ssem, rsem):
        self.pos, self.plus, self.minus = pos, plus, minus
        self.sb, self.rb = bufs
        self.ssem, self.rsem = ssem, rsem
        self.used = []

    def copy(self, i, dev):
        return rcopy(self.sb.at[i], self.rb.at[i], self.ssem.at[i], self.rsem.at[i], dev)

    def send(self, i, dev, value):
        self.sb[i] = value.astype(BF16)
        self.copy(i, dev).start()
        self.used.append((i, dev))

    def got(self, i):
        self.copy(i, self.plus).wait_recv()
        return self.rb[i].astype(F32)

    def start(self, part):
        p = self.pos
        self.send(0, self.plus, part((p + 2) % 4, 0))
        self.send(1, self.minus, part((p + 2) % 4, 1))

    def near(self, part):
        p = self.pos
        self.send(3, self.plus, part((p + 1) % 4, 1))
        self.send(4, self.minus, part((p + 3) % 4, 0))

    def middle(self, part):
        p = self.pos
        self.send(2, self.plus, part((p + 1) % 4, 0) + self.got(0))
        self.send(5, self.minus, part((p + 3) % 4, 1) + self.got(1))

    def end(self, part):
        p = self.pos
        first = part(p, 0) + self.got(2) + self.got(4)
        second = part(p, 1) + self.got(3) + self.got(5)
        return first, second

    def drain(self):
        for i, dev in self.used:
            self.copy(i, dev).wait_send()


class Gather:
    def __init__(self, h, kv_ref, where, ssem, rsem, psend, precv):
        self.h, self.kv_ref, self.where = h, kv_ref, where
        self.ssem, self.rsem, self.psend, self.precv = ssem, rsem, psend, precv
        self.kv, self.tp, self.z, self.y, self.c = where
        self.partner = (self.kv + 1 - 2 * self.c, self.tp)
        self.sends = []
        self.shares = []

    def at(self, a, b):
        dz, dy = (b, a) if self.h == 0 else (a, b)
        return ((self.z + dz) % 4) * 8 + ((self.y + dy) % 4) * 2 + self.c

    def ref(self, a, b, part, shift=0):
        lo, n = self.h * HALF, HALF
        if part is not None:
            lo, n = lo + part * QUART, QUART
        return self.kv_ref.at[self.at(a, b) + shift, pl.ds(lo, n)]

    def copy(self, i, a, b, part, to):
        r = self.ref(a, b, part)
        return rcopy(r, r, self.ssem.at[i], self.rsem.at[i], (self.at(*to), self.tp))

    def send(self, *args):
        self.copy(*args).start()
        self.sends.append(args)

    def recv(self, i, a, b, part):
        self.copy(i, a, b, part, (1, 0)).wait_recv()

    def share_copy(self, n, a, b, shift=0):
        r = self.ref(a, b, None, shift)
        return rcopy(r, r, self.psend.at[n], self.precv.at[n], self.partner)

    def share(self, a, b):
        n = len(self.shares)
        self.shares.append((a, b))
        self.share_copy(n, a, b).start()

    def shared(self):
        for n, (a, b) in enumerate(self.shares):
            self.share_copy(n, a, b, 1 - 2 * self.c).wait_recv()

    def drain(self):
        for args in self.sends:
            self.copy(*args).wait_send()
        for n, (a, b) in enumerate(self.shares):
            self.share_copy(n, a, b).wait_send()

    def first(self):
        self.send(0, 0, 0, None, (1, 0))
        self.send(1, 0, 0, None, (-1, 0))

    def own(self):
        self.second_start(0, 0)
        self.share(0, 0)

    def second_start(self, q, a):
        self.send(4 + 4 * q, a, 0, None, (0, 1))
        self.send(5 + 4 * q, a, 0, None, (0, -1))

    def second_forward(self, q, a):
        self.recv(4 + 4 * q, a, -1, None)
        self.send(6 + 4 * q, a, -1, 0, (0, 1))
        self.recv(5 + 4 * q, a, 1, None)
        self.send(7 + 4 * q, a, 1, 1, (0, -1))
        self.share(a, -1)
        self.share(a, 1)

    def second_end(self, q, a):
        self.recv(6 + 4 * q, a, 2, 0)
        self.recv(7 + 4 * q, a, 2, 1)
        self.share(a, 2)

    def first_forward(self):
        self.recv(0, -1, 0, None)
        self.send(2, -1, 0, 0, (1, 0))
        self.second_start(1, -1)
        self.recv(1, 1, 0, None)
        self.send(3, 1, 0, 1, (-1, 0))
        self.second_start(2, 1)
        self.share(-1, 0)
        self.share(1, 0)

    def first_end(self):
        self.recv(2, 2, 0, 0)
        self.recv(3, 2, 0, 1)
        self.second_start(3, 2)
        self.share(2, 0)


def gather_steps(pair):
    def each(*calls):
        def run():
            for name, *args in calls:
                for g in pair:
                    getattr(g, name)(*args)

        return run

    return [
        each(("first",), ("own",)),
        each(("first_forward",)),
        each(("second_forward", 0, 0), ("first_end",)),
        each(("second_forward", 1, -1), ("second_forward", 2, 1), ("second_end", 0, 0)),
        each(("second_forward", 3, 2), ("second_end", 1, -1), ("second_end", 2, 1)),
        each(("second_end", 3, 2), ("shared",)),
    ]


class Reduce:
    def __init__(self, table, mate, acc, abufs, bbufs, where, s_mate, r_mate, s_ring, r_ring):
        self.table, self.mate, self.acc = table, mate, acc
        self.kv, self.tp, self.z, self.y, self.c = where
        self.s_mate, self.r_mate = s_mate, r_mate
        kv, tp, z, y, c = where
        self.partner = (kv + 1 - 2 * c, tp)

        def to(dz, dy):
            return (((z + dz) % 4) * 8 + ((y + dy) % 4) * 2 + c, tp)

        ydir = (y, to(0, 1), to(0, 3))
        zdir = (z, to(1, 0), to(3, 0))
        self.ra = [
            Ring(*(ydir if h == 0 else zdir), [b.at[h] for b in abufs], s_ring.at[h], r_ring.at[h])
            for h in range(2)
        ]
        self.rb = [
            Ring(*(zdir if h == 0 else ydir), [b.at[h] for b in bbufs], s_ring.at[2 + h], r_ring.at[2 + h])
            for h in range(2)
        ]

    def mate_copy(self, h, g):
        rows = pl.ds(h * HALF, HALF)
        if h == 0:
            src = self.table.at[:, (self.y + g) % 4, 1 - self.c, rows]
            dst = self.mate.at[:, (self.y + g) % 4, rows]
        else:
            src = self.table.at[(self.z + g) % 4, :, 1 - self.c, rows]
            dst = self.mate.at[(self.z + g) % 4, :, rows]
        return rcopy(src, dst, self.s_mate.at[h * 4 + g], self.r_mate.at[h * 4 + g], self.partner)

    def share(self):
        for g in (2, 1, 3, 0):
            for h in range(2):
                self.mate_copy(h, g).start()

    def part_a(self, h):
        rows = slice(h * HALF, (h + 1) * HALF)

        def part(d, q):
            if h == 0:
                a = self.table[2 * q : 2 * q + 2, d, self.c, rows]
                b = self.mate[2 * q : 2 * q + 2, d, rows]
            else:
                a = self.table[d, 2 * q : 2 * q + 2, self.c, rows]
                b = self.mate[d, 2 * q : 2 * q + 2, rows]
            return a.astype(F32) + b.astype(F32)

        return part

    def part_b(self, h):
        def part(d, q):
            return self.acc[h, d, q * QUART : (q + 1) * QUART]

        return part

    def begin(self):
        for h in range(2):
            self.mate_copy(h, 2).wait_recv()
            self.ra[h].start(self.part_a(h))
        for h in range(2):
            self.mate_copy(h, 1).wait_recv()
            self.mate_copy(h, 3).wait_recv()
            self.ra[h].near(self.part_a(h))

    def middle(self):
        for h in range(2):
            self.ra[h].middle(self.part_a(h))

    def turn(self):
        for h in range(2):
            self.mate_copy(h, 0).wait_recv()
            first, second = self.ra[h].end(self.part_a(h))
            self.acc[h, 0:2] = first
            self.acc[h, 2:4] = second
            self.rb[h].start(self.part_b(h))
            self.rb[h].near(self.part_b(h))

    def middle_b(self):
        for h in range(2):
            self.rb[h].middle(self.part_b(h))

    def finish(self, out):
        for h in range(2):
            for q, value in enumerate(self.rb[h].end(self.part_b(h))):
                lo = h * HALF + q * QUART
                out[lo : lo + QUART] = value

    def drain(self):
        for h in range(2):
            for g in range(4):
                self.mate_copy(h, g).wait_send()
            self.ra[h].drain()
            self.rb[h].drain()


def whole_kernel(
    ids_hbm, k_hbm, v_hbm, gate_hbm, q_hbm, g_hbm, x_hbm,
    dq_ref, kg_ref, vg_ref, wg_ref,
    kv0, kv1, table0, table1, mate0, mate1, acc0, acc1, sa0, ra0, sa1, ra1, sb0, rb0, sb1, rb1,
    ids_ref, inv_ref, inv_v, k_ref, v_ref, gate_ref, q_in, g_in, x_in, gates_t, rows_all, kvbuf, scores, packed, picks, final,
    li_t, li_in, vsend, vland, rhs, w_out, w_own, w_mate, wsend, wland,
    l_sem, ag_s, ag_r, agp_s, agp_r, s_mate, r_mate, s_ring, r_ring, s_li, r_li, s_x, r_x, s_w, r_w, s_d, r_d,
):
    where = place()
    kv, tp, z, y, c = where
    other = 1 - c
    nrow = HEADS * BLK

    def zy(z_, y_):
        return ((z_ % 4) * 8 + (y_ % 4) * 2 + c, tp)

    partner = (kv + 1 - 2 * c, tp)
    xs = [(kv, (tp + d) % 4) for d in (1, 2, 3)]
    offsets = [(dz, dy) for dz in (2, 1, 3, 0) for dy in (2, 1, 3, 0)][:-1]
    kvs, tables = (kv0, kv1), (table0, table1)

    pairs = ((k_hbm, k_ref), (v_hbm, v_ref), (x_hbm, x_in), (q_hbm, q_in), (g_hbm, g_in), (gate_hbm, gate_ref), (ids_hbm, ids_ref))
    local = [pltpu.make_async_copy(a, b, l_sem.at[n]) for n, (a, b) in enumerate(pairs)]
    for d in local:
        d.start()
    peers = [partner] + xs + [zy(z + dz, y + dy) for dz, dy in offsets]
    barrier = pltpu.get_barrier_semaphore()
    for peer in peers:
        pl.semaphore_signal(barrier, inc=1, device_id=peer, device_id_type=MESH)
    local[0].wait()
    local[1].wait()
    for s in range(SEQS):
        kvs[s][kv] = jnp.concatenate([k_ref[s], v_ref[s]], axis=0).T
    pl.semaphore_wait(barrier, len(peers))

    gathers = [
        [Gather(h, kvs[s], where, ag_s.at[s, h], ag_r.at[s, h], agp_s.at[s, h], agp_r.at[s, h]) for h in range(2)]
        for s in range(SEQS)
    ]
    steps = [gather_steps(pair) for pair in gathers]
    reduces = [
        Reduce(
            tables[s], (mate0, mate1)[s], (acc0, acc1)[s],
            ((sa0, ra0), (sa1, ra1))[s], ((sb0, rb0), (sb1, rb1))[s],
            where, s_mate.at[s], r_mate.at[s], s_ring.at[s], r_ring.at[s],
        )
        for s in range(SEQS)
    ]

    def turn_input(i, carry):
        lo = pl.multiple_of(i * 512, 512)
        for s in range(SEQS):
            t = x_in[s, :, pl.ds(lo, 512)].T.reshape(2, 2, 4, 32, 96)
            for n in range(4):
                li_t[n, pl.ds(i * 2, 2), :, :, s * 96 : (s + 1) * 96] = t[:, :, n]
        return carry

    def li_copy(n):
        to = (tp + n + 1) % 4
        return rcopy(li_t.at[to], li_in.at[tp], s_li.at[n], r_li.at[n], (kv, to))

    def prepare(s, qb):
        lane = lax.broadcasted_iota(jnp.int32, (BLK, 2 * HD), 1)
        low = lane < HD
        rows = pl.ds(pl.multiple_of(qb * BLK, BLK), BLK)
        gates = gates_t[s, rows]
        at = s * BPD + qb
        for h in range(HEADS):
            pair = slice((h // 2) * 128, (h // 2) * 128 + 128)
            qv = q_in[s, rows, pair].astype(F32) * 0.125
            gv = gates[:, h : h + 1] * g_in[s, rows, pair].astype(F32)
            if h % 2 == 0:
                gv = pltpu.roll(gv, HD, 1)
            else:
                qv = pltpu.roll(qv, HD, 1)
            rows_all[at, h * BLK : (h + 1) * BLK] = jnp.where(low, qv, 0.0).astype(BF16)
            rows_all[at, nrow + h * BLK : nrow + (h + 1) * BLK] = jnp.where(low, 0.0, gv).astype(BF16)

    def attend(s, qb):
        at = s * BPD + qb
        kv_ref = kvs[s]
        block = kv * BPD + qb
        picked = [ids_ref[s, qb, 0, k] for k in range(TOPK)]
        for k in range(TOPK):
            kvbuf[k * BLK : (k + 1) * BLK] = kv_ref[picked[k] // BPD, pl.ds((picked[k] % BPD) * BLK, BLK)]
        scores[...] = lax.dot_general(
            kvbuf[...], rows_all[at], (((1,), (1,)), ((), ())), preferred_element_type=F32
        )
        qpos = block * BLK + lax.broadcasted_iota(jnp.int32, (BLK, nrow), 1) % BLK
        ahead = lax.broadcasted_iota(jnp.int32, (BLK, nrow), 0) - qpos

        def masked(k):
            sc = scores[k * BLK : (k + 1) * BLK, :nrow]
            return jnp.where(ahead <= -(picked[k] * BLK), sc, NEG)

        top = None
        for k in range(TOPK):
            m = jnp.max(masked(k).reshape(8, 8, nrow), axis=0)
            top = m if top is None else jnp.maximum(top, m)
        top = jnp.max(top, axis=0, keepdims=True)
        total = jnp.zeros((8, nrow), F32)
        for k in range(TOPK):
            e = jnp.exp(masked(k) - top)
            scores[k * BLK : (k + 1) * BLK, :nrow] = e
            total = total + jnp.sum(e.reshape(8, 8, nrow), axis=0)
        scale = 1.0 / jnp.sum(total, axis=0, keepdims=True)
        dot = jnp.zeros((8, nrow), F32)
        for k in range(TOPK):
            rows = slice(k * BLK, (k + 1) * BLK)
            w = (scores[rows, :nrow] * scale).astype(BF16)
            packed[rows, nrow:] = w
            t = w.astype(F32) * scores[rows, nrow:]
            dot = dot + jnp.sum(t.reshape(8, 8, nrow), axis=0)
        row_dot = jnp.sum(dot, axis=0, keepdims=True)
        for k in range(TOPK):
            rows = slice(k * BLK, (k + 1) * BLK)
            ds = (scores[rows, :nrow] * scale) * (scores[rows, nrow:] - row_dot)
            packed[rows, :nrow] = ds.astype(BF16)
        pick = jnp.dot(packed[...], rows_all[at], preferred_element_type=F32)
        picks[pl.ds(qb * TOPK, TOPK)] = pick.reshape(TOPK, BLK, 2 * HD)
        dq_t = jnp.dot(kvbuf[...].T, packed[:, :nrow], preferred_element_type=F32)
        dq = (dq_t[:HD] * 0.125).T
        dq_ref[s, pl.ds(pl.multiple_of(qb * BLK, BLK), BLK)] = jnp.concatenate(
            [dq[h * BLK : (h + 1) * BLK] for h in range(HEADS)], axis=1
        ).astype(BF16)

    def collect(s):
        def one(j, carry):
            for b in range(BPD):
                total = picks[inv_ref[s * BPD, j * BPD + b]]
                for q in range(1, BPD):
                    total = total + picks[inv_ref[s * BPD + q, j * BPD + b]]
                tables[s][j // 8, (j // 2) % 4, j % 2, b * BLK : (b + 1) * BLK] = total.astype(BF16)
            return carry

        lax.fori_loop(0, DEVS, one, 0)

    quarter = ROWS // 4

    def x_copy(s, n):
        to = (tp + n + 1) % 4
        return rcopy(vsend.at[s], vland.at[s, tp], s_x.at[s, n], r_x.at[s, n], (kv, to))

    def finish(s):
        reduces[s].finish(final)
        lane = lax.broadcasted_iota(jnp.int32, (HALF, 2 * HD), 1)
        low = pltpu.roll(final[0:HALF].astype(BF16).astype(F32), HD, 1)
        value = jnp.where(lane < HD, low, final[HALF:]).astype(BF16)
        vsend[s] = value
        vland[s, tp] = value
        for n in (1, 0, 2):
            x_copy(s, n).start()
        turned = final[...].T
        kg_ref[s] = turned[:HD].astype(BF16)
        vg_ref[s] = turned[HD:].astype(BF16)

    def landed(s):
        for n in range(3):
            frm = (tp + 3 - n) % 4
            slot = vland.at[s, frm]
            rcopy(slot, slot, s_x.at[s, n], r_x.at[s, n], (kv, frm)).wait_recv()
        lane = lax.broadcasted_iota(jnp.int32, (quarter, 2 * HD), 1)
        for t in range(4):
            rows = slice((t % 2) * quarter, (t % 2 + 1) * quarter)
            for p in range(2):
                even = vland[s, 2 * p, rows].astype(F32)
                odd = vland[s, 2 * p + 1, rows].astype(F32)
                if t < 2:
                    odd = pltpu.roll(odd, HD, 1)
                else:
                    even = pltpu.roll(even, HD, 1)
                rhs[t, s * quarter : (s + 1) * quarter, p * 128 : (p + 1) * 128] = jnp.where(
                    lane < HD, even, odd
                ).astype(BF16)

    steps[0][0]()
    local[6].wait()
    spot = lax.broadcasted_iota(jnp.int32, (1, 256), 1)
    for s in range(SEQS):
        for qb in range(BPD):
            slot = jnp.full((1, 256), BPD * TOPK, jnp.int32)
            for k in range(TOPK):
                slot = jnp.where(spot == ids_ref[s, qb, 0, k], qb * TOPK + k, slot)
            inv_v[s * BPD + qb : s * BPD + qb + 1] = slot
    to_scalar = pltpu.make_async_copy(inv_v, inv_ref, l_sem.at[8])
    to_scalar.start()
    local[2].wait()
    lax.fori_loop(0, 4, turn_input, 0)
    steps[0][1]()
    steps[1][0]()
    lax.fori_loop(4, 8, turn_input, 0)
    for n in (1, 0, 2):
        li_copy(n).start()
    for n in (3, 4, 5):
        local[n].wait()
    for s in range(SEQS):
        gates_t[s] = jax.nn.sigmoid(gate_ref[s]).T
    to_scalar.wait()
    picks[BPD * TOPK] = jnp.zeros((BLK, 2 * HD), F32)
    for n in range(2, 5):
        steps[0][n]()
        if n != 3:
            steps[1][n // 2]()

        def some(i, carry, n=n):
            at = (n - 2) * 4 + i
            prepare(at // BPD, at % BPD)
            return carry

        lax.fori_loop(0, 4, some, 0)
    steps[0][5]()

    def between(n, step):
        def at(qb):
            @pl.when(qb == n)
            def _():
                step()

        return at

    marks = [between(0, steps[1][3]), between(2, steps[1][4]), between(4, steps[1][5])]

    def attend0(qb, carry):
        attend(0, qb)
        for mark in marks:
            mark(qb)
        return carry

    lax.fori_loop(0, BPD, attend0, 0)
    collect(0)
    reduces[0].share()

    marks1 = [between(2, reduces[0].begin), between(4, reduces[0].middle)]

    def attend1(qb, carry):
        attend(1, qb)
        for mark in marks1:
            mark(qb)
        return carry

    lax.fori_loop(0, BPD, attend1, 0)
    collect(1)
    reduces[1].share()
    reduces[0].turn()
    reduces[1].begin()
    reduces[0].middle_b()
    reduces[1].middle()
    finish(0)
    reduces[1].turn()
    landed(0)
    reduces[1].middle_b()
    finish(1)
    for n in range(3):
        frm = (tp + 3 - n) % 4
        rcopy(li_in.at[frm], li_in.at[frm], s_li.at[n], r_li.at[n], (kv, frm)).wait_recv()
    mine_li = pltpu.make_async_copy(li_t.at[tp], li_in.at[tp], l_sem.at[7])
    mine_li.start()
    mine_li.wait()
    landed(1)

    def product(side, i):
        total = None
        for t in range(4):
            a = li_in[t, pl.ds(i * 4, 4), side].reshape(128, 192)
            p = jnp.dot(a, rhs[t], preferred_element_type=F32)
            total = p if total is None else total + p
        return total.reshape(4, 32, 256)

    order = (2, 1, 3, 0)
    mine = kv // 2

    def piece(dz):
        return pl.ds(((z + dz) % 4) * 4, 4)

    def w_copy(dz):
        rows = piece(dz)
        return rcopy(w_out.at[rows], w_mate.at[rows], s_w.at[dz], r_w.at[dz], partner)

    def d_copy(n):
        dz, dy = offsets[n]
        to = zy(z + dz, y + dy)
        return rcopy(wsend.at[to[0] // 2], wland.at[mine], s_d.at[n], r_d.at[n], to)

    for dz in order:
        w_out[piece(dz)] = product(other, (z + dz) % 4).astype(BF16)
        w_copy(dz).start()
    for dz in order:
        w_own[piece(dz)] = product(c, (z + dz) % 4)
    for dz in order:
        w_copy(dz).wait_recv()
        value = w_own[piece(dz)] + w_mate[piece(dz)].astype(F32)
        w_own[piece(dz)] = value
        wsend[piece(dz)] = value.astype(BF16)
        for n in range(len(offsets)):
            if offsets[n][0] == dz:
                d_copy(n).start()
    total = w_own[mine]
    for n, (dz, dy) in enumerate(offsets):
        frm = zy(z - dz, y - dy)
        slot = wland.at[frm[0] // 2]
        rcopy(slot, slot, s_d.at[n], r_d.at[n], frm).wait_recv()
        total = total + wland[frm[0] // 2].astype(F32)
    wg_ref[...] = total

    for pair in gathers:
        for g in pair:
            g.drain()
    for r in reduces:
        r.drain()
    for n in range(3):
        li_copy(n).wait_send()
        for s in range(SEQS):
            x_copy(s, n).wait_send()
    for dz in order:
        w_copy(dz).wait_send()
    for n in range(len(offsets)):
        d_copy(n).wait_send()


def whole(chosen, keys, values, gates, queries, cotangent, layer_input):
    v = pltpu.VMEM
    dma = pltpu.SemaphoreType.DMA
    wide = 2 * HD
    anywhere = pl.BlockSpec(memory_space=pltpu.HBM)
    onchip = pl.BlockSpec(memory_space=v)
    keys_n = TOPK * BLK
    nrow = HEADS * BLK
    return pl.pallas_call(
        whole_kernel,
        out_shape=[
            jax.ShapeDtypeStruct((SEQS, ROWS, HEADS * HD), BF16),
            jax.ShapeDtypeStruct((SEQS, HD, ROWS), BF16),
            jax.ShapeDtypeStruct((SEQS, HD, ROWS), BF16),
            jax.ShapeDtypeStruct((32, 256), F32),
        ],
        in_specs=[anywhere] * 7,
        out_specs=[onchip] * 4,
        scratch_shapes=[
            *[v((DEVS, ROWS, wide), BF16) for _ in range(2)],
            *[v((ZN, YN, 2, ROWS, wide), BF16) for _ in range(2)],
            *[v((ZN, YN, ROWS, wide), BF16) for _ in range(2)],
            *[v((2, 4, HALF, wide), F32) for _ in range(2)],
            *[v((2, 6, 2, HALF, wide), BF16) for _ in range(4)],
            *[v((2, 6, QUART, wide), BF16) for _ in range(4)],
            pltpu.SMEM((SEQS, BPD, 1, TOPK), jnp.int32),
            pltpu.SMEM((SEQS * BPD, 256), jnp.int32),
            v((SEQS * BPD, 256), jnp.int32),
            v((SEQS, HD, ROWS), BF16),
            v((SEQS, HD, ROWS), BF16),
            v((SEQS, HEADS, ROWS), F32),
            v((SEQS, ROWS, HEADS * HD), BF16),
            v((SEQS, ROWS, HEADS * HD), BF16),
            v((SEQS, ROWS // 4, 4096), BF16),
            v((SEQS, ROWS, HEADS), F32),
            v((SEQS * BPD, 2 * nrow, wide), BF16),
            v((keys_n, wide), BF16),
            v((keys_n, 2 * nrow), F32),
            v((keys_n, 2 * nrow), BF16),
            v((BPD * TOPK + 1, BLK, wide), F32),
            v((ROWS, wide), F32),
            v((4, 16, 2, 32, 192), BF16),
            v((4, 16, 2, 32, 192), BF16),
            v((SEQS, HALF, wide), BF16),
            v((SEQS, 4, HALF, wide), BF16),
            v((4, 192, 256), BF16),
            v((16, 32, 256), BF16),
            v((16, 32, 256), F32),
            v((16, 32, 256), BF16),
            v((16, 32, 256), BF16),
            v((16, 32, 256), BF16),
            dma((9,)),
            *[dma((2, 2, 20)) for _ in range(2)],
            *[dma((2, 2, 16)) for _ in range(2)],
            *[dma((2, 8)) for _ in range(2)],
            *[dma((2, 4, 6)) for _ in range(2)],
            *[dma((3,)) for _ in range(2)],
            *[dma((2, 3)) for _ in range(2)],
            *[dma((4,)) for _ in range(2)],
            *[dma((15,)) for _ in range(2)],
        ],
        compiler_params=pltpu.CompilerParams(
            collective_id=0, has_side_effects=True, vmem_limit_bytes=44 * 2**20
        ),
        name="whole",
    )(
        *[
            pltpu.with_memory_space_constraint(a, pltpu.HBM)
            for a in (chosen, keys, values, gates, queries, cotangent, layer_input)
        ],
    )


def on_device(queries, key_states, value_states, cotangent, gate_logits, layer_input, chosen):
    def turned(a):
        return jnp.swapaxes(a, 1, 2)

    query_grad, key_grad, value_grad, weight_grad = whole(
        chosen, turned(key_states), turned(value_states), turned(gate_logits),
        queries, cotangent, layer_input,
    )
    return query_grad, turned(key_grad), turned(value_grad), weight_grad


def solution(mesh):
    placed = (
        P(None, "kv", "tp"),
        P(None, "kv", "tp"),
        P(None, "kv", "tp"),
        P(None, "kv", "tp"),
        P(None, "kv", "tp"),
        P(None, ("kv", "tp"), None),
        P(None, "kv", "tp", None),
    )
    return jax.shard_map(
        on_device,
        mesh=mesh,
        in_specs=placed,
        out_specs=(P(None, "kv", "tp"), P(None, "kv", "tp"), P(None, "kv", "tp"), P(("kv", "tp"), None)),
        check_vma=False,
    )
```

```python
import jax
import jax.numpy as jnp
from jax import lax
from jax.experimental import pallas as pl
from jax.experimental.pallas import tpu as pltpu
from jax.sharding import PartitionSpec as P

BLK = 64
MESH = pl.DeviceIdType.MESH
F32 = jnp.float32
BF16 = jnp.bfloat16
SEQS = 2
BPD = 6
ROWS = BPD * BLK
ZN = 4
YN = 4
DEVS = ZN * YN * 2
HD = 64
HEADS = 4
TOPK = 16
NEG = -1e30
HALF = ROWS // 2
QUART = ROWS // 4


def place():
    kv = lax.axis_index("kv")
    tp = lax.axis_index("tp")
    z, y, c = kv // 8, (kv // 2) % 4, kv % 2
    return kv, tp, z, y, c


def rcopy(src, dst, ssem, rsem, device):
    return pltpu.make_async_remote_copy(
        src_ref=src, dst_ref=dst, send_sem=ssem, recv_sem=rsem, device_id=device, device_id_type=MESH
    )


def entry_barrier(peers):
    sem = pltpu.get_barrier_semaphore()
    for peer in peers:
        pl.semaphore_signal(sem, inc=1, device_id=peer, device_id_type=MESH)
    pl.semaphore_wait(sem, len(peers))


class Ring:
    def __init__(self, pos, plus, minus, bufs, ssem, rsem):
        self.pos, self.plus, self.minus = pos, plus, minus
        self.sb, self.rb = bufs
        self.ssem, self.rsem = ssem, rsem
        self.used = []

    def copy(self, i, dev):
        return rcopy(self.sb.at[i], self.rb.at[i], self.ssem.at[i], self.rsem.at[i], dev)

    def send(self, i, dev, value):
        self.sb[i] = value.astype(BF16)
        self.copy(i, dev).start()
        self.used.append((i, dev))

    def got(self, i):
        self.copy(i, self.plus).wait_recv()
        return self.rb[i].astype(F32)

    def start(self, part):
        p = self.pos
        self.send(0, self.plus, part((p + 2) % 4, 0))
        self.send(1, self.minus, part((p + 2) % 4, 1))

    def near(self, part):
        p = self.pos
        self.send(3, self.plus, part((p + 1) % 4, 1))
        self.send(4, self.minus, part((p + 3) % 4, 0))

    def middle(self, part):
        p = self.pos
        self.send(2, self.plus, part((p + 1) % 4, 0) + self.got(0))
        self.send(5, self.minus, part((p + 3) % 4, 1) + self.got(1))

    def end(self, part):
        p = self.pos
        first = part(p, 0) + self.got(2) + self.got(4)
        second = part(p, 1) + self.got(3) + self.got(5)
        return first, second

    def drain(self):
        for i, dev in self.used:
            self.copy(i, dev).wait_send()


class Gather:
    def __init__(self, h, kv_ref, where, ssem, rsem, psend, precv):
        self.h, self.kv_ref, self.where = h, kv_ref, where
        self.ssem, self.rsem, self.psend, self.precv = ssem, rsem, psend, precv
        self.kv, self.tp, self.z, self.y, self.c = where
        self.partner = (self.kv + 1 - 2 * self.c, self.tp)
        self.sends = []
        self.shares = []

    def at(self, a, b):
        dz, dy = (b, a) if self.h == 0 else (a, b)
        return ((self.z + dz) % 4) * 8 + ((self.y + dy) % 4) * 2 + self.c

    def ref(self, a, b, part, shift=0):
        lo, n = self.h * HALF, HALF
        if part is not None:
            lo, n = lo + part * QUART, QUART
        return self.kv_ref.at[self.at(a, b) + shift, pl.ds(lo, n)]

    def copy(self, i, a, b, part, to):
        r = self.ref(a, b, part)
        return rcopy(r, r, self.ssem.at[i], self.rsem.at[i], (self.at(*to), self.tp))

    def send(self, *args):
        self.copy(*args).start()
        self.sends.append(args)

    def recv(self, i, a, b, part):
        self.copy(i, a, b, part, (1, 0)).wait_recv()

    def share_copy(self, n, a, b, shift=0):
        r = self.ref(a, b, None, shift)
        return rcopy(r, r, self.psend.at[n], self.precv.at[n], self.partner)

    def share(self, a, b):
        n = len(self.shares)
        self.shares.append((a, b))
        self.share_copy(n, a, b).start()

    def shared(self):
        for n, (a, b) in enumerate(self.shares):
            self.share_copy(n, a, b, 1 - 2 * self.c).wait_recv()

    def drain(self):
        for args in self.sends:
            self.copy(*args).wait_send()
        for n, (a, b) in enumerate(self.shares):
            self.share_copy(n, a, b).wait_send()

    def first(self):
        self.send(0, 0, 0, None, (1, 0))
        self.send(1, 0, 0, None, (-1, 0))

    def own(self):
        self.second_start(0, 0)
        self.share(0, 0)

    def second_start(self, q, a):
        self.send(4 + 4 * q, a, 0, None, (0, 1))
        self.send(5 + 4 * q, a, 0, None, (0, -1))

    def second_forward(self, q, a):
        self.recv(4 + 4 * q, a, -1, None)
        self.send(6 + 4 * q, a, -1, 0, (0, 1))
        self.recv(5 + 4 * q, a, 1, None)
        self.send(7 + 4 * q, a, 1, 1, (0, -1))
        self.share(a, -1)
        self.share(a, 1)

    def second_end(self, q, a):
        self.recv(6 + 4 * q, a, 2, 0)
        self.recv(7 + 4 * q, a, 2, 1)
        self.share(a, 2)

    def first_forward(self):
        self.recv(0, -1, 0, None)
        self.send(2, -1, 0, 0, (1, 0))
        self.second_start(1, -1)
        self.recv(1, 1, 0, None)
        self.send(3, 1, 0, 1, (-1, 0))
        self.second_start(2, 1)
        self.share(-1, 0)
        self.share(1, 0)

    def first_end(self):
        self.recv(2, 2, 0, 0)
        self.recv(3, 2, 0, 1)
        self.second_start(3, 2)
        self.share(2, 0)


def gather_steps(pair):
    def each(*calls):
        def run():
            for name, *args in calls:
                for g in pair:
                    getattr(g, name)(*args)

        return run

    return [
        each(("first",), ("own",)),
        each(("first_forward",)),
        each(("second_forward", 0, 0), ("first_end",)),
        each(("second_forward", 1, -1), ("second_forward", 2, 1), ("second_end", 0, 0)),
        each(("second_forward", 3, 2), ("second_end", 1, -1), ("second_end", 2, 1)),
        each(("second_end", 3, 2), ("shared",)),
    ]


class Reduce:
    def __init__(self, table, mate, acc, abufs, bbufs, where, s_mate, r_mate, s_ring, r_ring):
        self.table, self.mate, self.acc = table, mate, acc
        self.kv, self.tp, self.z, self.y, self.c = where
        self.s_mate, self.r_mate = s_mate, r_mate
        kv, tp, z, y, c = where
        self.partner = (kv + 1 - 2 * c, tp)

        def to(dz, dy):
            return (((z + dz) % 4) * 8 + ((y + dy) % 4) * 2 + c, tp)

        ydir = (y, to(0, 1), to(0, 3))
        zdir = (z, to(1, 0), to(3, 0))
        self.ra = [
            Ring(*(ydir if h == 0 else zdir), [b.at[h] for b in abufs], s_ring.at[h], r_ring.at[h])
            for h in range(2)
        ]
        self.rb = [
            Ring(*(zdir if h == 0 else ydir), [b.at[h] for b in bbufs], s_ring.at[2 + h], r_ring.at[2 + h])
            for h in range(2)
        ]

    def mate_copy(self, h, g):
        rows = pl.ds(h * HALF, HALF)
        if h == 0:
            src = self.table.at[:, (self.y + g) % 4, 1 - self.c, rows]
            dst = self.mate.at[:, (self.y + g) % 4, rows]
        else:
            src = self.table.at[(self.z + g) % 4, :, 1 - self.c, rows]
            dst = self.mate.at[(self.z + g) % 4, :, rows]
        return rcopy(src, dst, self.s_mate.at[h * 4 + g], self.r_mate.at[h * 4 + g], self.partner)

    def part_a(self, h):
        rows = slice(h * HALF, (h + 1) * HALF)

        def part(d, q):
            if h == 0:
                a = self.table[2 * q : 2 * q + 2, d, self.c, rows]
                b = self.mate[2 * q : 2 * q + 2, d, rows]
            else:
                a = self.table[d, 2 * q : 2 * q + 2, self.c, rows]
                b = self.mate[d, 2 * q : 2 * q + 2, rows]
            return a.astype(F32) + b.astype(F32)

        return part

    def part_b(self, h):
        def part(d, q):
            return self.acc[h, d, q * QUART : (q + 1) * QUART]

        return part

    def begin(self):
        for h in range(2):
            self.mate_copy(h, 2).wait_recv()
            self.ra[h].start(self.part_a(h))
        for h in range(2):
            self.mate_copy(h, 1).wait_recv()
            self.mate_copy(h, 3).wait_recv()
            self.ra[h].near(self.part_a(h))

    def middle(self):
        for h in range(2):
            self.ra[h].middle(self.part_a(h))

    def turn(self):
        for h in range(2):
            self.mate_copy(h, 0).wait_recv()
            first, second = self.ra[h].end(self.part_a(h))
            self.acc[h, 0:2] = first
            self.acc[h, 2:4] = second
            self.rb[h].start(self.part_b(h))
            self.rb[h].near(self.part_b(h))

    def middle_b(self):
        for h in range(2):
            self.rb[h].middle(self.part_b(h))

    def finish(self, out):
        for h in range(2):
            for q, value in enumerate(self.rb[h].end(self.part_b(h))):
                lo = h * HALF + q * QUART
                out[lo : lo + QUART] = value

    def drain(self):
        for h in range(2):
            for g in range(4):
                self.mate_copy(h, g).wait_send()
            self.ra[h].drain()
            self.rb[h].drain()


def whole_kernel(
    ids_hbm, k_hbm, v_hbm, gate_hbm, q_hbm, g_hbm, x_hbm,
    dq_ref, kg_ref, vg_ref, wg_ref,
    kv0, kv1, table0, table1, mate0, mate1, acc0, acc1, sa0, ra0, sa1, ra1, sb0, rb0, sb1, rb1,
    ids_ref, inv_ref, inv_v, k_ref, v_ref, gate_ref, q_in, g_in, x_in, gates_t, rows_all, kvbuf_a, kvbuf_b, scores_a, scores_b, packed_a, packed_b, picks, final,
    li_t, li_in, vsend, vland, rhs, w_out, w_own, w_mate, wsend, wland,
    l_sem, ag_s, ag_r, agp_s, agp_r, s_mate, r_mate, s_ring, r_ring, s_li, r_li, s_x, r_x, s_w, r_w, s_d, r_d,
):
    where = place()
    kv, tp, z, y, c = where
    other = 1 - c
    nrow = HEADS * BLK

    def zy(z_, y_):
        return ((z_ % 4) * 8 + (y_ % 4) * 2 + c, tp)

    partner = (kv + 1 - 2 * c, tp)
    xs = [(kv, (tp + d) % 4) for d in (1, 2, 3)]
    offsets = [(dz, dy) for dz in (2, 1, 3, 0) for dy in (2, 1, 3, 0)][:-1]
    kvs, tables = (kv0, kv1), (table0, table1)
    kvbufs, score_bufs, packs = (kvbuf_a, kvbuf_b), (scores_a, scores_b), (packed_a, packed_b)

    pairs = ((k_hbm, k_ref), (v_hbm, v_ref), (x_hbm, x_in), (q_hbm, q_in), (g_hbm, g_in), (gate_hbm, gate_ref), (ids_hbm, ids_ref))
    local = [pltpu.make_async_copy(a, b, l_sem.at[n]) for n, (a, b) in enumerate(pairs)]
    for d in local:
        d.start()
    peers = [partner] + xs + [zy(z + dz, y + dy) for dz, dy in offsets]
    barrier = pltpu.get_barrier_semaphore()
    for peer in peers:
        pl.semaphore_signal(barrier, inc=1, device_id=peer, device_id_type=MESH)
    local[0].wait()
    local[1].wait()
    for s in range(SEQS):
        kvs[s][kv] = jnp.concatenate([k_ref[s], v_ref[s]], axis=0).T
    pl.semaphore_wait(barrier, len(peers))

    gathers = [
        [Gather(h, kvs[s], where, ag_s.at[s, h], ag_r.at[s, h], agp_s.at[s, h], agp_r.at[s, h]) for h in range(2)]
        for s in range(SEQS)
    ]
    steps = [gather_steps(pair) for pair in gathers]
    reduces = [
        Reduce(
            tables[s], (mate0, mate1)[s], (acc0, acc1)[s],
            ((sa0, ra0), (sa1, ra1))[s], ((sb0, rb0), (sb1, rb1))[s],
            where, s_mate.at[s], r_mate.at[s], s_ring.at[s], r_ring.at[s],
        )
        for s in range(SEQS)
    ]

    def turn_input(i, carry):
        lo = pl.multiple_of(i * 512, 512)
        for s in range(SEQS):
            t = x_in[s, :, pl.ds(lo, 512)].T.reshape(2, 2, 4, 32, 96)
            for n in range(4):
                li_t[n, pl.ds(i * 2, 2), :, :, s * 96 : (s + 1) * 96] = t[:, :, n]
        return carry

    def li_copy(n):
        to = (tp + n + 1) % 4
        return rcopy(li_t.at[to], li_in.at[tp], s_li.at[n], r_li.at[n], (kv, to))

    def prepare(s, qb):
        lane = lax.broadcasted_iota(jnp.int32, (BLK, 2 * HD), 1)
        low = lane < HD
        rows = pl.ds(pl.multiple_of(qb * BLK, BLK), BLK)
        gates = gates_t[s, rows]
        at = s * BPD + qb
        for h in range(HEADS):
            pair = slice((h // 2) * 128, (h // 2) * 128 + 128)
            qv = q_in[s, rows, pair].astype(F32) * 0.125
            gv = gates[:, h : h + 1] * g_in[s, rows, pair].astype(F32)
            if h % 2 == 0:
                gv = pltpu.roll(gv, HD, 1)
            else:
                qv = pltpu.roll(qv, HD, 1)
            rows_all[at, h * BLK : (h + 1) * BLK] = jnp.where(low, qv, 0.0).astype(BF16)
            rows_all[at, nrow + h * BLK : nrow + (h + 1) * BLK] = jnp.where(low, 0.0, gv).astype(BF16)

    def begin_block(s, qb, slot):
        kvbuf, scores = kvbufs[slot], score_bufs[slot]
        at = s * BPD + qb
        kv_ref = kvs[s]
        picked = [ids_ref[s, qb, 0, k] for k in range(TOPK)]
        for k in range(TOPK):
            kvbuf[k * BLK : (k + 1) * BLK] = kv_ref[picked[k] // BPD, pl.ds((picked[k] % BPD) * BLK, BLK)]
        scores[...] = lax.dot_general(
            kvbuf[...], rows_all[at], (((1,), (1,)), ((), ())), preferred_element_type=F32
        )
        return picked

    def end_block(s, qb, slot, picked):
        kvbuf, scores, packed = kvbufs[slot], score_bufs[slot], packs[slot]
        at = s * BPD + qb
        block = kv * BPD + qb
        qpos = block * BLK + lax.broadcasted_iota(jnp.int32, (BLK, nrow), 1) % BLK
        ahead = lax.broadcasted_iota(jnp.int32, (BLK, nrow), 0) - qpos

        def masked(k):
            sc = scores[k * BLK : (k + 1) * BLK, :nrow]
            return jnp.where(ahead <= -(picked[k] * BLK), sc, NEG)

        top = None
        for k in range(TOPK):
            m = jnp.max(masked(k).reshape(8, 8, nrow), axis=0)
            top = m if top is None else jnp.maximum(top, m)
        top = jnp.max(top, axis=0, keepdims=True)
        total = jnp.zeros((8, nrow), F32)
        for k in range(TOPK):
            e = jnp.exp(masked(k) - top)
            scores[k * BLK : (k + 1) * BLK, :nrow] = e
            total = total + jnp.sum(e.reshape(8, 8, nrow), axis=0)
        scale = 1.0 / jnp.sum(total, axis=0, keepdims=True)
        dot = jnp.zeros((8, nrow), F32)
        for k in range(TOPK):
            rows = slice(k * BLK, (k + 1) * BLK)
            w = (scores[rows, :nrow] * scale).astype(BF16)
            packed[rows, nrow:] = w
            t = w.astype(F32) * scores[rows, nrow:]
            dot = dot + jnp.sum(t.reshape(8, 8, nrow), axis=0)
        row_dot = jnp.sum(dot, axis=0, keepdims=True)
        for k in range(TOPK):
            rows = slice(k * BLK, (k + 1) * BLK)
            ds = (scores[rows, :nrow] * scale) * (scores[rows, nrow:] - row_dot)
            packed[rows, :nrow] = ds.astype(BF16)
        pick = jnp.dot(packed[...], rows_all[at], preferred_element_type=F32)
        picks[pl.ds(qb * TOPK, TOPK)] = pick.reshape(TOPK, BLK, 2 * HD)
        dq_t = jnp.dot(kvbuf[...].T, packed[:, :nrow], preferred_element_type=F32)
        dq = (dq_t[:HD] * 0.125).T
        dq_ref[s, pl.ds(pl.multiple_of(qb * BLK, BLK), BLK)] = jnp.concatenate(
            [dq[h * BLK : (h + 1) * BLK] for h in range(HEADS)], axis=1
        ).astype(BF16)

    def attend(s, pair):
        blocks = (2 * pair, 2 * pair + 1)
        ids = [begin_block(s, qb, slot) for slot, qb in enumerate(blocks)]
        for slot, qb in enumerate(blocks):
            end_block(s, qb, slot, ids[slot])

    def collect(s):
        table = tables[s]

        def made(zz, yy, cc, b):
            col = (zz * 8 + yy * 2 + cc) * BPD + b
            total = picks[inv_ref[s * BPD, col]]
            for q in range(1, BPD):
                total = total + picks[inv_ref[s * BPD + q, col]]
            table[zz, yy, cc, b * BLK : (b + 1) * BLK] = total.astype(BF16)

        for g in (2, 1, 3, 0):

            def one(i, carry, g=g):
                for b in range(BPD // 2):
                    made(i // 2, (y + g) % 4, i % 2, b)
                    made((z + g) % 4, i // 2, i % 2, BPD // 2 + b)
                return carry

            lax.fori_loop(0, 8, one, 0)
            for h in range(2):
                reduces[s].mate_copy(h, g).start()

    quarter = ROWS // 4

    def x_copy(s, n):
        to = (tp + n + 1) % 4
        return rcopy(vsend.at[s], vland.at[s, tp], s_x.at[s, n], r_x.at[s, n], (kv, to))

    def finish(s):
        reduces[s].finish(final)
        lane = lax.broadcasted_iota(jnp.int32, (HALF, 2 * HD), 1)
        low = pltpu.roll(final[0:HALF].astype(BF16).astype(F32), HD, 1)
        value = jnp.where(lane < HD, low, final[HALF:]).astype(BF16)
        vsend[s] = value
        vland[s, tp] = value
        for n in (1, 0, 2):
            x_copy(s, n).start()
        turned = final[...].T
        kg_ref[s] = turned[:HD].astype(BF16)
        vg_ref[s] = turned[HD:].astype(BF16)

    def landed(s):
        for n in range(3):
            frm = (tp + 3 - n) % 4
            slot = vland.at[s, frm]
            rcopy(slot, slot, s_x.at[s, n], r_x.at[s, n], (kv, frm)).wait_recv()
        lane = lax.broadcasted_iota(jnp.int32, (quarter, 2 * HD), 1)
        for t in range(4):
            rows = slice((t % 2) * quarter, (t % 2 + 1) * quarter)
            for p in range(2):
                even = vland[s, 2 * p, rows].astype(F32)
                odd = vland[s, 2 * p + 1, rows].astype(F32)
                if t < 2:
                    odd = pltpu.roll(odd, HD, 1)
                else:
                    even = pltpu.roll(even, HD, 1)
                rhs[t, s * quarter : (s + 1) * quarter, p * 128 : (p + 1) * 128] = jnp.where(
                    lane < HD, even, odd
                ).astype(BF16)

    steps[0][0]()
    local[6].wait()
    spot = lax.broadcasted_iota(jnp.int32, (1, 256), 1)
    for s in range(SEQS):
        for qb in range(BPD):
            slot = jnp.full((1, 256), BPD * TOPK, jnp.int32)
            for k in range(TOPK):
                slot = jnp.where(spot == ids_ref[s, qb, 0, k], qb * TOPK + k, slot)
            inv_v[s * BPD + qb : s * BPD + qb + 1] = slot
    to_scalar = pltpu.make_async_copy(inv_v, inv_ref, l_sem.at[8])
    to_scalar.start()
    local[2].wait()
    lax.fori_loop(0, 4, turn_input, 0)
    steps[0][1]()
    steps[1][0]()
    lax.fori_loop(4, 8, turn_input, 0)
    for n in (1, 0, 2):
        li_copy(n).start()
    for n in (3, 4, 5):
        local[n].wait()
    for s in range(SEQS):
        gates_t[s] = jax.nn.sigmoid(gate_ref[s]).T
    to_scalar.wait()
    picks[BPD * TOPK] = jnp.zeros((BLK, 2 * HD), F32)
    for n in range(2, 5):
        steps[0][n]()
        if n != 3:
            steps[1][n // 2]()

        def some(i, carry, n=n):
            at = (n - 2) * 4 + i
            prepare(at // BPD, at % BPD)
            return carry

        lax.fori_loop(0, 4, some, 0)
    steps[0][5]()

    def between(n, step):
        def at(qb):
            @pl.when(qb == n)
            def _():
                step()

        return at

    marks = [between(0, steps[1][3]), between(1, steps[1][4]), between(2, steps[1][5])]

    def attend0(qb, carry):
        attend(0, qb)
        for mark in marks:
            mark(qb)
        return carry

    lax.fori_loop(0, BPD // 2, attend0, 0)
    collect(0)

    marks1 = [between(1, reduces[0].begin), between(2, reduces[0].middle)]

    def attend1(qb, carry):
        attend(1, qb)
        for mark in marks1:
            mark(qb)
        return carry

    lax.fori_loop(0, BPD // 2, attend1, 0)
    collect(1)
    reduces[1].begin()
    reduces[0].turn()
    reduces[1].middle()
    reduces[0].middle_b()
    reduces[1].turn()
    finish(0)
    reduces[1].middle_b()
    landed(0)
    finish(1)
    for n in range(3):
        frm = (tp + 3 - n) % 4
        rcopy(li_in.at[frm], li_in.at[frm], s_li.at[n], r_li.at[n], (kv, frm)).wait_recv()
    mine_li = pltpu.make_async_copy(li_t.at[tp], li_in.at[tp], l_sem.at[7])
    mine_li.start()
    mine_li.wait()
    landed(1)

    def product(side, i):
        total = None
        for t in range(4):
            a = li_in[t, pl.ds(i * 4, 4), side].reshape(128, 192)
            p = jnp.dot(a, rhs[t], preferred_element_type=F32)
            total = p if total is None else total + p
        return total.reshape(4, 32, 256)

    order = (2, 1, 3, 0)
    mine = kv // 2

    def piece(dz):
        return pl.ds(((z + dz) % 4) * 4, 4)

    def w_copy(dz):
        rows = piece(dz)
        return rcopy(w_out.at[rows], w_mate.at[rows], s_w.at[dz], r_w.at[dz], partner)

    def d_copy(n):
        dz, dy = offsets[n]
        to = zy(z + dz, y + dy)
        return rcopy(wsend.at[to[0] // 2], wland.at[mine], s_d.at[n], r_d.at[n], to)

    for dz in order:
        w_out[piece(dz)] = product(other, (z + dz) % 4).astype(BF16)
        w_copy(dz).start()
    for dz in order:
        w_own[piece(dz)] = product(c, (z + dz) % 4)
    for dz in order:
        w_copy(dz).wait_recv()
        value = w_own[piece(dz)] + w_mate[piece(dz)].astype(F32)
        w_own[piece(dz)] = value
        wsend[piece(dz)] = value.astype(BF16)
        for n in range(len(offsets)):
            if offsets[n][0] == dz:
                d_copy(n).start()
    total = w_own[mine]
    for n, (dz, dy) in enumerate(offsets):
        frm = zy(z - dz, y - dy)
        slot = wland.at[frm[0] // 2]
        rcopy(slot, slot, s_d.at[n], r_d.at[n], frm).wait_recv()
        total = total + wland[frm[0] // 2].astype(F32)
    wg_ref[...] = total

    for pair in gathers:
        for g in pair:
            g.drain()
    for r in reduces:
        r.drain()
    for n in range(3):
        li_copy(n).wait_send()
        for s in range(SEQS):
            x_copy(s, n).wait_send()
    for dz in order:
        w_copy(dz).wait_send()
    for n in range(len(offsets)):
        d_copy(n).wait_send()


def whole(chosen, keys, values, gates, queries, cotangent, layer_input):
    v = pltpu.VMEM
    dma = pltpu.SemaphoreType.DMA
    wide = 2 * HD
    anywhere = pl.BlockSpec(memory_space=pltpu.HBM)
    onchip = pl.BlockSpec(memory_space=v)
    keys_n = TOPK * BLK
    nrow = HEADS * BLK
    return pl.pallas_call(
        whole_kernel,
        out_shape=[
            jax.ShapeDtypeStruct((SEQS, ROWS, HEADS * HD), BF16),
            jax.ShapeDtypeStruct((SEQS, HD, ROWS), BF16),
            jax.ShapeDtypeStruct((SEQS, HD, ROWS), BF16),
            jax.ShapeDtypeStruct((32, 256), F32),
        ],
        in_specs=[anywhere] * 7,
        out_specs=[onchip] * 4,
        scratch_shapes=[
            *[v((DEVS, ROWS, wide), BF16) for _ in range(2)],
            *[v((ZN, YN, 2, ROWS, wide), BF16) for _ in range(2)],
            *[v((ZN, YN, ROWS, wide), BF16) for _ in range(2)],
            *[v((2, 4, HALF, wide), F32) for _ in range(2)],
            *[v((2, 6, 2, HALF, wide), BF16) for _ in range(4)],
            *[v((2, 6, QUART, wide), BF16) for _ in range(4)],
            pltpu.SMEM((SEQS, BPD, 1, TOPK), jnp.int32),
            pltpu.SMEM((SEQS * BPD, 256), jnp.int32),
            v((SEQS * BPD, 256), jnp.int32),
            v((SEQS, HD, ROWS), BF16),
            v((SEQS, HD, ROWS), BF16),
            v((SEQS, HEADS, ROWS), F32),
            v((SEQS, ROWS, HEADS * HD), BF16),
            v((SEQS, ROWS, HEADS * HD), BF16),
            v((SEQS, ROWS // 4, 4096), BF16),
            v((SEQS, ROWS, HEADS), F32),
            v((SEQS * BPD, 2 * nrow, wide), BF16),
            *[v((keys_n, wide), BF16) for _ in range(2)],
            *[v((keys_n, 2 * nrow), F32) for _ in range(2)],
            *[v((keys_n, 2 * nrow), BF16) for _ in range(2)],
            v((BPD * TOPK + 1, BLK, wide), F32),
            v((ROWS, wide), F32),
            v((4, 16, 2, 32, 192), BF16),
            v((4, 16, 2, 32, 192), BF16),
            v((SEQS, HALF, wide), BF16),
            v((SEQS, 4, HALF, wide), BF16),
            v((4, 192, 256), BF16),
            v((16, 32, 256), BF16),
            v((16, 32, 256), F32),
            v((16, 32, 256), BF16),
            v((16, 32, 256), BF16),
            v((16, 32, 256), BF16),
            dma((9,)),
            *[dma((2, 2, 20)) for _ in range(2)],
            *[dma((2, 2, 16)) for _ in range(2)],
            *[dma((2, 8)) for _ in range(2)],
            *[dma((2, 4, 6)) for _ in range(2)],
            *[dma((3,)) for _ in range(2)],
            *[dma((2, 3)) for _ in range(2)],
            *[dma((4,)) for _ in range(2)],
            *[dma((15,)) for _ in range(2)],
        ],
        compiler_params=pltpu.CompilerParams(
            collective_id=0, has_side_effects=True, vmem_limit_bytes=48 * 2**20
        ),
        name="whole",
    )(
        *[
            pltpu.with_memory_space_constraint(a, pltpu.HBM)
            for a in (chosen, keys, values, gates, queries, cotangent, layer_input)
        ],
    )


def on_device(queries, key_states, value_states, cotangent, gate_logits, layer_input, chosen):
    def turned(a):
        return jnp.swapaxes(a, 1, 2)

    query_grad, key_grad, value_grad, weight_grad = whole(
        chosen, turned(key_states), turned(value_states), turned(gate_logits),
        queries, cotangent, layer_input,
    )
    return query_grad, turned(key_grad), turned(value_grad), weight_grad


def solution(mesh):
    placed = (
        P(None, "kv", "tp"),
        P(None, "kv", "tp"),
        P(None, "kv", "tp"),
        P(None, "kv", "tp"),
        P(None, "kv", "tp"),
        P(None, ("kv", "tp"), None),
        P(None, "kv", "tp", None),
    )
    return jax.shard_map(
        on_device,
        mesh=mesh,
        in_specs=placed,
        out_specs=(P(None, "kv", "tp"), P(None, "kv", "tp"), P(None, "kv", "tp"), P(("kv", "tp"), None)),
        check_vma=False,
    )
```

```python
import jax
import jax.numpy as jnp
from jax import lax
from jax.experimental import pallas as pl
from jax.experimental.pallas import tpu as pltpu
from jax.sharding import PartitionSpec as P

BLK = 64
MESH = pl.DeviceIdType.MESH
F32 = jnp.float32
BF16 = jnp.bfloat16
SEQS = 2
BPD = 6
ROWS = BPD * BLK
ZN = 4
YN = 4
DEVS = ZN * YN * 2
HD = 64
HEADS = 4
TOPK = 16
NEG = -1e30
HALF = ROWS // 2
QUART = ROWS // 4


def place():
    kv = lax.axis_index("kv")
    tp = lax.axis_index("tp")
    z, y, c = kv // 8, (kv // 2) % 4, kv % 2
    return kv, tp, z, y, c


def rcopy(src, dst, ssem, rsem, device):
    return pltpu.make_async_remote_copy(
        src_ref=src, dst_ref=dst, send_sem=ssem, recv_sem=rsem, device_id=device, device_id_type=MESH
    )


def entry_barrier(peers):
    sem = pltpu.get_barrier_semaphore()
    for peer in peers:
        pl.semaphore_signal(sem, inc=1, device_id=peer, device_id_type=MESH)
    pl.semaphore_wait(sem, len(peers))


class Ring:
    def __init__(self, pos, plus, minus, bufs, ssem, rsem):
        self.pos, self.plus, self.minus = pos, plus, minus
        self.sb, self.rb = bufs
        self.ssem, self.rsem = ssem, rsem
        self.used = []

    def copy(self, i, dev):
        return rcopy(self.sb.at[i], self.rb.at[i], self.ssem.at[i], self.rsem.at[i], dev)

    def send(self, i, dev, value):
        self.sb[i] = value.astype(BF16)
        self.copy(i, dev).start()
        self.used.append((i, dev))

    def got(self, i):
        self.copy(i, self.plus).wait_recv()
        return self.rb[i].astype(F32)

    def start(self, part):
        p = self.pos
        self.send(0, self.plus, part((p + 2) % 4, 0))
        self.send(1, self.minus, part((p + 2) % 4, 1))

    def near(self, part):
        p = self.pos
        self.send(3, self.plus, part((p + 1) % 4, 1))
        self.send(4, self.minus, part((p + 3) % 4, 0))

    def middle(self, part):
        p = self.pos
        self.send(2, self.plus, part((p + 1) % 4, 0) + self.got(0))
        self.send(5, self.minus, part((p + 3) % 4, 1) + self.got(1))

    def end(self, part):
        p = self.pos
        first = part(p, 0) + self.got(2) + self.got(4)
        second = part(p, 1) + self.got(3) + self.got(5)
        return first, second

    def drain(self):
        for i, dev in self.used:
            self.copy(i, dev).wait_send()


class Gather:
    def __init__(self, h, kv_ref, where, ssem, rsem, psend, precv):
        self.h, self.kv_ref, self.where = h, kv_ref, where
        self.ssem, self.rsem, self.psend, self.precv = ssem, rsem, psend, precv
        self.kv, self.tp, self.z, self.y, self.c = where
        self.partner = (self.kv + 1 - 2 * self.c, self.tp)
        self.sends = []
        self.shares = []

    def at(self, a, b):
        dz, dy = (b, a) if self.h == 0 else (a, b)
        return ((self.z + dz) % 4) * 8 + ((self.y + dy) % 4) * 2 + self.c

    def ref(self, a, b, part, shift=0):
        lo, n = self.h * HALF, HALF
        if part is not None:
            lo, n = lo + part * QUART, QUART
        return self.kv_ref.at[self.at(a, b) + shift, pl.ds(lo, n)]

    def copy(self, i, a, b, part, to):
        r = self.ref(a, b, part)
        return rcopy(r, r, self.ssem.at[i], self.rsem.at[i], (self.at(*to), self.tp))

    def send(self, *args):
        self.copy(*args).start()
        self.sends.append(args)

    def recv(self, i, a, b, part):
        self.copy(i, a, b, part, (1, 0)).wait_recv()

    def share_copy(self, n, a, b, shift=0):
        r = self.ref(a, b, None, shift)
        return rcopy(r, r, self.psend.at[n], self.precv.at[n], self.partner)

    def share(self, a, b):
        n = len(self.shares)
        self.shares.append((a, b))
        self.share_copy(n, a, b).start()

    def shared(self):
        for n, (a, b) in enumerate(self.shares):
            self.share_copy(n, a, b, 1 - 2 * self.c).wait_recv()

    def drain(self):
        for args in self.sends:
            self.copy(*args).wait_send()
        for n, (a, b) in enumerate(self.shares):
            self.share_copy(n, a, b).wait_send()

    def first(self):
        self.send(0, 0, 0, None, (1, 0))
        self.send(1, 0, 0, None, (-1, 0))

    def own(self):
        self.second_start(0, 0)
        self.share(0, 0)

    def second_start(self, q, a):
        self.send(4 + 4 * q, a, 0, None, (0, 1))
        self.send(5 + 4 * q, a, 0, None, (0, -1))

    def second_forward(self, q, a):
        self.recv(4 + 4 * q, a, -1, None)
        self.send(6 + 4 * q, a, -1, 0, (0, 1))
        self.recv(5 + 4 * q, a, 1, None)
        self.send(7 + 4 * q, a, 1, 1, (0, -1))
        self.share(a, -1)
        self.share(a, 1)

    def second_end(self, q, a):
        self.recv(6 + 4 * q, a, 2, 0)
        self.recv(7 + 4 * q, a, 2, 1)
        self.share(a, 2)

    def first_forward(self):
        self.recv(0, -1, 0, None)
        self.send(2, -1, 0, 0, (1, 0))
        self.second_start(1, -1)
        self.recv(1, 1, 0, None)
        self.send(3, 1, 0, 1, (-1, 0))
        self.second_start(2, 1)
        self.share(-1, 0)
        self.share(1, 0)

    def first_end(self):
        self.recv(2, 2, 0, 0)
        self.recv(3, 2, 0, 1)
        self.second_start(3, 2)
        self.share(2, 0)


def gather_steps(pair):
    def each(*calls):
        def run():
            for name, *args in calls:
                for g in pair:
                    getattr(g, name)(*args)

        return run

    return [
        each(("first",), ("own",)),
        each(("first_forward",)),
        each(("second_forward", 0, 0), ("first_end",)),
        each(("second_forward", 1, -1), ("second_forward", 2, 1), ("second_end", 0, 0)),
        each(("second_forward", 3, 2), ("second_end", 1, -1), ("second_end", 2, 1)),
        each(("second_end", 3, 2), ("shared",)),
    ]


class Reduce:
    def __init__(self, table, mate, acc, abufs, bbufs, where, s_mate, r_mate, s_ring, r_ring):
        self.table, self.mate, self.acc = table, mate, acc
        self.kv, self.tp, self.z, self.y, self.c = where
        self.s_mate, self.r_mate = s_mate, r_mate
        kv, tp, z, y, c = where
        self.partner = (kv + 1 - 2 * c, tp)

        def to(dz, dy):
            return (((z + dz) % 4) * 8 + ((y + dy) % 4) * 2 + c, tp)

        ydir = (y, to(0, 1), to(0, 3))
        zdir = (z, to(1, 0), to(3, 0))
        self.ra = [
            Ring(*(ydir if h == 0 else zdir), [b.at[h] for b in abufs], s_ring.at[h], r_ring.at[h])
            for h in range(2)
        ]
        self.rb = [
            Ring(*(zdir if h == 0 else ydir), [b.at[h] for b in bbufs], s_ring.at[2 + h], r_ring.at[2 + h])
            for h in range(2)
        ]

    def mate_copy(self, h, g):
        rows = pl.ds(h * HALF, HALF)
        if h == 0:
            src = self.table.at[:, (self.y + g) % 4, 1 - self.c, rows]
            dst = self.mate.at[:, (self.y + g) % 4, rows]
        else:
            src = self.table.at[(self.z + g) % 4, :, 1 - self.c, rows]
            dst = self.mate.at[(self.z + g) % 4, :, rows]
        return rcopy(src, dst, self.s_mate.at[h * 4 + g], self.r_mate.at[h * 4 + g], self.partner)

    def part_a(self, h):
        rows = slice(h * HALF, (h + 1) * HALF)

        def part(d, q):
            if h == 0:
                a = self.table[2 * q : 2 * q + 2, d, self.c, rows]
                b = self.mate[2 * q : 2 * q + 2, d, rows]
            else:
                a = self.table[d, 2 * q : 2 * q + 2, self.c, rows]
                b = self.mate[d, 2 * q : 2 * q + 2, rows]
            return a.astype(F32) + b.astype(F32)

        return part

    def part_b(self, h):
        def part(d, q):
            return self.acc[h, d, q * QUART : (q + 1) * QUART]

        return part

    def begin(self):
        for h in range(2):
            self.mate_copy(h, 2).wait_recv()
            self.ra[h].start(self.part_a(h))
        for h in range(2):
            self.mate_copy(h, 1).wait_recv()
            self.mate_copy(h, 3).wait_recv()
            self.ra[h].near(self.part_a(h))

    def middle(self):
        for h in range(2):
            self.ra[h].middle(self.part_a(h))

    def turn(self):
        for h in range(2):
            self.mate_copy(h, 0).wait_recv()
            first, second = self.ra[h].end(self.part_a(h))
            self.acc[h, 0:2] = first
            self.acc[h, 2:4] = second
            self.rb[h].start(self.part_b(h))
            self.rb[h].near(self.part_b(h))

    def middle_b(self):
        for h in range(2):
            self.rb[h].middle(self.part_b(h))

    def finish(self, out):
        for h in range(2):
            for q, value in enumerate(self.rb[h].end(self.part_b(h))):
                lo = h * HALF + q * QUART
                out[lo : lo + QUART] = value

    def drain(self):
        for h in range(2):
            for g in range(4):
                self.mate_copy(h, g).wait_send()
            self.ra[h].drain()
            self.rb[h].drain()


def whole_kernel(
    ids_hbm, k_hbm, v_hbm, gate_hbm, q_hbm, g_hbm, x_hbm,
    dq_ref, kg_ref, vg_ref, wg_ref,
    kv0, kv1, table0, table1, mate0, mate1, acc0, acc1, sa0, ra0, sa1, ra1, sb0, rb0, sb1, rb1,
    ids_ref, inv_ref, inv_v, k_ref, v_ref, gate_ref, q_in, g_in, x_in, gates_t, rows_all, kvbuf_a, kvbuf_b, kvbuf_c, scores_a, scores_b, scores_c, packed_a, packed_b, packed_c, picks, final,
    li_t, li_in, vsend, vland, rhs, w_out, w_own, w_mate, wsend, wland,
    l_sem, ag_s, ag_r, agp_s, agp_r, s_mate, r_mate, s_ring, r_ring, s_li, r_li, s_x, r_x, s_w, r_w, s_d, r_d,
):
    where = place()
    kv, tp, z, y, c = where
    other = 1 - c
    nrow = HEADS * BLK

    def zy(z_, y_):
        return ((z_ % 4) * 8 + (y_ % 4) * 2 + c, tp)

    partner = (kv + 1 - 2 * c, tp)
    xs = [(kv, (tp + d) % 4) for d in (1, 2, 3)]
    offsets = [(dz, dy) for dz in (2, 1, 3, 0) for dy in (2, 1, 3, 0)][:-1]
    kvs, tables = (kv0, kv1), (table0, table1)
    kvbufs, score_bufs, packs = (kvbuf_a, kvbuf_b, kvbuf_c), (scores_a, scores_b, scores_c), (packed_a, packed_b, packed_c)

    pairs = ((k_hbm, k_ref), (v_hbm, v_ref), (x_hbm, x_in), (q_hbm, q_in), (g_hbm, g_in), (gate_hbm, gate_ref), (ids_hbm, ids_ref))
    local = [pltpu.make_async_copy(a, b, l_sem.at[n]) for n, (a, b) in enumerate(pairs)]
    for d in local:
        d.start()
    peers = [partner] + xs + [zy(z + dz, y + dy) for dz, dy in offsets]
    barrier = pltpu.get_barrier_semaphore()
    for peer in peers:
        pl.semaphore_signal(barrier, inc=1, device_id=peer, device_id_type=MESH)
    local[0].wait()
    local[1].wait()
    for s in range(SEQS):
        kvs[s][kv] = jnp.concatenate([k_ref[s], v_ref[s]], axis=0).T
    pl.semaphore_wait(barrier, len(peers))

    gathers = [
        [Gather(h, kvs[s], where, ag_s.at[s, h], ag_r.at[s, h], agp_s.at[s, h], agp_r.at[s, h]) for h in range(2)]
        for s in range(SEQS)
    ]
    steps = [gather_steps(pair) for pair in gathers]
    reduces = [
        Reduce(
            tables[s], (mate0, mate1)[s], (acc0, acc1)[s],
            ((sa0, ra0), (sa1, ra1))[s], ((sb0, rb0), (sb1, rb1))[s],
            where, s_mate.at[s], r_mate.at[s], s_ring.at[s], r_ring.at[s],
        )
        for s in range(SEQS)
    ]

    def turn_input(i, carry):
        lo = pl.multiple_of(i * 512, 512)
        for s in range(SEQS):
            t = x_in[s, :, pl.ds(lo, 512)].T.reshape(2, 2, 4, 32, 96)
            for n in range(4):
                li_t[n, pl.ds(i * 2, 2), :, :, s * 96 : (s + 1) * 96] = t[:, :, n]
        return carry

    def li_copy(n):
        to = (tp + n + 1) % 4
        return rcopy(li_t.at[to], li_in.at[tp], s_li.at[n], r_li.at[n], (kv, to))

    def prepare(s, qb):
        lane = lax.broadcasted_iota(jnp.int32, (BLK, 2 * HD), 1)
        low = lane < HD
        rows = pl.ds(pl.multiple_of(qb * BLK, BLK), BLK)
        gates = gates_t[s, rows]
        at = s * BPD + qb
        for h in range(HEADS):
            pair = slice((h // 2) * 128, (h // 2) * 128 + 128)
            qv = q_in[s, rows, pair].astype(F32) * 0.125
            gv = gates[:, h : h + 1] * g_in[s, rows, pair].astype(F32)
            if h % 2 == 0:
                gv = pltpu.roll(gv, HD, 1)
            else:
                qv = pltpu.roll(qv, HD, 1)
            rows_all[at, h * BLK : (h + 1) * BLK] = jnp.where(low, qv, 0.0).astype(BF16)
            rows_all[at, nrow + h * BLK : nrow + (h + 1) * BLK] = jnp.where(low, 0.0, gv).astype(BF16)

    def begin_block(s, qb, slot):
        kvbuf, scores = kvbufs[slot], score_bufs[slot]
        at = s * BPD + qb
        kv_ref = kvs[s]
        picked = [ids_ref[s, qb, 0, k] for k in range(TOPK)]
        for k in range(TOPK):
            kvbuf[k * BLK : (k + 1) * BLK] = kv_ref[picked[k] // BPD, pl.ds((picked[k] % BPD) * BLK, BLK)]
        scores[...] = lax.dot_general(
            kvbuf[...], rows_all[at], (((1,), (1,)), ((), ())), preferred_element_type=F32
        )
        return picked

    def end_block(s, qb, slot, picked):
        kvbuf, scores, packed = kvbufs[slot], score_bufs[slot], packs[slot]
        at = s * BPD + qb
        block = kv * BPD + qb
        qpos = block * BLK + lax.broadcasted_iota(jnp.int32, (BLK, nrow), 1) % BLK
        ahead = lax.broadcasted_iota(jnp.int32, (BLK, nrow), 0) - qpos

        def masked(k):
            sc = scores[k * BLK : (k + 1) * BLK, :nrow]
            return jnp.where(ahead <= -(picked[k] * BLK), sc, NEG)

        top = None
        for k in range(TOPK):
            m = jnp.max(masked(k).reshape(8, 8, nrow), axis=0)
            top = m if top is None else jnp.maximum(top, m)
        top = jnp.max(top, axis=0, keepdims=True)
        total = jnp.zeros((8, nrow), F32)
        for k in range(TOPK):
            e = jnp.exp(masked(k) - top)
            scores[k * BLK : (k + 1) * BLK, :nrow] = e
            total = total + jnp.sum(e.reshape(8, 8, nrow), axis=0)
        scale = 1.0 / jnp.sum(total, axis=0, keepdims=True)
        dot = jnp.zeros((8, nrow), F32)
        for k in range(TOPK):
            rows = slice(k * BLK, (k + 1) * BLK)
            w = (scores[rows, :nrow] * scale).astype(BF16)
            packed[rows, nrow:] = w
            t = w.astype(F32) * scores[rows, nrow:]
            dot = dot + jnp.sum(t.reshape(8, 8, nrow), axis=0)
        row_dot = jnp.sum(dot, axis=0, keepdims=True)
        for k in range(TOPK):
            rows = slice(k * BLK, (k + 1) * BLK)
            ds = (scores[rows, :nrow] * scale) * (scores[rows, nrow:] - row_dot)
            packed[rows, :nrow] = ds.astype(BF16)
        pick = jnp.dot(packed[...], rows_all[at], preferred_element_type=F32)
        picks[pl.ds(qb * TOPK, TOPK)] = pick.reshape(TOPK, BLK, 2 * HD)
        dq_t = jnp.dot(kvbuf[...].T, packed[:, :nrow], preferred_element_type=F32)
        dq = (dq_t[:HD] * 0.125).T
        dq_ref[s, pl.ds(pl.multiple_of(qb * BLK, BLK), BLK)] = jnp.concatenate(
            [dq[h * BLK : (h + 1) * BLK] for h in range(HEADS)], axis=1
        ).astype(BF16)

    def attend(s, pair):
        blocks = (3 * pair, 3 * pair + 1, 3 * pair + 2)
        ids = [begin_block(s, qb, slot) for slot, qb in enumerate(blocks)]
        for slot, qb in enumerate(blocks):
            end_block(s, qb, slot, ids[slot])

    def collect(s):
        table = tables[s]

        def made(zz, yy, cc, b):
            col = (zz * 8 + yy * 2 + cc) * BPD + b
            total = picks[inv_ref[s * BPD, col]]
            for q in range(1, BPD):
                total = total + picks[inv_ref[s * BPD + q, col]]
            table[zz, yy, cc, b * BLK : (b + 1) * BLK] = total.astype(BF16)

        for g in (2, 1, 3, 0):

            def one(i, carry, g=g):
                for b in range(BPD // 2):
                    made(i // 2, (y + g) % 4, i % 2, b)
                    made((z + g) % 4, i // 2, i % 2, BPD // 2 + b)
                return carry

            lax.fori_loop(0, 8, one, 0)
            for h in range(2):
                reduces[s].mate_copy(h, g).start()

    quarter = ROWS // 4

    def x_copy(s, n):
        to = (tp + n + 1) % 4
        return rcopy(vsend.at[s], vland.at[s, tp], s_x.at[s, n], r_x.at[s, n], (kv, to))

    def finish(s):
        reduces[s].finish(final)
        lane = lax.broadcasted_iota(jnp.int32, (HALF, 2 * HD), 1)
        low = pltpu.roll(final[0:HALF].astype(BF16).astype(F32), HD, 1)
        value = jnp.where(lane < HD, low, final[HALF:]).astype(BF16)
        vsend[s] = value
        vland[s, tp] = value
        for n in (1, 0, 2):
            x_copy(s, n).start()
        turned = final[...].T
        kg_ref[s] = turned[:HD].astype(BF16)
        vg_ref[s] = turned[HD:].astype(BF16)

    def landed(s):
        for n in range(3):
            frm = (tp + 3 - n) % 4
            slot = vland.at[s, frm]
            rcopy(slot, slot, s_x.at[s, n], r_x.at[s, n], (kv, frm)).wait_recv()
        lane = lax.broadcasted_iota(jnp.int32, (quarter, 2 * HD), 1)
        for t in range(4):
            rows = slice((t % 2) * quarter, (t % 2 + 1) * quarter)
            for p in range(2):
                even = vland[s, 2 * p, rows].astype(F32)
                odd = vland[s, 2 * p + 1, rows].astype(F32)
                if t < 2:
                    odd = pltpu.roll(odd, HD, 1)
                else:
                    even = pltpu.roll(even, HD, 1)
                rhs[t, s * quarter : (s + 1) * quarter, p * 128 : (p + 1) * 128] = jnp.where(
                    lane < HD, even, odd
                ).astype(BF16)

    steps[0][0]()
    local[6].wait()
    spot = lax.broadcasted_iota(jnp.int32, (1, 256), 1)
    for s in range(SEQS):
        for qb in range(BPD):
            slot = jnp.full((1, 256), BPD * TOPK, jnp.int32)
            for k in range(TOPK):
                slot = jnp.where(spot == ids_ref[s, qb, 0, k], qb * TOPK + k, slot)
            inv_v[s * BPD + qb : s * BPD + qb + 1] = slot
    to_scalar = pltpu.make_async_copy(inv_v, inv_ref, l_sem.at[8])
    to_scalar.start()
    local[2].wait()
    lax.fori_loop(0, 4, turn_input, 0)
    steps[0][1]()
    steps[1][0]()
    lax.fori_loop(4, 8, turn_input, 0)
    for n in (1, 0, 2):
        li_copy(n).start()
    for n in (3, 4, 5):
        local[n].wait()
    for s in range(SEQS):
        gates_t[s] = jax.nn.sigmoid(gate_ref[s]).T
    to_scalar.wait()
    picks[BPD * TOPK] = jnp.zeros((BLK, 2 * HD), F32)
    for n in range(2, 5):
        steps[0][n]()
        if n != 3:
            steps[1][n // 2]()

        def some(i, carry, n=n):
            at = (n - 2) * 4 + i
            prepare(at // BPD, at % BPD)
            return carry

        lax.fori_loop(0, 4, some, 0)
    steps[0][5]()

    def between(n, step):
        def at(qb):
            @pl.when(qb == n)
            def _():
                step()

        return at

    marks = [between(0, steps[1][3]), between(1, steps[1][4])]

    def attend0(qb, carry):
        attend(0, qb)
        for mark in marks:
            mark(qb)
        return carry

    lax.fori_loop(0, BPD // 3, attend0, 0)
    collect(0)
    steps[1][5]()

    marks1 = [between(0, reduces[0].begin), between(1, reduces[0].middle)]

    def attend1(qb, carry):
        attend(1, qb)
        for mark in marks1:
            mark(qb)
        return carry

    lax.fori_loop(0, BPD // 3, attend1, 0)
    collect(1)
    reduces[1].begin()
    reduces[0].turn()
    reduces[1].middle()
    reduces[0].middle_b()
    reduces[1].turn()
    finish(0)
    reduces[1].middle_b()
    landed(0)
    finish(1)
    for n in range(3):
        frm = (tp + 3 - n) % 4
        rcopy(li_in.at[frm], li_in.at[frm], s_li.at[n], r_li.at[n], (kv, frm)).wait_recv()
    mine_li = pltpu.make_async_copy(li_t.at[tp], li_in.at[tp], l_sem.at[7])
    mine_li.start()
    mine_li.wait()
    landed(1)

    def product(side, i):
        total = None
        for t in range(4):
            a = li_in[t, pl.ds(i * 4, 4), side].reshape(128, 192)
            p = jnp.dot(a, rhs[t], preferred_element_type=F32)
            total = p if total is None else total + p
        return total.reshape(4, 32, 256)

    order = (2, 1, 3, 0)
    mine = kv // 2

    def piece(dz):
        return pl.ds(((z + dz) % 4) * 4, 4)

    def w_copy(dz):
        rows = piece(dz)
        return rcopy(w_out.at[rows], w_mate.at[rows], s_w.at[dz], r_w.at[dz], partner)

    def d_copy(n):
        dz, dy = offsets[n]
        to = zy(z + dz, y + dy)
        return rcopy(wsend.at[to[0] // 2], wland.at[mine], s_d.at[n], r_d.at[n], to)

    for dz in order:
        w_out[piece(dz)] = product(other, (z + dz) % 4).astype(BF16)
        w_copy(dz).start()
    for dz in order:
        w_own[piece(dz)] = product(c, (z + dz) % 4)
    for dz in order:
        w_copy(dz).wait_recv()
        value = w_own[piece(dz)] + w_mate[piece(dz)].astype(F32)
        w_own[piece(dz)] = value
        wsend[piece(dz)] = value.astype(BF16)
        for n in range(len(offsets)):
            if offsets[n][0] == dz:
                d_copy(n).start()
    total = w_own[mine]
    for n, (dz, dy) in enumerate(offsets):
        frm = zy(z - dz, y - dy)
        slot = wland.at[frm[0] // 2]
        rcopy(slot, slot, s_d.at[n], r_d.at[n], frm).wait_recv()
        total = total + wland[frm[0] // 2].astype(F32)
    wg_ref[...] = total

    for pair in gathers:
        for g in pair:
            g.drain()
    for r in reduces:
        r.drain()
    for n in range(3):
        li_copy(n).wait_send()
        for s in range(SEQS):
            x_copy(s, n).wait_send()
    for dz in order:
        w_copy(dz).wait_send()
    for n in range(len(offsets)):
        d_copy(n).wait_send()


def whole(chosen, keys, values, gates, queries, cotangent, layer_input):
    v = pltpu.VMEM
    dma = pltpu.SemaphoreType.DMA
    wide = 2 * HD
    anywhere = pl.BlockSpec(memory_space=pltpu.HBM)
    onchip = pl.BlockSpec(memory_space=v)
    keys_n = TOPK * BLK
    nrow = HEADS * BLK
    return pl.pallas_call(
        whole_kernel,
        out_shape=[
            jax.ShapeDtypeStruct((SEQS, ROWS, HEADS * HD), BF16),
            jax.ShapeDtypeStruct((SEQS, HD, ROWS), BF16),
            jax.ShapeDtypeStruct((SEQS, HD, ROWS), BF16),
            jax.ShapeDtypeStruct((32, 256), F32),
        ],
        in_specs=[anywhere] * 7,
        out_specs=[onchip] * 4,
        scratch_shapes=[
            *[v((DEVS, ROWS, wide), BF16) for _ in range(2)],
            *[v((ZN, YN, 2, ROWS, wide), BF16) for _ in range(2)],
            *[v((ZN, YN, ROWS, wide), BF16) for _ in range(2)],
            *[v((2, 4, HALF, wide), F32) for _ in range(2)],
            *[v((2, 6, 2, HALF, wide), BF16) for _ in range(4)],
            *[v((2, 6, QUART, wide), BF16) for _ in range(4)],
            pltpu.SMEM((SEQS, BPD, 1, TOPK), jnp.int32),
            pltpu.SMEM((SEQS * BPD, 256), jnp.int32),
            v((SEQS * BPD, 256), jnp.int32),
            v((SEQS, HD, ROWS), BF16),
            v((SEQS, HD, ROWS), BF16),
            v((SEQS, HEADS, ROWS), F32),
            v((SEQS, ROWS, HEADS * HD), BF16),
            v((SEQS, ROWS, HEADS * HD), BF16),
            v((SEQS, ROWS // 4, 4096), BF16),
            v((SEQS, ROWS, HEADS), F32),
            v((SEQS * BPD, 2 * nrow, wide), BF16),
            *[v((keys_n, wide), BF16) for _ in range(3)],
            *[v((keys_n, 2 * nrow), F32) for _ in range(3)],
            *[v((keys_n, 2 * nrow), BF16) for _ in range(3)],
            v((BPD * TOPK + 1, BLK, wide), F32),
            v((ROWS, wide), F32),
            v((4, 16, 2, 32, 192), BF16),
            v((4, 16, 2, 32, 192), BF16),
            v((SEQS, HALF, wide), BF16),
            v((SEQS, 4, HALF, wide), BF16),
            v((4, 192, 256), BF16),
            v((16, 32, 256), BF16),
            v((16, 32, 256), F32),
            v((16, 32, 256), BF16),
            v((16, 32, 256), BF16),
            v((16, 32, 256), BF16),
            dma((9,)),
            *[dma((2, 2, 20)) for _ in range(2)],
            *[dma((2, 2, 16)) for _ in range(2)],
            *[dma((2, 8)) for _ in range(2)],
            *[dma((2, 4, 6)) for _ in range(2)],
            *[dma((3,)) for _ in range(2)],
            *[dma((2, 3)) for _ in range(2)],
            *[dma((4,)) for _ in range(2)],
            *[dma((15,)) for _ in range(2)],
        ],
        compiler_params=pltpu.CompilerParams(
            collective_id=0, has_side_effects=True, vmem_limit_bytes=52 * 2**20
        ),
        name="whole",
    )(
        *[
            pltpu.with_memory_space_constraint(a, pltpu.HBM)
            for a in (chosen, keys, values, gates, queries, cotangent, layer_input)
        ],
    )


def on_device(queries, key_states, value_states, cotangent, gate_logits, layer_input, chosen):
    def turned(a):
        return jnp.swapaxes(a, 1, 2)

    query_grad, key_grad, value_grad, weight_grad = whole(
        chosen, turned(key_states), turned(value_states), turned(gate_logits),
        queries, cotangent, layer_input,
    )
    return query_grad, turned(key_grad), turned(value_grad), weight_grad


def solution(mesh):
    placed = (
        P(None, "kv", "tp"),
        P(None, "kv", "tp"),
        P(None, "kv", "tp"),
        P(None, "kv", "tp"),
        P(None, "kv", "tp"),
        P(None, ("kv", "tp"), None),
        P(None, "kv", "tp", None),
    )
    return jax.shard_map(
        on_device,
        mesh=mesh,
        in_specs=placed,
        out_specs=(P(None, "kv", "tp"), P(None, "kv", "tp"), P(None, "kv", "tp"), P(("kv", "tp"), None)),
        check_vma=False,
    )
```

```python
import jax
import jax.numpy as jnp
from jax import lax
from jax.experimental import pallas as pl
from jax.experimental.pallas import tpu as pltpu
from jax.sharding import PartitionSpec as P

BLK = 64
MESH = pl.DeviceIdType.MESH
F32 = jnp.float32
BF16 = jnp.bfloat16
SEQS = 2
BPD = 6
ROWS = BPD * BLK
ZN = 4
YN = 4
DEVS = ZN * YN * 2
HD = 64
HEADS = 4
TOPK = 16
NEG = -1e30
HALF = ROWS // 2
QUART = ROWS // 4


def place():
    kv = lax.axis_index("kv")
    tp = lax.axis_index("tp")
    z, y, c = kv // 8, (kv // 2) % 4, kv % 2
    return kv, tp, z, y, c


def rcopy(src, dst, ssem, rsem, device):
    return pltpu.make_async_remote_copy(
        src_ref=src, dst_ref=dst, send_sem=ssem, recv_sem=rsem, device_id=device, device_id_type=MESH
    )


def entry_barrier(peers):
    sem = pltpu.get_barrier_semaphore()
    for peer in peers:
        pl.semaphore_signal(sem, inc=1, device_id=peer, device_id_type=MESH)
    pl.semaphore_wait(sem, len(peers))


class Ring:
    def __init__(self, pos, plus, minus, bufs, ssem, rsem):
        self.pos, self.plus, self.minus = pos, plus, minus
        self.sb, self.rb = bufs
        self.ssem, self.rsem = ssem, rsem
        self.used = []

    def copy(self, i, dev):
        return rcopy(self.sb.at[i], self.rb.at[i], self.ssem.at[i], self.rsem.at[i], dev)

    def send(self, i, dev, value):
        self.sb[i] = value.astype(BF16)
        self.copy(i, dev).start()
        self.used.append((i, dev))

    def got(self, i):
        self.copy(i, self.plus).wait_recv()
        return self.rb[i].astype(F32)

    def start(self, part):
        p = self.pos
        self.send(0, self.plus, part((p + 2) % 4, 0))
        self.send(1, self.minus, part((p + 2) % 4, 1))

    def near(self, part):
        p = self.pos
        self.send(3, self.plus, part((p + 1) % 4, 1))
        self.send(4, self.minus, part((p + 3) % 4, 0))

    def middle(self, part):
        p = self.pos
        self.send(2, self.plus, part((p + 1) % 4, 0) + self.got(0))
        self.send(5, self.minus, part((p + 3) % 4, 1) + self.got(1))

    def end(self, part):
        p = self.pos
        first = part(p, 0) + self.got(2) + self.got(4)
        second = part(p, 1) + self.got(3) + self.got(5)
        return first, second

    def drain(self):
        for i, dev in self.used:
            self.copy(i, dev).wait_send()


class Gather:
    def __init__(self, h, kv_ref, where, ssem, rsem, psend, precv):
        self.h, self.kv_ref, self.where = h, kv_ref, where
        self.ssem, self.rsem, self.psend, self.precv = ssem, rsem, psend, precv
        self.kv, self.tp, self.z, self.y, self.c = where
        self.partner = (self.kv + 1 - 2 * self.c, self.tp)
        self.sends = []
        self.shares = []

    def at(self, a, b):
        dz, dy = (b, a) if self.h == 0 else (a, b)
        return ((self.z + dz) % 4) * 8 + ((self.y + dy) % 4) * 2 + self.c

    def ref(self, a, b, part, shift=0):
        lo, n = self.h * HALF, HALF
        if part is not None:
            lo, n = lo + part * QUART, QUART
        return self.kv_ref.at[self.at(a, b) + shift, pl.ds(lo, n)]

    def copy(self, i, a, b, part, to):
        r = self.ref(a, b, part)
        return rcopy(r, r, self.ssem.at[i], self.rsem.at[i], (self.at(*to), self.tp))

    def send(self, *args):
        self.copy(*args).start()
        self.sends.append(args)

    def recv(self, i, a, b, part):
        self.copy(i, a, b, part, (1, 0)).wait_recv()

    def share_copy(self, n, a, b, shift=0):
        r = self.ref(a, b, None, shift)
        return rcopy(r, r, self.psend.at[n], self.precv.at[n], self.partner)

    def share(self, a, b):
        n = len(self.shares)
        self.shares.append((a, b))
        self.share_copy(n, a, b).start()

    def shared(self):
        for n, (a, b) in enumerate(self.shares):
            self.share_copy(n, a, b, 1 - 2 * self.c).wait_recv()

    def drain(self):
        for args in self.sends:
            self.copy(*args).wait_send()
        for n, (a, b) in enumerate(self.shares):
            self.share_copy(n, a, b).wait_send()

    def first(self):
        self.send(0, 0, 0, None, (1, 0))
        self.send(1, 0, 0, None, (-1, 0))

    def own(self):
        self.second_start(0, 0)
        self.share(0, 0)

    def second_start(self, q, a):
        self.send(4 + 4 * q, a, 0, None, (0, 1))
        self.send(5 + 4 * q, a, 0, None, (0, -1))

    def second_forward(self, q, a):
        self.recv(4 + 4 * q, a, -1, None)
        self.send(6 + 4 * q, a, -1, 0, (0, 1))
        self.recv(5 + 4 * q, a, 1, None)
        self.send(7 + 4 * q, a, 1, 1, (0, -1))
        self.share(a, -1)
        self.share(a, 1)

    def second_end(self, q, a):
        self.recv(6 + 4 * q, a, 2, 0)
        self.recv(7 + 4 * q, a, 2, 1)
        self.share(a, 2)

    def first_forward(self):
        self.recv(0, -1, 0, None)
        self.send(2, -1, 0, 0, (1, 0))
        self.second_start(1, -1)
        self.recv(1, 1, 0, None)
        self.send(3, 1, 0, 1, (-1, 0))
        self.second_start(2, 1)
        self.share(-1, 0)
        self.share(1, 0)

    def first_end(self):
        self.recv(2, 2, 0, 0)
        self.recv(3, 2, 0, 1)
        self.second_start(3, 2)
        self.share(2, 0)


def gather_steps(pair):
    def each(*calls):
        def run():
            for name, *args in calls:
                for g in pair:
                    getattr(g, name)(*args)

        return run

    return [
        each(("first",), ("own",)),
        each(("first_forward",)),
        each(("second_forward", 0, 0), ("first_end",)),
        each(("second_forward", 1, -1), ("second_forward", 2, 1), ("second_end", 0, 0)),
        each(("second_forward", 3, 2), ("second_end", 1, -1), ("second_end", 2, 1)),
        each(("second_end", 3, 2), ("shared",)),
    ]


class Reduce:
    def __init__(self, table, mate, acc, abufs, bbufs, where, s_mate, r_mate, s_ring, r_ring):
        self.table, self.mate, self.acc = table, mate, acc
        self.kv, self.tp, self.z, self.y, self.c = where
        self.s_mate, self.r_mate = s_mate, r_mate
        kv, tp, z, y, c = where
        self.partner = (kv + 1 - 2 * c, tp)

        def to(dz, dy):
            return (((z + dz) % 4) * 8 + ((y + dy) % 4) * 2 + c, tp)

        ydir = (y, to(0, 1), to(0, 3))
        zdir = (z, to(1, 0), to(3, 0))
        self.ra = [
            Ring(*(ydir if h == 0 else zdir), [b.at[h] for b in abufs], s_ring.at[h], r_ring.at[h])
            for h in range(2)
        ]
        self.rb = [
            Ring(*(zdir if h == 0 else ydir), [b.at[h] for b in bbufs], s_ring.at[2 + h], r_ring.at[2 + h])
            for h in range(2)
        ]

    def mate_copy(self, h, g):
        rows = pl.ds(h * HALF, HALF)
        if h == 0:
            src = self.table.at[:, (self.y + g) % 4, 1 - self.c, rows]
            dst = self.mate.at[:, (self.y + g) % 4, rows]
        else:
            src = self.table.at[(self.z + g) % 4, :, 1 - self.c, rows]
            dst = self.mate.at[(self.z + g) % 4, :, rows]
        return rcopy(src, dst, self.s_mate.at[h * 4 + g], self.r_mate.at[h * 4 + g], self.partner)

    def part_a(self, h):
        rows = slice(h * HALF, (h + 1) * HALF)

        def part(d, q):
            if h == 0:
                a = self.table[2 * q : 2 * q + 2, d, self.c, rows]
                b = self.mate[2 * q : 2 * q + 2, d, rows]
            else:
                a = self.table[d, 2 * q : 2 * q + 2, self.c, rows]
                b = self.mate[d, 2 * q : 2 * q + 2, rows]
            return a.astype(F32) + b.astype(F32)

        return part

    def part_b(self, h):
        def part(d, q):
            return self.acc[h, d, q * QUART : (q + 1) * QUART]

        return part

    def begin(self):
        for h in range(2):
            self.mate_copy(h, 2).wait_recv()
            self.ra[h].start(self.part_a(h))
        for h in range(2):
            self.mate_copy(h, 1).wait_recv()
            self.mate_copy(h, 3).wait_recv()
            self.ra[h].near(self.part_a(h))

    def middle(self):
        for h in range(2):
            self.ra[h].middle(self.part_a(h))

    def turn(self):
        for h in range(2):
            self.mate_copy(h, 0).wait_recv()
            first, second = self.ra[h].end(self.part_a(h))
            self.acc[h, 0:2] = first
            self.acc[h, 2:4] = second
            self.rb[h].start(self.part_b(h))
            self.rb[h].near(self.part_b(h))

    def middle_b(self):
        for h in range(2):
            self.rb[h].middle(self.part_b(h))

    def finish(self, out):
        for h in range(2):
            for q, value in enumerate(self.rb[h].end(self.part_b(h))):
                lo = h * HALF + q * QUART
                out[lo : lo + QUART] = value

    def drain(self):
        for h in range(2):
            for g in range(4):
                self.mate_copy(h, g).wait_send()
            self.ra[h].drain()
            self.rb[h].drain()


def whole_kernel(
    ids_hbm, k_hbm, v_hbm, gate_hbm, q_hbm, g_hbm, x_hbm,
    dq_ref, kg_ref, vg_ref, wg_ref,
    kv0, kv1, table0, table1, mate0, mate1, acc0, acc1, sa0, ra0, sa1, ra1, sb0, rb0, sb1, rb1,
    ids_ref, inv_ref, inv_v, k_ref, v_ref, gate_ref, q_in, g_in, x_in, gates_t, rows_all, kvbuf_a, kvbuf_b, kvbuf_c, scores_a, scores_b, scores_c, packed_a, packed_b, packed_c, picks, final,
    li_t, li_in, vsend, vland, rhs, w_out, w_own, w_mate, wsend, wland,
    l_sem, ag_s, ag_r, agp_s, agp_r, s_mate, r_mate, s_ring, r_ring, s_li, r_li, s_x, r_x, s_w, r_w, s_d, r_d,
):
    where = place()
    kv, tp, z, y, c = where
    other = 1 - c
    nrow = HEADS * BLK

    def zy(z_, y_):
        return ((z_ % 4) * 8 + (y_ % 4) * 2 + c, tp)

    partner = (kv + 1 - 2 * c, tp)
    xs = [(kv, (tp + d) % 4) for d in (1, 2, 3)]
    offsets = [(dz, dy) for dz in (2, 1, 3, 0) for dy in (2, 1, 3, 0)][:-1]
    kvs, tables = (kv0, kv1), (table0, table1)
    kvbufs, score_bufs, packs = (kvbuf_a, kvbuf_b, kvbuf_c), (scores_a, scores_b, scores_c), (packed_a, packed_b, packed_c)

    pairs = ((k_hbm, k_ref), (v_hbm, v_ref), (x_hbm, x_in), (q_hbm, q_in), (g_hbm, g_in), (gate_hbm, gate_ref), (ids_hbm, ids_ref))
    local = [pltpu.make_async_copy(a, b, l_sem.at[n]) for n, (a, b) in enumerate(pairs)]
    for d in local:
        d.start()
    peers = [partner] + xs + [zy(z + dz, y + dy) for dz, dy in offsets]
    barrier = pltpu.get_barrier_semaphore()
    for peer in peers:
        pl.semaphore_signal(barrier, inc=1, device_id=peer, device_id_type=MESH)
    local[0].wait()
    local[1].wait()
    for s in range(SEQS):
        kvs[s][kv] = jnp.concatenate([k_ref[s], v_ref[s]], axis=0).T
    pl.semaphore_wait(barrier, len(peers))

    gathers = [
        [Gather(h, kvs[s], where, ag_s.at[s, h], ag_r.at[s, h], agp_s.at[s, h], agp_r.at[s, h]) for h in range(2)]
        for s in range(SEQS)
    ]
    steps = [gather_steps(pair) for pair in gathers]
    reduces = [
        Reduce(
            tables[s], (mate0, mate1)[s], (acc0, acc1)[s],
            ((sa0, ra0), (sa1, ra1))[s], ((sb0, rb0), (sb1, rb1))[s],
            where, s_mate.at[s], r_mate.at[s], s_ring.at[s], r_ring.at[s],
        )
        for s in range(SEQS)
    ]

    def turn_input(i, carry):
        lo = pl.multiple_of(i * 512, 512)
        for s in range(SEQS):
            t = x_in[s, :, pl.ds(lo, 512)].T.reshape(2, 2, 4, 32, 96)
            for n in range(4):
                li_t[n, pl.ds(i * 2, 2), :, :, s * 96 : (s + 1) * 96] = t[:, :, n]
        return carry

    def li_copy(n):
        to = (tp + n + 1) % 4
        return rcopy(li_t.at[to], li_in.at[tp], s_li.at[n], r_li.at[n], (kv, to))

    def prepare(s, qb):
        lane = lax.broadcasted_iota(jnp.int32, (BLK, 2 * HD), 1)
        low = lane < HD
        rows = pl.ds(pl.multiple_of(qb * BLK, BLK), BLK)
        gates = gates_t[s, rows]
        at = s * BPD + qb
        for h in range(HEADS):
            pair = slice((h // 2) * 128, (h // 2) * 128 + 128)
            qv = q_in[s, rows, pair].astype(F32) * 0.125
            gv = gates[:, h : h + 1] * g_in[s, rows, pair].astype(F32)
            if h % 2 == 0:
                gv = pltpu.roll(gv, HD, 1)
            else:
                qv = pltpu.roll(qv, HD, 1)
            rows_all[at, h * BLK : (h + 1) * BLK] = jnp.where(low, qv, 0.0).astype(BF16)
            rows_all[at, nrow + h * BLK : nrow + (h + 1) * BLK] = jnp.where(low, 0.0, gv).astype(BF16)

    def begin_block(s, qb, slot):
        kvbuf, scores = kvbufs[slot], score_bufs[slot]
        at = s * BPD + qb
        kv_ref = kvs[s]
        picked = [ids_ref[s, qb, 0, k] for k in range(TOPK)]
        for k in range(TOPK):
            kvbuf[k * BLK : (k + 1) * BLK] = kv_ref[picked[k] // BPD, pl.ds((picked[k] % BPD) * BLK, BLK)]
        scores[...] = lax.dot_general(
            kvbuf[...], rows_all[at], (((1,), (1,)), ((), ())), preferred_element_type=F32
        )
        return picked

    def end_block(s, qb, slot, picked):
        kvbuf, scores, packed = kvbufs[slot], score_bufs[slot], packs[slot]
        at = s * BPD + qb
        block = kv * BPD + qb
        qpos = block * BLK + lax.broadcasted_iota(jnp.int32, (BLK, nrow), 1) % BLK
        ahead = lax.broadcasted_iota(jnp.int32, (BLK, nrow), 0) - qpos

        def masked(k):
            sc = scores[k * BLK : (k + 1) * BLK, :nrow]
            return jnp.where(ahead <= -(picked[k] * BLK), sc, NEG)

        top = None
        for k in range(TOPK):
            m = jnp.max(masked(k).reshape(8, 8, nrow), axis=0)
            top = m if top is None else jnp.maximum(top, m)
        top = jnp.max(top, axis=0, keepdims=True)
        total = jnp.zeros((8, nrow), F32)
        for k in range(TOPK):
            e = jnp.exp(masked(k) - top)
            scores[k * BLK : (k + 1) * BLK, :nrow] = e
            total = total + jnp.sum(e.reshape(8, 8, nrow), axis=0)
        scale = 1.0 / jnp.sum(total, axis=0, keepdims=True)
        dot = jnp.zeros((8, nrow), F32)
        for k in range(TOPK):
            rows = slice(k * BLK, (k + 1) * BLK)
            w = (scores[rows, :nrow] * scale).astype(BF16)
            packed[rows, nrow:] = w
            t = w.astype(F32) * scores[rows, nrow:]
            dot = dot + jnp.sum(t.reshape(8, 8, nrow), axis=0)
        row_dot = jnp.sum(dot, axis=0, keepdims=True)
        for k in range(TOPK):
            rows = slice(k * BLK, (k + 1) * BLK)
            ds = (scores[rows, :nrow] * scale) * (scores[rows, nrow:] - row_dot)
            packed[rows, :nrow] = ds.astype(BF16)
        pick = jnp.dot(packed[...], rows_all[at], preferred_element_type=F32)
        picks[pl.ds(qb * TOPK, TOPK)] = pick.reshape(TOPK, BLK, 2 * HD)
        dq_t = jnp.dot(kvbuf[...].T, packed[:, :nrow], preferred_element_type=F32)
        dq = (dq_t[:HD] * 0.125).T
        dq_ref[s, pl.ds(pl.multiple_of(qb * BLK, BLK), BLK)] = jnp.concatenate(
            [dq[h * BLK : (h + 1) * BLK] for h in range(HEADS)], axis=1
        ).astype(BF16)

    def attend(s, pair):
        blocks = (3 * pair, 3 * pair + 1, 3 * pair + 2)
        ids = [begin_block(s, qb, slot) for slot, qb in enumerate(blocks)]
        for slot, qb in enumerate(blocks):
            end_block(s, qb, slot, ids[slot])

    def collect(s):
        table = tables[s]

        def made(zz, yy, cc, b):
            col = (zz * 8 + yy * 2 + cc) * BPD + b
            total = picks[inv_ref[s * BPD, col]]
            for q in range(1, BPD):
                total = total + picks[inv_ref[s * BPD + q, col]]
            table[zz, yy, cc, b * BLK : (b + 1) * BLK] = total.astype(BF16)

        for g in (2, 1, 3, 0):

            def one(i, carry, g=g):
                for b in range(BPD // 2):
                    made(i // 2, (y + g) % 4, i % 2, b)
                    made((z + g) % 4, i // 2, i % 2, BPD // 2 + b)
                return carry

            lax.fori_loop(0, 8, one, 0)
            for h in range(2):
                reduces[s].mate_copy(h, g).start()

    quarter = ROWS // 4

    def x_copy(s, n):
        to = (tp + n + 1) % 4
        return rcopy(vsend.at[s], vland.at[s, tp], s_x.at[s, n], r_x.at[s, n], (kv, to))

    def finish(s):
        reduces[s].finish(final)
        lane = lax.broadcasted_iota(jnp.int32, (HALF, 2 * HD), 1)
        low = pltpu.roll(final[0:HALF].astype(BF16).astype(F32), HD, 1)
        value = jnp.where(lane < HD, low, final[HALF:]).astype(BF16)
        vsend[s] = value
        vland[s, tp] = value
        for n in (1, 0, 2):
            x_copy(s, n).start()
        turned = final[...].T
        kg_ref[s] = turned[:HD].astype(BF16)
        vg_ref[s] = turned[HD:].astype(BF16)

    def landed(s):
        for n in range(3):
            frm = (tp + 3 - n) % 4
            slot = vland.at[s, frm]
            rcopy(slot, slot, s_x.at[s, n], r_x.at[s, n], (kv, frm)).wait_recv()
        lane = lax.broadcasted_iota(jnp.int32, (quarter, 2 * HD), 1)
        for t in range(4):
            rows = slice((t % 2) * quarter, (t % 2 + 1) * quarter)
            for p in range(2):
                even = vland[s, 2 * p, rows].astype(F32)
                odd = vland[s, 2 * p + 1, rows].astype(F32)
                if t < 2:
                    odd = pltpu.roll(odd, HD, 1)
                else:
                    even = pltpu.roll(even, HD, 1)
                rhs[t, s * quarter : (s + 1) * quarter, p * 128 : (p + 1) * 128] = jnp.where(
                    lane < HD, even, odd
                ).astype(BF16)

    steps[0][0]()
    local[6].wait()
    spot = lax.broadcasted_iota(jnp.int32, (1, 256), 1)
    for s in range(SEQS):
        for qb in range(BPD):
            slot = jnp.full((1, 256), BPD * TOPK, jnp.int32)
            for k in range(TOPK):
                slot = jnp.where(spot == ids_ref[s, qb, 0, k], qb * TOPK + k, slot)
            inv_v[s * BPD + qb : s * BPD + qb + 1] = slot
    to_scalar = pltpu.make_async_copy(inv_v, inv_ref, l_sem.at[8])
    to_scalar.start()
    local[2].wait()
    lax.fori_loop(0, 4, turn_input, 0)
    steps[0][1]()
    steps[1][0]()
    lax.fori_loop(4, 8, turn_input, 0)
    for n in (1, 0, 2):
        li_copy(n).start()
    for n in (3, 4, 5):
        local[n].wait()
    for s in range(SEQS):
        gates_t[s] = jax.nn.sigmoid(gate_ref[s]).T
    to_scalar.wait()
    picks[BPD * TOPK] = jnp.zeros((BLK, 2 * HD), F32)
    for n in range(2, 5):
        steps[0][n]()
        if n != 3:
            steps[1][n // 2]()

        def some(i, carry, n=n):
            at = (n - 2) * 4 + i
            prepare(at // BPD, at % BPD)
            return carry

        lax.fori_loop(0, 4, some, 0)
    steps[0][5]()

    def between(n, step):
        def at(qb):
            @pl.when(qb == n)
            def _():
                step()

        return at

    marks = [between(0, steps[1][3]), between(1, steps[1][4])]

    def attend0(qb, carry):
        attend(0, qb)
        for mark in marks:
            mark(qb)
        return carry

    lax.fori_loop(0, BPD // 3, attend0, 0)
    collect(0)
    reduces[0].begin()
    steps[1][5]()

    marks1 = [between(0, reduces[0].middle), between(1, reduces[0].turn)]

    def attend1(qb, carry):
        attend(1, qb)
        for mark in marks1:
            mark(qb)
        return carry

    lax.fori_loop(0, BPD // 3, attend1, 0)
    collect(1)
    reduces[1].begin()
    reduces[1].middle()
    reduces[0].middle_b()
    reduces[1].turn()
    finish(0)
    reduces[1].middle_b()
    landed(0)
    finish(1)
    for n in range(3):
        frm = (tp + 3 - n) % 4
        rcopy(li_in.at[frm], li_in.at[frm], s_li.at[n], r_li.at[n], (kv, frm)).wait_recv()
    mine_li = pltpu.make_async_copy(li_t.at[tp], li_in.at[tp], l_sem.at[7])
    mine_li.start()
    mine_li.wait()
    landed(1)

    def product(side, i):
        total = None
        for t in range(4):
            a = li_in[t, pl.ds(i * 4, 4), side].reshape(128, 192)
            p = jnp.dot(a, rhs[t], preferred_element_type=F32)
            total = p if total is None else total + p
        return total.reshape(4, 32, 256)

    order = (2, 1, 3, 0)
    mine = kv // 2

    def piece(dz):
        return pl.ds(((z + dz) % 4) * 4, 4)

    def w_copy(dz):
        rows = piece(dz)
        return rcopy(w_out.at[rows], w_mate.at[rows], s_w.at[dz], r_w.at[dz], partner)

    def d_copy(n):
        dz, dy = offsets[n]
        to = zy(z + dz, y + dy)
        return rcopy(wsend.at[to[0] // 2], wland.at[mine], s_d.at[n], r_d.at[n], to)

    for dz in order:
        w_out[piece(dz)] = product(other, (z + dz) % 4).astype(BF16)
        w_copy(dz).start()
    for dz in order:
        w_own[piece(dz)] = product(c, (z + dz) % 4)
    for dz in order:
        w_copy(dz).wait_recv()
        value = w_own[piece(dz)] + w_mate[piece(dz)].astype(F32)
        w_own[piece(dz)] = value
        wsend[piece(dz)] = value.astype(BF16)
        for n in range(len(offsets)):
            if offsets[n][0] == dz:
                d_copy(n).start()
    total = w_own[mine]
    for n, (dz, dy) in enumerate(offsets):
        frm = zy(z - dz, y - dy)
        slot = wland.at[frm[0] // 2]
        rcopy(slot, slot, s_d.at[n], r_d.at[n], frm).wait_recv()
        total = total + wland[frm[0] // 2].astype(F32)
    wg_ref[...] = total

    for pair in gathers:
        for g in pair:
            g.drain()
    for r in reduces:
        r.drain()
    for n in range(3):
        li_copy(n).wait_send()
        for s in range(SEQS):
            x_copy(s, n).wait_send()
    for dz in order:
        w_copy(dz).wait_send()
    for n in range(len(offsets)):
        d_copy(n).wait_send()


def whole(chosen, keys, values, gates, queries, cotangent, layer_input):
    v = pltpu.VMEM
    dma = pltpu.SemaphoreType.DMA
    wide = 2 * HD
    anywhere = pl.BlockSpec(memory_space=pltpu.HBM)
    onchip = pl.BlockSpec(memory_space=v)
    keys_n = TOPK * BLK
    nrow = HEADS * BLK
    return pl.pallas_call(
        whole_kernel,
        out_shape=[
            jax.ShapeDtypeStruct((SEQS, ROWS, HEADS * HD), BF16),
            jax.ShapeDtypeStruct((SEQS, HD, ROWS), BF16),
            jax.ShapeDtypeStruct((SEQS, HD, ROWS), BF16),
            jax.ShapeDtypeStruct((32, 256), F32),
        ],
        in_specs=[anywhere] * 7,
        out_specs=[onchip] * 4,
        scratch_shapes=[
            *[v((DEVS, ROWS, wide), BF16) for _ in range(2)],
            *[v((ZN, YN, 2, ROWS, wide), BF16) for _ in range(2)],
            *[v((ZN, YN, ROWS, wide), BF16) for _ in range(2)],
            *[v((2, 4, HALF, wide), F32) for _ in range(2)],
            *[v((2, 6, 2, HALF, wide), BF16) for _ in range(4)],
            *[v((2, 6, QUART, wide), BF16) for _ in range(4)],
            pltpu.SMEM((SEQS, BPD, 1, TOPK), jnp.int32),
            pltpu.SMEM((SEQS * BPD, 256), jnp.int32),
            v((SEQS * BPD, 256), jnp.int32),
            v((SEQS, HD, ROWS), BF16),
            v((SEQS, HD, ROWS), BF16),
            v((SEQS, HEADS, ROWS), F32),
            v((SEQS, ROWS, HEADS * HD), BF16),
            v((SEQS, ROWS, HEADS * HD), BF16),
            v((SEQS, ROWS // 4, 4096), BF16),
            v((SEQS, ROWS, HEADS), F32),
            v((SEQS * BPD, 2 * nrow, wide), BF16),
            *[v((keys_n, wide), BF16) for _ in range(3)],
            *[v((keys_n, 2 * nrow), F32) for _ in range(3)],
            *[v((keys_n, 2 * nrow), BF16) for _ in range(3)],
            v((BPD * TOPK + 1, BLK, wide), F32),
            v((ROWS, wide), F32),
            v((4, 16, 2, 32, 192), BF16),
            v((4, 16, 2, 32, 192), BF16),
            v((SEQS, HALF, wide), BF16),
            v((SEQS, 4, HALF, wide), BF16),
            v((4, 192, 256), BF16),
            v((16, 32, 256), BF16),
            v((16, 32, 256), F32),
            v((16, 32, 256), BF16),
            v((16, 32, 256), BF16),
            v((16, 32, 256), BF16),
            dma((9,)),
            *[dma((2, 2, 20)) for _ in range(2)],
            *[dma((2, 2, 16)) for _ in range(2)],
            *[dma((2, 8)) for _ in range(2)],
            *[dma((2, 4, 6)) for _ in range(2)],
            *[dma((3,)) for _ in range(2)],
            *[dma((2, 3)) for _ in range(2)],
            *[dma((4,)) for _ in range(2)],
            *[dma((15,)) for _ in range(2)],
        ],
        compiler_params=pltpu.CompilerParams(
            collective_id=0, has_side_effects=True, vmem_limit_bytes=52 * 2**20
        ),
        name="whole",
    )(
        *[
            pltpu.with_memory_space_constraint(a, pltpu.HBM)
            for a in (chosen, keys, values, gates, queries, cotangent, layer_input)
        ],
    )


def on_device(queries, key_states, value_states, cotangent, gate_logits, layer_input, chosen):
    def turned(a):
        return jnp.swapaxes(a, 1, 2)

    query_grad, key_grad, value_grad, weight_grad = whole(
        chosen, turned(key_states), turned(value_states), turned(gate_logits),
        queries, cotangent, layer_input,
    )
    return query_grad, turned(key_grad), turned(value_grad), weight_grad


def solution(mesh):
    placed = (
        P(None, "kv", "tp"),
        P(None, "kv", "tp"),
        P(None, "kv", "tp"),
        P(None, "kv", "tp"),
        P(None, "kv", "tp"),
        P(None, ("kv", "tp"), None),
        P(None, "kv", "tp", None),
    )
    return jax.shard_map(
        on_device,
        mesh=mesh,
        in_specs=placed,
        out_specs=(P(None, "kv", "tp"), P(None, "kv", "tp"), P(None, "kv", "tp"), P(("kv", "tp"), None)),
        check_vma=False,
    )
```
